32 devices in a mesh: sp: 4 (over z), dp: 8 (over y, x, core).
Axes of the slice: x: 2, y: 2, z: 4, core: 2. Of those that a mesh axis runs over, the one named last changes fastest.
Arguments:
- queries: bfloat16 [8, 512, 1024], P('dp', 'sp'), may hold values from -6 to 6
- key_rows: bfloat16 [8, 512, 1024], P('dp', 'sp'), may hold values from -6 to 6
- values: bfloat16 [8, 512, 2048], P('dp', 'sp'), may hold values from -6 to 6
- out_gate: bfloat16 [8, 512, 2048], P('dp', 'sp'), may hold values from -6 to 6
- input_gate: bfloat16 [8, 4, 512], P('dp', None, 'sp'), may hold values from -6 to 205
- forget_gate: bfloat16 [8, 4, 512], P('dp', None, 'sp'), may hold values from 0.5 to 13
- out_weight: bfloat16 [2048, 2048], P(None, 'dp'), may hold values from -0.125 to 0.125
Outputs:
- layer_out: bfloat16 [8, 512, 2048], P('dp', 'sp')
The draws below stay inside these ranges and needn't reach their ends.
All inputs are finite; a program needn't handle non-finite values.
Results may differ from the reference program's by a relative error of at most 0.0057.
Values may be sent and summed in bfloat16 or wider, within the bound.
No kernel may reach another device: no remote copies, remote signals or barrier semaphores. Data moves between devices by JAX's collectives and lax.ppermute only.
A program may use at most 64 MiB of HBM per device.

```python
import jax
import jax.numpy as jnp
from jax import lax

D = 2048
MEMORY_UNITS = 4
DK = 256
DV = 512
BLOCK = 128
TOK_DEV = 128
STEP_TOTAL = 512
STREAM_TOTAL = 8
VW = 2048


def draw_input_gate(key, part):
    dims_all = (STREAM_TOTAL, MEMORY_UNITS, STEP_TOTAL)
    result = jnp.clip(1.5 * jax.random.normal(jax.random.fold_in(key, 4), dims_all, jnp.float32), -6.0, 6.0)
    return result.astype(jnp.bfloat16)


def draw_forget_gate(key, part):
    dims_all = (STREAM_TOTAL, MEMORY_UNITS, STEP_TOTAL)
    multiplier = jnp.exp(jax.random.uniform(jax.random.fold_in(key, 11), (STREAM_TOTAL, MEMORY_UNITS, STEP_TOTAL // TOK_DEV, 1), jnp.float32, -0.7, 0.7))
    multiplier = jnp.broadcast_to(multiplier, (STREAM_TOTAL, MEMORY_UNITS, STEP_TOTAL // TOK_DEV, TOK_DEV)).reshape(dims_all)
    gaussian_jitter = jnp.exp(0.5 * jnp.clip(jax.random.normal(jax.random.fold_in(key, 12), dims_all, jnp.float32), -3.0, 3.0))
    ranking = jax.random.randint(jax.random.fold_in(key, 13), (STREAM_TOTAL, MEMORY_UNITS), 0, 1 << 20) * MEMORY_UNITS + lax.broadcasted_iota(jnp.int32, (STREAM_TOTAL, MEMORY_UNITS), 1)
    order = jnp.argsort(ranking, axis=1)
    position_rank = jnp.argsort(order, axis=1)
    quick_head = (position_rank < MEMORY_UNITS // 2)[:, :, None]
    background_level = jnp.where(quick_head, 1.0 / 40.0, 0.5 / STEP_TOTAL) * jnp.ones(dims_all, jnp.float32)
    spike_offset = jax.random.randint(jax.random.fold_in(key, 14), (STREAM_TOTAL, MEMORY_UNITS, 3, 1), 0, STEP_TOTAL)
    spike_indices = lax.broadcasted_iota(jnp.int32, (1, 1, 1, STEP_TOTAL), 3)
    spike_count = jnp.any(spike_indices == spike_offset, axis=2)
    spike_magnitude = jnp.where(spike_count, 0.4, background_level * multiplier * gaussian_jitter)
    gate_logits = -jnp.log(jnp.expm1(spike_magnitude))
    return gate_logits.astype(jnp.bfloat16)


def levels(rng, shape, cuts, smallest, high):
    def one(position, shards_of):
        steps = jax.random.uniform(jax.random.fold_in(jax.random.fold_in(rng, 6), position), (shards_of,), jnp.float32, smallest / len(cuts), high / len(cuts))
        return jnp.repeat(jnp.exp(steps), shape[position] // shards_of).reshape((-1,) + (1,) * (len(shape) - position - 1))

    gain = one(*cuts[0])
    for cut in cuts[1:]:
        gain = gain * one(*cut)
    return gain


def bell_draw(own_key, dims, width, bound, shards=(), dtype=jnp.bfloat16):
    entries = jax.random.normal(own_key, dims, jnp.float32) * width
    if len(shards) > 0:
        entries = levels(own_key, dims, shards, -0.22, 0.18) * entries
    return jnp.clip(entries, min=-bound, max=bound).astype(dtype)


def setup_inputs(seed: int = 0) -> dict:
    key_of = jax.random.split(jax.random.key(seed), 8)
    return {
        "queries": bell_draw(key_of[0], (STREAM_TOTAL, STEP_TOTAL, MEMORY_UNITS * DK), 1.0, 6.0, ((0, 8), (1, 4))),
        "key_rows": bell_draw(key_of[1], (STREAM_TOTAL, STEP_TOTAL, MEMORY_UNITS * DK), 1.0, 6.0, ((0, 8), (1, 4))),
        "values": bell_draw(key_of[2], (STREAM_TOTAL, STEP_TOTAL, VW), 1.0, 6.0, ((0, 8), (1, 4))),
        "out_gate": bell_draw(key_of[3], (STREAM_TOTAL, STEP_TOTAL, VW), 1.0, 6.0, ((0, 8), (1, 4))),
        "input_gate": draw_input_gate(jax.random.fold_in(key_of[7], 71), 0),
        "forget_gate": draw_forget_gate(jax.random.fold_in(key_of[7], 71), 0),
        "out_weight": bell_draw(key_of[6], (VW, D), VW ** -0.5, 0.125, ((1, 8),)),
    }


def memory_cell(query_rows, key_in, value_rows, input_log, forget_log):
    block_count = query_rows.shape[0] // BLOCK
    key_width = query_rows.shape[1]
    value_width = value_rows.shape[1]
    key_scale = key_width ** -0.5
    causal = lax.broadcasted_iota(jnp.int32, (BLOCK, BLOCK), 0) >= lax.broadcasted_iota(jnp.int32, (BLOCK, BLOCK), 1)
    highest = lax.Precision.HIGHEST

    def block_step(state_in, inputs):
        memory, normer, stabil = state_in
        query_part, key_part, value_part, gain_part, decay_part = inputs
        query_part = query_part.astype(jnp.float32)
        key_part = key_part.astype(jnp.float32) * key_scale
        value_part = value_part.astype(jnp.float32)
        running = jnp.cumsum(decay_part)
        log_weight = running[:, None] - running[None, :] + gain_part[None, :]
        log_weight = jnp.where(causal, log_weight, -jnp.inf)
        carried_log = running + stabil
        row_top = jnp.maximum(carried_log, jnp.max(log_weight, axis=1))
        scores = jnp.dot(query_part, key_part.T, precision=highest) * jnp.exp(log_weight - row_top[:, None])
        carried = jnp.exp(carried_log - row_top)
        numerator = jnp.dot(scores, value_part, precision=highest) + carried[:, None] * jnp.dot(query_part, memory, precision=highest)
        denominator = jnp.sum(scores, axis=1) + carried * jnp.dot(query_part, normer, precision=highest)
        output = numerator / jnp.maximum(jnp.abs(denominator), 1.0)[:, None]
        block_end = running[-1]
        weight_log = block_end - running + gain_part
        new_top = jnp.maximum(block_end + stabil, jnp.max(weight_log))
        weights = jnp.exp(weight_log - new_top)
        retain = jnp.exp(block_end + stabil - new_top)
        memory = retain * memory + jnp.dot((key_part * weights[:, None]).T, value_part, precision=highest)
        normer = retain * normer + jnp.dot(weights, key_part, precision=highest)
        return (memory, normer, new_top), output

    start_state = (jnp.zeros((key_width, value_width), jnp.float32), jnp.zeros((key_width,), jnp.float32), jnp.zeros((), jnp.float32))
    blocks = tuple(source.reshape((block_count, BLOCK) + source.shape[1:]) for source in (query_rows, key_in, value_rows, input_log, forget_log))
    _, outputs = lax.scan(block_step, start_state, blocks)
    return outputs.reshape(block_count * BLOCK, value_width)


def reference(queries, key_rows, values, out_gate, input_gate, forget_gate, out_weight):
    query_heads = queries.reshape(STREAM_TOTAL, STEP_TOTAL, MEMORY_UNITS, DK).transpose(0, 2, 1, 3)
    key_heads = key_rows.reshape(STREAM_TOTAL, STEP_TOTAL, MEMORY_UNITS, DK).transpose(0, 2, 1, 3)
    value_heads = values.reshape(STREAM_TOTAL, STEP_TOTAL, MEMORY_UNITS, DV).transpose(0, 2, 1, 3)
    input_log = input_gate.astype(jnp.float32)
    forget_log = jax.nn.log_sigmoid(forget_gate.astype(jnp.float32))
    per_head = jax.vmap(jax.vmap(memory_cell))
    cell_out = per_head(query_heads, key_heads, value_heads, input_log, forget_log)
    hidden = cell_out.transpose(0, 2, 1, 3).reshape(STREAM_TOTAL, STEP_TOTAL, VW).astype(jnp.bfloat16)
    hidden = lax.optimization_barrier(hidden)
    gated = (hidden.astype(jnp.float32) * jax.nn.sigmoid(out_gate.astype(jnp.float32))).astype(jnp.bfloat16)
    projected = jnp.dot(gated.reshape(STREAM_TOTAL * STEP_TOTAL, VW), out_weight, preferred_element_type=jnp.float32)
    return projected.reshape(STREAM_TOTAL, STEP_TOTAL, D).astype(jnp.bfloat16)
```

```python
import functools

import jax
import jax.numpy as jnp
from jax import lax
from jax.experimental import pallas as pl
from jax.experimental.pallas import tpu as pltpu
from jax.sharding import PartitionSpec as P

BLOCK = 128


def memory_cell(query_rows, key_in, value_rows, input_log, forget_log):
    block_count = query_rows.shape[0] // BLOCK
    key_width = query_rows.shape[1]
    value_width = value_rows.shape[1]
    key_scale = key_width ** (-0.5)
    causal = lax.broadcasted_iota(jnp.int32, (BLOCK, BLOCK), 0) >= lax.broadcasted_iota(
        jnp.int32, (BLOCK, BLOCK), 1
    )
    highest = lax.Precision.HIGHEST

    def block_step(state_in, inputs):
        memory, normer, stabil = state_in
        query_part, key_part, value_part, gain_part, decay_part = inputs
        query_part = query_part.astype(jnp.float32)
        key_part = key_part.astype(jnp.float32) * key_scale
        value_part = value_part.astype(jnp.float32)
        running = jnp.cumsum(decay_part)
        log_weight = running[:, None] - running[None, :] + gain_part[None, :]
        log_weight = jnp.where(causal, log_weight, -jnp.inf)
        carried_log = running + stabil
        row_top = jnp.maximum(carried_log, jnp.max(log_weight, axis=1))
        scores = jnp.dot(query_part, key_part.T, precision=highest) * jnp.exp(
            log_weight - row_top[:, None]
        )
        carried = jnp.exp(carried_log - row_top)
        numerator = jnp.dot(scores, value_part, precision=highest) + carried[:, None] * jnp.dot(
            query_part, memory, precision=highest
        )
        denominator = jnp.sum(scores, axis=1) + carried * jnp.dot(
            query_part, normer, precision=highest
        )
        output = numerator / jnp.maximum(jnp.abs(denominator), 1.0)[:, None]
        block_end = running[-1]
        weight_log = block_end - running + gain_part
        new_top = jnp.maximum(block_end + stabil, jnp.max(weight_log))
        weights = jnp.exp(weight_log - new_top)
        retain = jnp.exp(block_end + stabil - new_top)
        memory = retain * memory + jnp.dot(
            (key_part * weights[:, None]).T, value_part, precision=highest
        )
        normer = retain * normer + jnp.dot(weights, key_part, precision=highest)
        return ((memory, normer, new_top), output)

    start_state = (
        jnp.zeros((key_width, value_width), jnp.float32),
        jnp.zeros((key_width,), jnp.float32),
        jnp.zeros((), jnp.float32),
    )
    blocks = tuple(
        (
            source.reshape((block_count, BLOCK) + source.shape[1:])
            for source in (query_rows, key_in, value_rows, input_log, forget_log)
        )
    )
    _, outputs = lax.scan(block_step, start_state, blocks)
    return outputs.reshape(block_count * BLOCK, value_width)


CORE, XBIT, YBIT = 1, 2, 4


def gather_weight(shard):
    rows = shard.shape[0]
    half = rows // 2

    def swap(piece, bit):
        pairs = [(i, i ^ bit) for i in range(lax.axis_size("dp"))]
        return lax.ppermute(piece, "dp", pairs)

    from_x = swap(shard, XBIT)
    from_y = swap(shard, YBIT)
    from_core = swap(shard, CORE)
    top = swap(from_x[:half], YBIT)
    bottom = swap(from_y[half:], XBIT)
    x_core = swap(from_x, CORE)
    y_core = swap(from_y, CORE)
    top_core = swap(top, CORE)
    bottom_core = swap(bottom, CORE)
    return [
        (0, 0, shard),
        (CORE, 0, from_core),
        (XBIT, 0, from_x),
        (XBIT | CORE, 0, x_core),
        (YBIT, 0, from_y),
        (YBIT | CORE, 0, y_core),
        (XBIT | YBIT, 0, top),
        (XBIT | YBIT, half, bottom),
        (XBIT | YBIT | CORE, 0, top_core),
        (XBIT | YBIT | CORE, half, bottom_core),
    ]


def project_kernel(plan, place_ref, hidden_ref, gate_ref, *refs):
    pieces, out_ref = refs[:-1], refs[-1]
    gated = (
        hidden_ref[...].astype(jnp.float32) * jax.nn.sigmoid(gate_ref[...].astype(jnp.float32))
    ).astype(jnp.bfloat16)
    totals = {}
    for (mask, start), piece in zip(plan, pieces):
        part = jnp.dot(
            gated[:, start : start + piece.shape[0]], piece[...], preferred_element_type=jnp.float32
        )
        totals[mask] = totals[mask] + part if mask in totals else part
    width = pieces[0].shape[1]
    for mask, total in totals.items():
        place = pl.multiple_of((place_ref[0] ^ mask) * width, width)
        out_ref[:, pl.ds(place, width)] = total.astype(out_ref.dtype)


def project(hidden, gate, pieces):
    place = lax.axis_index("dp").astype(jnp.int32).reshape(1)
    plan = tuple((mask, start) for mask, start, _ in pieces)
    arrays = [piece for _, _, piece in pieces]
    columns = arrays[0].shape[1] * lax.axis_size("dp")
    vmem = pl.BlockSpec(memory_space=pltpu.VMEM)
    return pl.pallas_call(
        functools.partial(project_kernel, plan),
        out_shape=jax.ShapeDtypeStruct((hidden.shape[0], columns), jnp.bfloat16),
        in_specs=[pl.BlockSpec(memory_space=pltpu.SMEM)] + [vmem] * (2 + len(arrays)),
        out_specs=vmem,
        name="project",
    )(place, hidden, gate, *arrays)


def body(queries, key_rows, values, out_gate, input_gate, forget_gate, out_weight):
    group_count = lax.axis_size("sp")
    token_count = queries.shape[1]
    head_count = input_gate.shape[1]
    copies = group_count // head_count
    head_key = queries.shape[2] // head_count
    slice_width = values.shape[2] // group_count

    def spread(source):
        widened = jnp.broadcast_to(
            source[0].reshape(token_count, head_count, 1, head_key),
            (token_count, head_count, copies, head_key),
        )
        return widened.reshape(token_count, group_count, head_key)

    def spread_gate(source):
        return jnp.repeat(source[0].T, copies, axis=1)

    query_all, key_all = (
        lax.all_to_all(spread(queries), "sp", split_axis=1, concat_axis=0, tiled=True),
        lax.all_to_all(spread(key_rows), "sp", split_axis=1, concat_axis=0, tiled=True),
    )
    value_all, input_all, forget_all = (
        lax.all_to_all(
            values[0].reshape(token_count, group_count, slice_width),
            "sp",
            split_axis=1,
            concat_axis=0,
            tiled=True,
        ),
        lax.all_to_all(spread_gate(input_gate), "sp", split_axis=1, concat_axis=0, tiled=True),
        lax.all_to_all(spread_gate(forget_gate), "sp", split_axis=1, concat_axis=0, tiled=True),
    )
    output = memory_cell(
        query_all[:, 0],
        key_all[:, 0],
        value_all[:, 0],
        input_all[:, 0].astype(jnp.float32),
        jax.nn.log_sigmoid(forget_all[:, 0].astype(jnp.float32)),
    )
    hidden = output.astype(jnp.bfloat16)
    token_rows = lax.all_to_all(hidden, "sp", split_axis=0, concat_axis=1, tiled=True)
    if lax.axis_size("dp") == 8:
        return project(token_rows, out_gate[0], gather_weight(out_weight))[None]
    gated_rows = (
        token_rows.astype(jnp.float32) * jax.nn.sigmoid(out_gate[0].astype(jnp.float32))
    ).astype(jnp.bfloat16)
    projected = jnp.dot(
        gated_rows,
        lax.all_gather(out_weight, "dp", axis=1, tiled=True),
        preferred_element_type=jnp.float32,
    )
    return projected.astype(jnp.bfloat16)[None]


def solution(mesh):
    return jax.shard_map(
        body,
        mesh=mesh,
        in_specs=(
            P("dp", "sp", None),
            P("dp", "sp", None),
            P("dp", "sp", None),
            P("dp", "sp", None),
            P("dp", None, "sp"),
            P("dp", None, "sp"),
            P(None, "dp"),
        ),
        out_specs=P("dp", "sp", None),
        check_vma=False,
    )
```

```python
import functools

import jax
import jax.numpy as jnp
from jax import lax
from jax.experimental import pallas as pl
from jax.experimental.pallas import tpu as pltpu
from jax.sharding import PartitionSpec as P

BLOCK = 128


def memory_cell(query_rows, key_in, value_rows, input_log, forget_log):
    block_count = query_rows.shape[0] // BLOCK
    key_width = query_rows.shape[1]
    value_width = value_rows.shape[1]
    key_scale = key_width ** (-0.5)
    causal = lax.broadcasted_iota(jnp.int32, (BLOCK, BLOCK), 0) >= lax.broadcasted_iota(
        jnp.int32, (BLOCK, BLOCK), 1
    )
    highest = lax.Precision.HIGHEST

    def block_step(state_in, inputs):
        memory, normer, stabil = state_in
        query_part, key_part, value_part, gain_part, decay_part = inputs
        query_part = query_part.astype(jnp.float32)
        key_part = key_part.astype(jnp.float32) * key_scale
        value_part = value_part.astype(jnp.float32)
        running = jnp.cumsum(decay_part)
        log_weight = running[:, None] - running[None, :] + gain_part[None, :]
        log_weight = jnp.where(causal, log_weight, -jnp.inf)
        carried_log = running + stabil
        row_top = jnp.maximum(carried_log, jnp.max(log_weight, axis=1))
        scores = jnp.dot(query_part, key_part.T, precision=highest) * jnp.exp(
            log_weight - row_top[:, None]
        )
        carried = jnp.exp(carried_log - row_top)
        numerator = jnp.dot(scores, value_part, precision=highest) + carried[:, None] * jnp.dot(
            query_part, memory, precision=highest
        )
        denominator = jnp.sum(scores, axis=1) + carried * jnp.dot(
            query_part, normer, precision=highest
        )
        output = numerator / jnp.maximum(jnp.abs(denominator), 1.0)[:, None]
        block_end = running[-1]
        weight_log = block_end - running + gain_part
        new_top = jnp.maximum(block_end + stabil, jnp.max(weight_log))
        weights = jnp.exp(weight_log - new_top)
        retain = jnp.exp(block_end + stabil - new_top)
        memory = retain * memory + jnp.dot(
            (key_part * weights[:, None]).T, value_part, precision=highest
        )
        normer = retain * normer + jnp.dot(weights, key_part, precision=highest)
        return ((memory, normer, new_top), output)

    start_state = (
        jnp.zeros((key_width, value_width), jnp.float32),
        jnp.zeros((key_width,), jnp.float32),
        jnp.zeros((), jnp.float32),
    )
    blocks = tuple(
        (
            source.reshape((block_count, BLOCK) + source.shape[1:])
            for source in (query_rows, key_in, value_rows, input_log, forget_log)
        )
    )
    _, outputs = lax.scan(block_step, start_state, blocks)
    return outputs.reshape(block_count * BLOCK, value_width)


CORE, XBIT, YBIT = 1, 2, 4


def gather_weight(shard):
    rows = shard.shape[0]
    half = rows // 2

    def swap(piece, bit):
        pairs = [(i, i ^ bit) for i in range(lax.axis_size("dp"))]
        return lax.ppermute(piece, "dp", pairs)

    from_x = swap(shard, XBIT)
    from_y = swap(shard, YBIT)
    from_core = swap(shard, CORE)
    top = swap(from_x[:half], YBIT)
    bottom = swap(from_y[half:], XBIT)
    x_core = swap(from_x, CORE)
    y_core = swap(from_y, CORE)
    top_core = swap(top, CORE)
    bottom_core = swap(bottom, CORE)
    return [
        (0, 0, shard),
        (CORE, 0, from_core),
        (XBIT, 0, from_x),
        (XBIT | CORE, 0, x_core),
        (YBIT, 0, from_y),
        (YBIT | CORE, 0, y_core),
        (XBIT | YBIT, 0, top),
        (XBIT | YBIT, half, bottom),
        (XBIT | YBIT | CORE, 0, top_core),
        (XBIT | YBIT | CORE, half, bottom_core),
    ]


LANES = 128


def log_forget(gates):
    return -jnp.log1p(jnp.exp(-gates))


def running_sum(rows):
    width = rows.shape[1]
    upto = lax.broadcasted_iota(jnp.int32, (width, width), 0) <= lax.broadcasted_iota(
        jnp.int32, (width, width), 1
    )
    return jnp.dot(
        rows,
        upto.astype(jnp.float32),
        precision=lax.Precision.HIGHEST,
        preferred_element_type=jnp.float32,
    )


def times_transpose(left, right):
    return lax.dot_general(
        left, right, (((1,), (1,)), ((), ())), preferred_element_type=jnp.float32
    )


def three_terms(value):
    high = value.astype(jnp.bfloat16).astype(jnp.float32)
    middle = (value - high).astype(jnp.bfloat16).astype(jnp.float32)
    return [high, middle, value - high - middle]


def to_lanes(columns, rows):
    lane = lax.broadcasted_iota(jnp.int32, (rows, LANES), 1)
    tile = jnp.zeros((rows, LANES), jnp.float32)
    for place, column in enumerate(columns):
        tile = jnp.where(lane == place, column, tile)
    return tile


def pack_kernel(key_ref, value_ref, input_ref, forget_ref, *payload_refs):
    tokens = key_ref.shape[0]
    key_width = key_ref.shape[1] // len(payload_refs)
    value_width = value_ref.shape[1] // len(payload_refs)
    gates = jnp.concatenate(
        [input_ref[...].astype(jnp.float32), forget_ref[...].astype(jnp.float32)], axis=0
    ).astype(jnp.bfloat16)
    for place, payload in enumerate(payload_refs):
        payload[:tokens, :key_width] = key_ref[:, place * key_width : (place + 1) * key_width]
        payload[:tokens, key_width:] = value_ref[
            :, place * value_width : (place + 1) * value_width
        ]
        payload[tokens:, : gates.shape[1]] = gates
        payload[tokens:, gates.shape[1] :] = jnp.zeros(
            (gates.shape[0], payload.shape[1] - gates.shape[1]), jnp.bfloat16
        )


def local_kernel(heads, query_ref, key_ref, value_ref, input_ref, forget_ref, total_ref, note_ref):
    tokens = query_ref.shape[0]
    key_width = query_ref.shape[1] // heads
    value_width = value_ref.shape[1] // heads
    running = running_sum(log_forget(forget_ref[...].astype(jnp.float32)))
    level = input_ref[...].astype(jnp.float32) - running
    causal = lax.broadcasted_iota(jnp.int32, (tokens, tokens), 0) >= lax.broadcasted_iota(
        jnp.int32, (tokens, tokens), 1
    )
    notes = []
    for head in range(heads):
        keys = slice(head * key_width, (head + 1) * key_width)
        channels = slice(head * value_width, (head + 1) * value_width)
        masked = jnp.where(causal, level[head : head + 1, :], -jnp.inf)
        top = jnp.max(masked, axis=1, keepdims=True)
        scores = times_transpose(query_ref[:, keys], key_ref[:, keys])
        scores = scores * (key_width ** (-0.5)) * jnp.exp(masked - top)
        notes += [jnp.sum(scores, axis=1, keepdims=True), top]
        total_ref[:, channels] = jnp.dot(
            scores.astype(jnp.bfloat16), value_ref[:, channels], preferred_element_type=jnp.float32
        )
    note_ref[...] = to_lanes(notes, tokens)


def serve_kernel(
    heads, first, count, leads_ref, earlier_ref, here_ref, query_ref, near_ref, far_ref,
    own_ref, next_ref, later_ref,
):
    tokens = query_ref.shape[0]
    key_width = query_ref.shape[1] // heads
    value_width = (here_ref.shape[1] - count * key_width) // count
    leads = leads_ref[0] != 0
    gates0 = earlier_ref[tokens:, :tokens].astype(jnp.float32)
    gates1 = here_ref[tokens:, :tokens].astype(jnp.float32)
    running0 = running_sum(log_forget(gates0[heads:]))
    running1 = running_sum(log_forget(gates1[heads:]))
    end0, end1 = running0[:, tokens - 1 :], running1[:, tokens - 1 :]
    shift = jnp.where(leads, end0, 0.0)
    level0 = gates0[:heads] - running0
    level1 = gates1[:heads] - running1 - shift
    top0 = jnp.maximum(jnp.max(level0, axis=1, keepdims=True), 0.0)
    top = jnp.max(level1, axis=1, keepdims=True)
    top = jnp.where(leads, jnp.maximum(top, top0), top)
    weight_own = jnp.exp(level0 - top0)
    weight0 = jnp.where(leads, jnp.exp(level0 - top), 0.0)
    weight1 = jnp.exp(level1 - top)
    weight = jnp.concatenate([weight0, weight1], axis=1)
    reach, reach_own = top + shift + end1, top0 + end0
    key_scale = key_width ** (-0.5)
    own_notes, next_notes, later_notes = [], [], []
    for place in range(count):
        head = first + place
        pick = slice(head, head + 1)
        columns = slice(head * key_width, (head + 1) * key_width)
        keys = slice(place * key_width, (place + 1) * key_width)
        start = count * key_width + place * value_width
        channels = slice(start, start + value_width)
        out = slice(place * value_width, (place + 1) * value_width)
        key0, value0 = earlier_ref[:tokens, keys], earlier_ref[:tokens, channels]
        key_both = jnp.concatenate([key0, here_ref[:tokens, keys]], axis=0)
        value_both = jnp.concatenate([value0, here_ref[:tokens, channels]], axis=0)
        rows = jnp.concatenate([near_ref[:, columns], far_ref[:, columns]], axis=0)
        scores = times_transpose(rows, key_both) * key_scale * weight[pick]
        sums = jnp.sum(scores, axis=1, keepdims=True)
        given = jnp.dot(
            scores.astype(jnp.bfloat16), value_both, preferred_element_type=jnp.float32
        ).astype(jnp.bfloat16)
        next_ref[:, out] = given[:tokens]
        later_ref[:, out] = given[tokens:]
        scores = times_transpose(query_ref[:, columns], key0) * key_scale * weight_own[pick]
        own_ref[:, out] = jnp.dot(
            scores.astype(jnp.bfloat16), value0, preferred_element_type=jnp.float32
        ).astype(jnp.bfloat16)
        tail = three_terms(end1[pick])
        next_notes += three_terms(sums[:tokens]) + three_terms(reach[pick]) + tail
        later_notes += three_terms(sums[tokens:]) + three_terms(reach[pick]) + tail
        own_notes += (
            three_terms(jnp.sum(scores, axis=1, keepdims=True))
            + three_terms(reach_own[pick])
            + tail
        )
    for ref, notes in ((own_ref, own_notes), (next_ref, next_notes), (later_ref, later_notes)):
        ref[:, count * value_width :] = to_lanes(notes, tokens).astype(jnp.bfloat16)


def finish_kernel(plan, heads, place_ref, total_ref, note_ref, gate_ref, *refs):
    out_ref, pieces, messages = refs[-1], refs[-1 - len(plan) : -1], refs[: -1 - len(plan)]
    chunks = len(messages) // 3
    owns, nears, fars = messages[:chunks], messages[chunks : 2 * chunks], messages[2 * chunks :]
    count = heads // chunks
    value_width = total_ref.shape[1] // heads
    block = place_ref[1]
    from_own, from_near, from_far = block == 1, block >= 2, block >= 3
    notes = note_ref[...]
    gated = []
    for head in range(heads):
        chunk, place = divmod(head, count)
        channels = slice(head * value_width, (head + 1) * value_width)
        out = slice(place * value_width, (place + 1) * value_width)

        def note(ref, entry):
            tile = ref[:, count * value_width :].astype(jnp.float32)
            at = (place * 3 + entry) * 3
            return tile[:, at : at + 1] + tile[:, at + 1 : at + 2] + tile[:, at + 2 : at + 3]

        own, near, far = owns[chunk], nears[chunk], fars[chunk]
        top = notes[:, 2 * head + 1 : 2 * head + 2]
        reach_own, reach_near = note(own, 1), note(near, 1)
        reach_far = note(far, 1) + note(near, 2)
        state = jnp.where(from_own, reach_own, jnp.where(from_near, reach_near, 0.0))
        state = jnp.where(from_far, jnp.maximum(state, reach_far), state)
        peak = jnp.maximum(top, state)
        scale = jnp.exp(top - peak)
        scale_own = jnp.where(from_own, jnp.exp(reach_own - peak), 0.0)
        scale_near = jnp.where(from_near, jnp.exp(reach_near - peak), 0.0)
        scale_far = jnp.where(from_far, jnp.exp(reach_far - peak), 0.0)
        weight = (
            scale * notes[:, 2 * head : 2 * head + 1]
            + scale_own * note(own, 0)
            + scale_near * note(near, 0)
            + scale_far * note(far, 0)
        )
        inverse = 1.0 / jnp.maximum(jnp.abs(weight), 1.0)
        cell = (
            scale * total_ref[:, channels]
            + scale_own * own[:, out].astype(jnp.float32)
            + scale_near * near[:, out].astype(jnp.float32)
            + scale_far * far[:, out].astype(jnp.float32)
        ) * inverse
        hidden = cell.astype(jnp.bfloat16).astype(jnp.float32)
        gate = jax.nn.sigmoid(gate_ref[:, channels].astype(jnp.float32))
        gated.append((hidden * gate).astype(jnp.bfloat16))
    gated = jnp.concatenate(gated, axis=1)
    totals = {}
    for (mask, start), piece in zip(plan, pieces):
        part = jnp.dot(
            gated[:, start : start + piece.shape[0]], piece[...], preferred_element_type=jnp.float32
        )
        totals[mask] = totals[mask] + part if mask in totals else part
    width = pieces[0].shape[1]
    for mask, total in totals.items():
        start = pl.multiple_of((place_ref[0] ^ mask) * width, width)
        out_ref[:, pl.ds(start, width)] = total.astype(out_ref.dtype)


MIB = 1 << 20
CHUNKS = 2


def kernel_call(kernel, name, scalars, operands, outs, flops, limit):
    vmem = pl.BlockSpec(memory_space=pltpu.VMEM)
    size = sum(x.size * x.dtype.itemsize for x in operands + outs)
    return pl.pallas_call(
        kernel,
        out_shape=outs,
        in_specs=[pl.BlockSpec(memory_space=pltpu.SMEM)] * len(scalars) + [vmem] * len(operands),
        out_specs=[vmem] * len(outs),
        compiler_params=pltpu.CompilerParams(vmem_limit_bytes=limit * MIB),
        cost_estimate=pl.CostEstimate(flops=flops, bytes_accessed=size, transcendentals=0),
        name=name,
    )(*scalars, *operands)


def block_body(queries, key_rows, values, out_gate, input_gate, forget_gate, out_weight):
    query, key, value, gate = queries[0], key_rows[0], values[0], out_gate[0]
    input_log, forget = input_gate[0], forget_gate[0]
    tokens, heads = query.shape[0], input_log.shape[0]
    key_width, value_width = query.shape[1] // heads, value.shape[1] // heads
    count = heads // CHUNKS
    position = lax.axis_index("sp").astype(jnp.int32)
    shape = jax.ShapeDtypeStruct

    payloads = kernel_call(
        pack_kernel,
        "pack",
        [],
        [key, value, input_log, forget],
        [shape((tokens + 2 * heads, count * (key_width + value_width)), jnp.bfloat16)] * CHUNKS,
        0,
        8,
    )
    earlier = [lax.ppermute(payload, "sp", [(0, 1)]) for payload in payloads]
    near = lax.ppermute(query, "sp", [(2, 1), (3, 2)])
    far = lax.ppermute(query, "sp", [(3, 1)])
    pieces = gather_weight(out_weight)
    total, notes = kernel_call(
        functools.partial(local_kernel, heads),
        "local",
        [],
        [query, key, value, input_log, forget],
        [shape(value.shape, jnp.float32), shape((tokens, LANES), jnp.float32)],
        2 * heads * tokens * tokens * (key_width + value_width),
        12,
    )
    leads = (position == 1).astype(jnp.int32).reshape(1)
    message = shape((tokens, count * value_width + LANES), jnp.bfloat16)
    owns, nears, fars = [], [], []
    for chunk in range(CHUNKS):
        own, given_next, given_later = kernel_call(
            functools.partial(serve_kernel, heads, chunk * count, count),
            "serve",
            [leads],
            [earlier[chunk], payloads[chunk], query, near, far],
            [message] * 3,
            2 * count * 5 * tokens * tokens * (key_width + value_width),
            12,
        )
        owns.append(own)
        nears.append(lax.ppermute(given_next, "sp", [(1, 2), (2, 3)]))
        fars.append(lax.ppermute(given_later, "sp", [(1, 3)]))
    place = jnp.stack([lax.axis_index("dp").astype(jnp.int32), position])
    plan = tuple((mask, start) for mask, start, _ in pieces)
    columns = out_weight.shape[1] * lax.axis_size("dp")
    (out,) = kernel_call(
        functools.partial(finish_kernel, plan, heads),
        "finish",
        [place],
        [total, notes, gate, *owns, *nears, *fars, *(piece for _, _, piece in pieces)],
        [shape((tokens, columns), jnp.bfloat16)],
        2 * tokens * value.shape[1] * columns,
        24,
    )
    return out[None]


def body(queries, key_rows, values, out_gate, input_gate, forget_gate, out_weight):
    group_count = lax.axis_size("sp")
    token_count = queries.shape[1]
    head_count = input_gate.shape[1]
    copies = group_count // head_count
    head_key = queries.shape[2] // head_count
    slice_width = values.shape[2] // group_count

    def spread(source):
        widened = jnp.broadcast_to(
            source[0].reshape(token_count, head_count, 1, head_key),
            (token_count, head_count, copies, head_key),
        )
        return widened.reshape(token_count, group_count, head_key)

    def spread_gate(source):
        return jnp.repeat(source[0].T, copies, axis=1)

    query_all, key_all = (
        lax.all_to_all(spread(queries), "sp", split_axis=1, concat_axis=0, tiled=True),
        lax.all_to_all(spread(key_rows), "sp", split_axis=1, concat_axis=0, tiled=True),
    )
    value_all, input_all, forget_all = (
        lax.all_to_all(
            values[0].reshape(token_count, group_count, slice_width),
            "sp",
            split_axis=1,
            concat_axis=0,
            tiled=True,
        ),
        lax.all_to_all(spread_gate(input_gate), "sp", split_axis=1, concat_axis=0, tiled=True),
        lax.all_to_all(spread_gate(forget_gate), "sp", split_axis=1, concat_axis=0, tiled=True),
    )
    output = memory_cell(
        query_all[:, 0],
        key_all[:, 0],
        value_all[:, 0],
        input_all[:, 0].astype(jnp.float32),
        jax.nn.log_sigmoid(forget_all[:, 0].astype(jnp.float32)),
    )
    hidden = output.astype(jnp.bfloat16)
    token_rows = lax.all_to_all(hidden, "sp", split_axis=0, concat_axis=1, tiled=True)
    gated_rows = (
        token_rows.astype(jnp.float32) * jax.nn.sigmoid(out_gate[0].astype(jnp.float32))
    ).astype(jnp.bfloat16)
    projected = jnp.dot(
        gated_rows,
        lax.all_gather(out_weight, "dp", axis=1, tiled=True),
        preferred_element_type=jnp.float32,
    )
    return projected.astype(jnp.bfloat16)[None]


def solution(mesh):
    blocks = mesh.shape["sp"] == 4 and mesh.shape["dp"] == 8
    return jax.shard_map(
        block_body if blocks else body,
        mesh=mesh,
        in_specs=(
            P("dp", "sp", None),
            P("dp", "sp", None),
            P("dp", "sp", None),
            P("dp", "sp", None),
            P("dp", None, "sp"),
            P("dp", None, "sp"),
            P(None, "dp"),
        ),
        out_specs=P("dp", "sp", None),
        check_vma=False,
    )
```

```python
import functools

import jax
import jax.numpy as jnp
from jax import lax
from jax.experimental import pallas as pl
from jax.experimental.pallas import tpu as pltpu
from jax.sharding import PartitionSpec as P


BLOCK = 128


def memory_cell(query_rows, key_in, value_rows, input_log, forget_log):
    block_count = query_rows.shape[0] // BLOCK
    key_width = query_rows.shape[1]
    value_width = value_rows.shape[1]
    key_scale = key_width ** (-0.5)
    causal = lax.broadcasted_iota(jnp.int32, (BLOCK, BLOCK), 0) >= lax.broadcasted_iota(
        jnp.int32, (BLOCK, BLOCK), 1
    )
    highest = lax.Precision.HIGHEST

    def block_step(state_in, inputs):
        memory, normer, stabil = state_in
        query_part, key_part, value_part, gain_part, decay_part = inputs
        query_part = query_part.astype(jnp.float32)
        key_part = key_part.astype(jnp.float32) * key_scale
        value_part = value_part.astype(jnp.float32)
        running = jnp.cumsum(decay_part)
        log_weight = running[:, None] - running[None, :] + gain_part[None, :]
        log_weight = jnp.where(causal, log_weight, -jnp.inf)
        carried_log = running + stabil
        row_top = jnp.maximum(carried_log, jnp.max(log_weight, axis=1))
        scores = jnp.dot(query_part, key_part.T, precision=highest) * jnp.exp(
            log_weight - row_top[:, None]
        )
        carried = jnp.exp(carried_log - row_top)
        numerator = jnp.dot(scores, value_part, precision=highest) + carried[:, None] * jnp.dot(
            query_part, memory, precision=highest
        )
        denominator = jnp.sum(scores, axis=1) + carried * jnp.dot(
            query_part, normer, precision=highest
        )
        output = numerator / jnp.maximum(jnp.abs(denominator), 1.0)[:, None]
        block_end = running[-1]
        weight_log = block_end - running + gain_part
        new_top = jnp.maximum(block_end + stabil, jnp.max(weight_log))
        weights = jnp.exp(weight_log - new_top)
        retain = jnp.exp(block_end + stabil - new_top)
        memory = retain * memory + jnp.dot(
            (key_part * weights[:, None]).T, value_part, precision=highest
        )
        normer = retain * normer + jnp.dot(weights, key_part, precision=highest)
        return ((memory, normer, new_top), output)

    start_state = (
        jnp.zeros((key_width, value_width), jnp.float32),
        jnp.zeros((key_width,), jnp.float32),
        jnp.zeros((), jnp.float32),
    )
    blocks = tuple(
        (
            source.reshape((block_count, BLOCK) + source.shape[1:])
            for source in (query_rows, key_in, value_rows, input_log, forget_log)
        )
    )
    _, outputs = lax.scan(block_step, start_state, blocks)
    return outputs.reshape(block_count * BLOCK, value_width)


LANES = 128


def log_forget(gates):
    return -jnp.log1p(jnp.exp(-gates))


def running_sum(rows):
    width = rows.shape[1]
    upto = lax.broadcasted_iota(jnp.int32, (width, width), 0) <= lax.broadcasted_iota(
        jnp.int32, (width, width), 1
    )
    return jnp.dot(
        rows,
        upto.astype(jnp.float32),
        precision=lax.Precision.HIGHEST,
        preferred_element_type=jnp.float32,
    )


def times_transpose(left, right):
    return lax.dot_general(
        left, right, (((1,), (1,)), ((), ())), preferred_element_type=jnp.float32
    )


def three_terms(value):
    high = value.astype(jnp.bfloat16).astype(jnp.float32)
    middle = (value - high).astype(jnp.bfloat16).astype(jnp.float32)
    return [high, middle, value - high - middle]


def to_lanes(columns, rows):
    lane = lax.broadcasted_iota(jnp.int32, (rows, LANES), 1)
    tile = jnp.zeros((rows, LANES), jnp.float32)
    for place, column in enumerate(columns):
        tile = jnp.where(lane == place, column, tile)
    return tile


MIB = 1 << 20
COUNTS = (2, 2)
CORE, XBIT, YBIT = 1, 2, 4


def pack_kernel(heads, counts, key_ref, value_ref, input_ref, forget_ref, *refs):
    payloads, copied = refs[:-1], refs[-1]
    tokens = key_ref.shape[0]
    key_width, value_width = key_ref.shape[1] // heads, value_ref.shape[1] // heads
    copies, first = [], 0
    for place, (payload, count) in enumerate(zip(payloads, counts)):
        for part, (source, width, start) in enumerate(
            ((key_ref, key_width, 0), (value_ref, value_width, count * key_width))
        ):
            copies.append(
                pltpu.make_async_copy(
                    source.at[:, first * width : (first + count) * width],
                    payload.at[:tokens, start : start + count * width],
                    copied.at[2 * place + part],
                )
            )
        first += count
    for copy in copies:
        copy.start()
    gates = jnp.concatenate(
        [input_ref[...].astype(jnp.float32), forget_ref[...].astype(jnp.float32)], axis=0
    ).astype(jnp.bfloat16)
    for payload in payloads:
        payload[tokens:, : gates.shape[1]] = gates
        payload[tokens:, gates.shape[1] :] = jnp.zeros(
            (gates.shape[0], payload.shape[1] - gates.shape[1]), jnp.bfloat16
        )
    for copy in copies:
        copy.wait()


def gate_rows(payload, heads, tokens):
    gates = payload[tokens:, :tokens].astype(jnp.float32)
    running = running_sum(log_forget(gates[heads:]))
    return gates[:heads] - running, running[:, tokens - 1 :]


def two_term_dot(left, right):
    high = left.astype(jnp.bfloat16)
    low = (left - high.astype(jnp.float32)).astype(jnp.bfloat16)
    return jnp.dot(high, right, preferred_element_type=jnp.float32) + jnp.dot(
        low, right, preferred_element_type=jnp.float32
    )


def home_kernel(heads, first, count, block_ref, earlier_ref, here_ref, query_ref, total_ref, note_ref):
    tokens = query_ref.shape[0]
    key_width = query_ref.shape[1] // heads
    value_width = total_ref.shape[1] // count
    block = block_ref[0]
    second = lax.rem(block, 2) == 1
    level0, end0 = gate_rows(earlier_ref, heads, tokens)
    level1, _ = gate_rows(here_ref, heads, tokens)
    top0 = jnp.max(level0, axis=1, keepdims=True)
    top0 = jnp.where(block == 1, jnp.maximum(top0, 0.0), top0)
    weight0 = jnp.exp(level0 - top0)
    state = jnp.where(second, top0 + end0, jnp.where(block == 0, 0.0, -jnp.inf))
    shift = jnp.where(block == 3, end0, 0.0)
    causal = lax.broadcasted_iota(jnp.int32, (tokens, tokens), 0) >= lax.broadcasted_iota(
        jnp.int32, (tokens, tokens), 1
    )
    key_scale = key_width ** (-0.5)
    notes = []
    for place in range(count):
        head = first + place
        pick = slice(head, head + 1)
        keys = slice(place * key_width, (place + 1) * key_width)
        start = count * key_width + place * value_width
        channels = slice(start, start + value_width)
        rows = query_ref[:, head * key_width : (head + 1) * key_width]
        masked = jnp.where(causal, level1[pick], -jnp.inf)
        top = jnp.maximum(jnp.max(masked, axis=1, keepdims=True), state[pick])
        scores1 = times_transpose(rows, here_ref[:tokens, keys]) * key_scale
        scores1 = scores1 * jnp.exp(masked - top)
        scale0 = jnp.where(second, jnp.exp(state[pick] - top), 0.0)
        scores0 = times_transpose(rows, earlier_ref[:tokens, keys]) * key_scale
        scores0 = scores0 * weight0[pick] * scale0
        sums = jnp.sum(scores0 + scores1, axis=1, keepdims=True)
        total_ref[:, place * value_width : (place + 1) * value_width] = two_term_dot(
            scores1, here_ref[:tokens, channels]
        ) + two_term_dot(scores0, earlier_ref[:tokens, channels])
        notes += [sums, top, shift[pick]]
    note_ref[...] = to_lanes(notes, tokens)


def serve_kernel(
    heads, first, count, earlier_ref, here_ref, near_ref, far_ref, next_ref, later_ref
):
    tokens = near_ref.shape[0]
    key_width = near_ref.shape[1] // heads
    value_width = (next_ref.shape[1] - LANES) // count
    level0, end0 = gate_rows(earlier_ref, heads, tokens)
    level1, end1 = gate_rows(here_ref, heads, tokens)
    level = jnp.concatenate([level0, level1 - end0], axis=1)
    top = jnp.maximum(jnp.max(level, axis=1, keepdims=True), 0.0)
    weight = jnp.exp(level - top) * (key_width ** (-0.5))
    reach = top + end0 + end1
    next_notes, later_notes = [], []
    for place in range(count):
        head = first + place
        pick = slice(head, head + 1)
        columns = slice(head * key_width, (head + 1) * key_width)
        keys = slice(place * key_width, (place + 1) * key_width)
        start = count * key_width + place * value_width
        channels = slice(start, start + value_width)
        out = slice(place * value_width, (place + 1) * value_width)
        key_both = jnp.concatenate([earlier_ref[:tokens, keys], here_ref[:tokens, keys]], axis=0)
        value_both = jnp.concatenate(
            [earlier_ref[:tokens, channels], here_ref[:tokens, channels]], axis=0
        )
        rows = jnp.concatenate([near_ref[:, columns], far_ref[:, columns]], axis=0)
        scores = times_transpose(rows, key_both) * weight[pick]
        sums = jnp.sum(scores, axis=1, keepdims=True)
        given = jnp.dot(
            scores.astype(jnp.bfloat16), value_both, preferred_element_type=jnp.float32
        ).astype(jnp.bfloat16)
        next_ref[:, out] = given[:tokens]
        later_ref[:, out] = given[tokens:]
        next_notes += three_terms(sums[:tokens]) + three_terms(reach[pick])
        later_notes += three_terms(sums[tokens:]) + three_terms(reach[pick])
    next_ref[:, count * value_width :] = to_lanes(next_notes, tokens).astype(jnp.bfloat16)
    later_ref[:, count * value_width :] = to_lanes(later_notes, tokens).astype(jnp.bfloat16)


def finish_kernel(plan, counts, place_ref, *refs):
    chunks, heads, size = len(counts), sum(counts), 1 + 4 * len(counts) + len(plan)
    out_ref, held, copied = refs[size], refs[size + 1 : -1], refs[-1]
    copies = [
        pltpu.make_async_copy(source, target, copied.at[i])
        for i, (source, target) in enumerate(zip(refs[:size], held))
    ]
    for copy in copies:
        copy.start()
    for copy in copies[: 1 + 4 * chunks]:
        copy.wait()
    gate_ref, parts, pieces = held[0], held[1 : 1 + 4 * chunks], held[1 + 4 * chunks :]
    totals, notes, nears, fars = (parts[i * chunks : (i + 1) * chunks] for i in range(4))
    value_width = gate_ref.shape[1] // heads
    given = place_ref[1] >= 2
    gated = []
    for chunk, count in enumerate(counts):
        tail = slice(count * value_width, count * value_width + LANES)
        near, far = nears[chunk], fars[chunk]
        lanes = near[:, tail].astype(jnp.float32) + far[:, tail].astype(jnp.float32)
        own = notes[chunk][...]
        for place in range(count):
            out = slice(place * value_width, (place + 1) * value_width)
            start = len(gated) * value_width
            at = 6 * place
            sums = lanes[:, at : at + 1] + lanes[:, at + 1 : at + 2] + lanes[:, at + 2 : at + 3]
            at += 3
            reach = lanes[:, at : at + 1] + lanes[:, at + 1 : at + 2] + lanes[:, at + 2 : at + 3]
            reach = reach + own[:, 3 * place + 2 : 3 * place + 3]
            top = own[:, 3 * place + 1 : 3 * place + 2]
            peak = jnp.where(given, jnp.maximum(top, reach), top)
            scale = jnp.exp(top - peak)
            scale_given = jnp.where(given, jnp.exp(reach - peak), 0.0)
            weight = scale * own[:, 3 * place : 3 * place + 1] + scale_given * sums
            inverse = 1.0 / jnp.maximum(jnp.abs(weight), 1.0)
            message = near[:, out].astype(jnp.float32) + far[:, out].astype(jnp.float32)
            cell = (scale * inverse) * totals[chunk][:, out] + (scale_given * inverse) * message
            hidden = cell.astype(jnp.bfloat16).astype(jnp.float32)
            gate = jax.nn.sigmoid(gate_ref[:, start : start + value_width].astype(jnp.float32))
            gated.append((hidden * gate).astype(jnp.bfloat16))
    gated = jnp.concatenate(gated, axis=1)
    sums = {}
    for (mask, start), piece, copy in zip(plan, pieces, copies[1 + 4 * chunks :]):
        copy.wait()
        part = jnp.dot(
            gated[:, start : start + piece.shape[0]], piece[...], preferred_element_type=jnp.float32
        )
        sums[mask] = sums[mask] + part if mask in sums else part
    width = pieces[0].shape[1]
    for mask, total in sums.items():
        start = pl.multiple_of((place_ref[0] ^ mask) * width, width)
        out_ref[:, pl.ds(start, width)] = total.astype(out_ref.dtype)


def kernel_call(kernel, scalars, operands, outs, flops, limit, spaces=(), scratch=()):
    vmem = pl.BlockSpec(memory_space=pltpu.VMEM)
    size = sum(x.size * x.dtype.itemsize for x in operands + outs)
    specs = [pl.BlockSpec(memory_space=pltpu.SMEM)] * len(scalars) + list(spaces)
    specs += [vmem] * (len(operands) - len(spaces))
    return pl.pallas_call(
        kernel,
        out_shape=outs,
        in_specs=specs,
        out_specs=[vmem] * len(outs),
        scratch_shapes=scratch,
        compiler_params=pltpu.CompilerParams(vmem_limit_bytes=limit * MIB),
        cost_estimate=pl.CostEstimate(flops=flops, bytes_accessed=size, transcendentals=0),
    )(*scalars, *operands)


def block_body(queries, key_rows, values, out_gate, input_gate, forget_gate, out_weight):
    return block_steps(
        queries[0], key_rows[0], values[0], out_gate[0], input_gate[0], forget_gate[0], out_weight
    )[None]


def block_steps(query, key, value, gate, input_log, forget, out_weight):
    tokens, heads = query.shape[0], input_log.shape[0]
    key_width, value_width = query.shape[1] // heads, value.shape[1] // heads
    block = lax.axis_index("sp").astype(jnp.int32)
    shape = jax.ShapeDtypeStruct
    far_memory = pl.BlockSpec(memory_space=pltpu.HBM)
    device_count = lax.axis_size("dp")

    def swap(piece, bit):
        return lax.ppermute(piece, "dp", [(i, i ^ bit) for i in range(device_count)])

    near = lax.ppermute(query, "sp", [(2, 1)])
    far = lax.ppermute(query, "sp", [(3, 1)])
    payloads = kernel_call(
        functools.partial(pack_kernel, heads, COUNTS),
        [],
        [key, value, input_log, forget],
        [
            shape((tokens + 2 * heads, count * (key_width + value_width)), jnp.bfloat16)
            for count in COUNTS
        ],
        0,
        60,
        [far_memory] * 2,
        [pltpu.SemaphoreType.DMA((2 * len(COUNTS),))],
    )
    earlier = [lax.ppermute(payload, "sp", [(0, 1), (2, 3)]) for payload in payloads]

    half = out_weight.shape[0] // 2
    from_x = swap(out_weight, XBIT)
    from_y = swap(out_weight, YBIT)
    from_core = swap(out_weight, CORE)
    top = swap(from_x[:half], YBIT)
    bottom = swap(from_y[half:], XBIT)
    pieces = [
        (0, 0, out_weight),
        (CORE, 0, from_core),
        (XBIT, 0, from_x),
        (XBIT | CORE, 0, swap(from_x, CORE)),
        (YBIT, 0, from_y),
        (YBIT | CORE, 0, swap(from_y, CORE)),
        (XBIT | YBIT, 0, top),
        (XBIT | YBIT, half, bottom),
        (XBIT | YBIT | CORE, 0, swap(top, CORE)),
        (XBIT | YBIT | CORE, half, swap(bottom, CORE)),
    ]

    totals, notes, nears, fars = [], [], [], []
    first = 0
    for chunk, count in enumerate(COUNTS):
        work = 2 * count * tokens * tokens * (key_width + value_width)
        message = shape((tokens, count * value_width + LANES), jnp.bfloat16)
        given_next, given_later = kernel_call(
            functools.partial(serve_kernel, heads, first, count),
            [],
            [earlier[chunk], payloads[chunk], near, far],
            [message] * 2,
            4 * work,
            8,
        )
        nears.append(lax.ppermute(given_next, "sp", [(1, 2)]))
        fars.append(lax.ppermute(given_later, "sp", [(1, 3)]))
        total, note = kernel_call(
            functools.partial(home_kernel, heads, first, count),
            [block.reshape(1)],
            [earlier[chunk], payloads[chunk], query],
            [shape((tokens, count * value_width), jnp.float32), shape((tokens, LANES), jnp.float32)],
            3 * work,
            8,
        )
        totals.append(total)
        notes.append(note)
        first += count
    place = jnp.stack([lax.axis_index("dp").astype(jnp.int32), block])
    columns = out_weight.shape[1] * device_count
    operands = [gate, *totals, *notes, *nears, *fars, *(piece for _, _, piece in pieces)]
    (out,) = kernel_call(
        functools.partial(finish_kernel, tuple((mask, start) for mask, start, _ in pieces), COUNTS),
        [place],
        operands,
        [shape((tokens, columns), jnp.bfloat16)],
        2 * tokens * value.shape[1] * columns,
        60,
        [far_memory] * len(operands),
        [pltpu.VMEM(x.shape, x.dtype) for x in operands]
        + [pltpu.SemaphoreType.DMA((len(operands),))],
    )
    return out


def body(queries, key_rows, values, out_gate, input_gate, forget_gate, out_weight):
    group_count = lax.axis_size("sp")
    token_count = queries.shape[1]
    head_count = input_gate.shape[1]
    copies = group_count // head_count
    head_key = queries.shape[2] // head_count
    slice_width = values.shape[2] // group_count

    def spread(source):
        widened = jnp.broadcast_to(
            source[0].reshape(token_count, head_count, 1, head_key),
            (token_count, head_count, copies, head_key),
        )
        return widened.reshape(token_count, group_count, head_key)

    def spread_gate(source):
        return jnp.repeat(source[0].T, copies, axis=1)

    query_all, key_all = (
        lax.all_to_all(spread(queries), "sp", split_axis=1, concat_axis=0, tiled=True),
        lax.all_to_all(spread(key_rows), "sp", split_axis=1, concat_axis=0, tiled=True),
    )
    value_all, input_all, forget_all = (
        lax.all_to_all(
            values[0].reshape(token_count, group_count, slice_width),
            "sp",
            split_axis=1,
            concat_axis=0,
            tiled=True,
        ),
        lax.all_to_all(spread_gate(input_gate), "sp", split_axis=1, concat_axis=0, tiled=True),
        lax.all_to_all(spread_gate(forget_gate), "sp", split_axis=1, concat_axis=0, tiled=True),
    )
    output = memory_cell(
        query_all[:, 0],
        key_all[:, 0],
        value_all[:, 0],
        input_all[:, 0].astype(jnp.float32),
        jax.nn.log_sigmoid(forget_all[:, 0].astype(jnp.float32)),
    )
    hidden = output.astype(jnp.bfloat16)
    token_rows = lax.all_to_all(hidden, "sp", split_axis=0, concat_axis=1, tiled=True)
    gated_rows = (
        token_rows.astype(jnp.float32) * jax.nn.sigmoid(out_gate[0].astype(jnp.float32))
    ).astype(jnp.bfloat16)
    projected = jnp.dot(
        gated_rows,
        lax.all_gather(out_weight, "dp", axis=1, tiled=True),
        preferred_element_type=jnp.float32,
    )
    return projected.astype(jnp.bfloat16)[None]


def solution(mesh):
    blocks = mesh.shape["sp"] == 4 and mesh.shape["dp"] == 8
    return jax.shard_map(
        block_body if blocks else body,
        mesh=mesh,
        in_specs=(
            P("dp", "sp", None),
            P("dp", "sp", None),
            P("dp", "sp", None),
            P("dp", "sp", None),
            P("dp", None, "sp"),
            P("dp", None, "sp"),
            P(None, "dp"),
        ),
        out_specs=P("dp", "sp", None),
        check_vma=False,
    )
```

```python
import functools

import jax
import jax.numpy as jnp
from jax import lax
from jax.experimental import pallas as pl
from jax.experimental.pallas import tpu as pltpu
from jax.sharding import PartitionSpec as P


BLOCK = 128


def memory_cell(query_rows, key_in, value_rows, input_log, forget_log):
    block_count = query_rows.shape[0] // BLOCK
    key_width = query_rows.shape[1]
    value_width = value_rows.shape[1]
    key_scale = key_width ** (-0.5)
    causal = lax.broadcasted_iota(jnp.int32, (BLOCK, BLOCK), 0) >= lax.broadcasted_iota(
        jnp.int32, (BLOCK, BLOCK), 1
    )
    highest = lax.Precision.HIGHEST

    def block_step(state_in, inputs):
        memory, normer, stabil = state_in
        query_part, key_part, value_part, gain_part, decay_part = inputs
        query_part = query_part.astype(jnp.float32)
        key_part = key_part.astype(jnp.float32) * key_scale
        value_part = value_part.astype(jnp.float32)
        running = jnp.cumsum(decay_part)
        log_weight = running[:, None] - running[None, :] + gain_part[None, :]
        log_weight = jnp.where(causal, log_weight, -jnp.inf)
        carried_log = running + stabil
        row_top = jnp.maximum(carried_log, jnp.max(log_weight, axis=1))
        scores = jnp.dot(query_part, key_part.T, precision=highest) * jnp.exp(
            log_weight - row_top[:, None]
        )
        carried = jnp.exp(carried_log - row_top)
        numerator = jnp.dot(scores, value_part, precision=highest) + carried[:, None] * jnp.dot(
            query_part, memory, precision=highest
        )
        denominator = jnp.sum(scores, axis=1) + carried * jnp.dot(
            query_part, normer, precision=highest
        )
        output = numerator / jnp.maximum(jnp.abs(denominator), 1.0)[:, None]
        block_end = running[-1]
        weight_log = block_end - running + gain_part
        new_top = jnp.maximum(block_end + stabil, jnp.max(weight_log))
        weights = jnp.exp(weight_log - new_top)
        retain = jnp.exp(block_end + stabil - new_top)
        memory = retain * memory + jnp.dot(
            (key_part * weights[:, None]).T, value_part, precision=highest
        )
        normer = retain * normer + jnp.dot(weights, key_part, precision=highest)
        return ((memory, normer, new_top), output)

    start_state = (
        jnp.zeros((key_width, value_width), jnp.float32),
        jnp.zeros((key_width,), jnp.float32),
        jnp.zeros((), jnp.float32),
    )
    blocks = tuple(
        (
            source.reshape((block_count, BLOCK) + source.shape[1:])
            for source in (query_rows, key_in, value_rows, input_log, forget_log)
        )
    )
    _, outputs = lax.scan(block_step, start_state, blocks)
    return outputs.reshape(block_count * BLOCK, value_width)


LANES = 128


def log_forget(gates):
    return -jnp.log1p(jnp.exp(-gates))


def running_sum(rows):
    width = rows.shape[1]
    upto = lax.broadcasted_iota(jnp.int32, (width, width), 0) <= lax.broadcasted_iota(
        jnp.int32, (width, width), 1
    )
    return jnp.dot(
        rows,
        upto.astype(jnp.float32),
        precision=lax.Precision.HIGHEST,
        preferred_element_type=jnp.float32,
    )


def times_transpose(left, right):
    return lax.dot_general(
        left, right, (((1,), (1,)), ((), ())), preferred_element_type=jnp.float32
    )


def three_terms(value):
    high = value.astype(jnp.bfloat16).astype(jnp.float32)
    middle = (value - high).astype(jnp.bfloat16).astype(jnp.float32)
    return [high, middle, value - high - middle]


def to_lanes(columns, rows):
    lane = lax.broadcasted_iota(jnp.int32, (rows, LANES), 1)
    tile = jnp.zeros((rows, LANES), jnp.float32)
    for place, column in enumerate(columns):
        tile = jnp.where(lane == place, column, tile)
    return tile


MIB = 1 << 20
COUNTS = (2, 2)
CORE, XBIT, YBIT = 1, 2, 4


def gates_kernel(input_ref, forget_ref, out_ref):
    running = running_sum(log_forget(forget_ref[...].astype(jnp.float32)))
    heads, tokens = running.shape
    level = input_ref[...].astype(jnp.float32) - running
    decay = jnp.broadcast_to(running[:, tokens - 1 :], (heads, tokens))
    out_ref[...] = jnp.concatenate([level, decay], axis=0)


def levels(ref):
    heads = ref.shape[0] // 2
    return ref[:heads, :], ref[heads:, :1]


def two_term_dot(left, right):
    high = left.astype(jnp.bfloat16)
    low = (left - high.astype(jnp.float32)).astype(jnp.bfloat16)
    return jnp.dot(high, right, preferred_element_type=jnp.float32) + jnp.dot(
        low, right, preferred_element_type=jnp.float32
    )


def own_kernel(counts, gates_ref, key_ref, value_ref, query_ref, *outs):
    heads = sum(counts)
    tokens = query_ref.shape[0]
    key_width, value_width = query_ref.shape[1] // heads, value_ref.shape[1] // heads
    level, _ = levels(gates_ref)
    causal = lax.broadcasted_iota(jnp.int32, (tokens, tokens), 0) >= lax.broadcasted_iota(
        jnp.int32, (tokens, tokens), 1
    )
    key_scale = key_width ** (-0.5)
    first = 0
    for total_ref, note_ref, count in zip(outs[::2], outs[1::2], counts):
        notes = []
        for head in range(first, first + count):
            keys = slice(head * key_width, (head + 1) * key_width)
            channels = slice(head * value_width, (head + 1) * value_width)
            out = slice((head - first) * value_width, (head - first + 1) * value_width)
            masked = jnp.where(causal, level[head : head + 1], -jnp.inf)
            top = jnp.max(masked, axis=1, keepdims=True)
            scores = times_transpose(query_ref[:, keys], key_ref[:, keys]) * key_scale
            scores = scores * jnp.exp(masked - top)
            total_ref[:, out] = two_term_dot(scores, value_ref[:, channels])
            notes += [jnp.sum(scores, axis=1, keepdims=True), top]
        note_ref[...] = to_lanes(notes, tokens)
        first += count


def join_kernel(counts, gates0_ref, key0_ref, value0_ref, query_ref, *refs):
    chunks, heads = len(counts), sum(counts)
    tokens = query_ref.shape[0]
    key_width, value_width = query_ref.shape[1] // heads, value0_ref.shape[1] // heads
    block = lax.axis_index("sp")
    second = lax.rem(block, 2) == 1
    level0, end0 = levels(gates0_ref)
    top0 = jnp.max(level0, axis=1, keepdims=True)
    top0 = jnp.where(block == 1, jnp.maximum(top0, 0.0), top0)
    weight0 = jnp.exp(level0 - top0) * (key_width ** (-0.5))
    state = jnp.where(second, top0 + end0, jnp.where(block == 0, 0.0, -jnp.inf))
    shift = jnp.where(block == 3, end0, 0.0)
    first = 0
    for chunk, count in enumerate(counts):
        own_total, own_note, total_ref, note_ref = refs[chunk * 2 : chunk * 2 + 2] + refs[
            (chunks + chunk) * 2 : (chunks + chunk) * 2 + 2
        ]
        own = own_note[...]
        notes = []
        for head in range(first, first + count):
            pick = slice(head, head + 1)
            keys = slice(head * key_width, (head + 1) * key_width)
            channels = slice(head * value_width, (head + 1) * value_width)
            place = head - first
            out = slice(place * value_width, (place + 1) * value_width)
            own_top = own[:, 2 * place + 1 : 2 * place + 2]
            top = jnp.maximum(own_top, state[pick])
            scale = jnp.exp(own_top - top)
            scale0 = jnp.where(second, jnp.exp(state[pick] - top), 0.0)
            scores = times_transpose(query_ref[:, keys], key0_ref[:, keys])
            scores = scores * weight0[pick] * scale0
            total_ref[:, out] = scale * own_total[:, out] + two_term_dot(
                scores, value0_ref[:, channels]
            )
            sums = scale * own[:, 2 * place : 2 * place + 1] + jnp.sum(
                scores, axis=1, keepdims=True
            )
            notes += [sums, top, shift[pick]]
        note_ref[...] = to_lanes(notes, tokens)
        first += count


def serve_kernel(
    heads, first, count, gates0_ref, key0_ref, value0_ref, gates_ref, key_ref, value_ref,
    near_ref, far_ref, next_ref, later_ref,
):
    tokens = near_ref.shape[0]
    key_width, value_width = near_ref.shape[1] // heads, value_ref.shape[1] // heads
    level0, end0 = levels(gates0_ref)
    level1, end1 = levels(gates_ref)
    level = jnp.concatenate([level0, level1 - end0], axis=1)
    top = jnp.maximum(jnp.max(level, axis=1, keepdims=True), 0.0)
    weight = jnp.exp(level - top) * (key_width ** (-0.5))
    reach = top + end0 + end1
    next_notes, later_notes = [], []
    for head in range(first, first + count):
        pick = slice(head, head + 1)
        keys = slice(head * key_width, (head + 1) * key_width)
        channels = slice(head * value_width, (head + 1) * value_width)
        out = slice((head - first) * value_width, (head - first + 1) * value_width)
        key_both = jnp.concatenate([key0_ref[:, keys], key_ref[:, keys]], axis=0)
        value_both = jnp.concatenate([value0_ref[:, channels], value_ref[:, channels]], axis=0)
        rows = jnp.concatenate([near_ref[:, keys], far_ref[:, keys]], axis=0)
        scores = times_transpose(rows, key_both) * weight[pick]
        sums = jnp.sum(scores, axis=1, keepdims=True)
        given = jnp.dot(
            scores.astype(jnp.bfloat16), value_both, preferred_element_type=jnp.float32
        ).astype(jnp.bfloat16)
        next_ref[:, out] = given[:tokens]
        later_ref[:, out] = given[tokens:]
        next_notes += three_terms(sums[:tokens]) + three_terms(reach[pick])
        later_notes += three_terms(sums[tokens:]) + three_terms(reach[pick])
    next_ref[:, count * value_width :] = to_lanes(next_notes, tokens).astype(jnp.bfloat16)
    later_ref[:, count * value_width :] = to_lanes(later_notes, tokens).astype(jnp.bfloat16)


def finish_kernel(plan, counts, gate_ref, *refs):
    chunks, heads, out_ref = len(counts), sum(counts), refs[-1]
    totals, notes, nears, fars = (refs[i * chunks : (i + 1) * chunks] for i in range(4))
    pieces = refs[4 * chunks : -1]
    value_width = gate_ref.shape[1] // heads
    given = lax.axis_index("sp") >= 2
    gated = []
    for chunk, count in enumerate(counts):
        tail = slice(count * value_width, count * value_width + LANES)
        near, far = nears[chunk], fars[chunk]
        lanes = near[:, tail].astype(jnp.float32) + far[:, tail].astype(jnp.float32)
        own = notes[chunk][...]
        for place in range(count):
            out = slice(place * value_width, (place + 1) * value_width)
            start = len(gated) * value_width
            at = 6 * place
            sums = lanes[:, at : at + 1] + lanes[:, at + 1 : at + 2] + lanes[:, at + 2 : at + 3]
            at += 3
            reach = lanes[:, at : at + 1] + lanes[:, at + 1 : at + 2] + lanes[:, at + 2 : at + 3]
            reach = reach + own[:, 3 * place + 2 : 3 * place + 3]
            top = own[:, 3 * place + 1 : 3 * place + 2]
            peak = jnp.where(given, jnp.maximum(top, reach), top)
            scale = jnp.exp(top - peak)
            scale_given = jnp.where(given, jnp.exp(reach - peak), 0.0)
            weight = scale * own[:, 3 * place : 3 * place + 1] + scale_given * sums
            inverse = 1.0 / jnp.maximum(jnp.abs(weight), 1.0)
            message = near[:, out].astype(jnp.float32) + far[:, out].astype(jnp.float32)
            cell = (scale * inverse) * totals[chunk][:, out] + (scale_given * inverse) * message
            hidden = cell.astype(jnp.bfloat16).astype(jnp.float32)
            gate = jax.nn.sigmoid(gate_ref[:, start : start + value_width].astype(jnp.float32))
            gated.append((hidden * gate).astype(jnp.bfloat16))
    gated = jnp.concatenate(gated, axis=1)
    sums = {}
    for (mask, start), piece in zip(plan, pieces):
        part = jnp.dot(
            gated[:, start : start + piece.shape[0]], piece[...], preferred_element_type=jnp.float32
        )
        sums[mask] = sums[mask] + part if mask in sums else part
    width, device = pieces[0].shape[1], lax.axis_index("dp")
    for mask, total in sums.items():
        start = pl.multiple_of((device ^ mask) * width, width)
        out_ref[:, pl.ds(start, width)] = total.astype(out_ref.dtype)


def kernel_call(kernel, operands, outs, flops, limit):
    vmem = pl.BlockSpec(memory_space=pltpu.VMEM)
    size = sum(x.size * x.dtype.itemsize for x in (*operands, *outs))
    return pl.pallas_call(
        kernel,
        out_shape=outs,
        in_specs=[vmem] * len(operands),
        out_specs=[vmem] * len(outs),
        compiler_params=pltpu.CompilerParams(vmem_limit_bytes=limit * MIB),
        cost_estimate=pl.CostEstimate(flops=flops, bytes_accessed=size, transcendentals=0),
    )(*operands)


def block_body(queries, key_rows, values, out_gate, input_gate, forget_gate, out_weight):
    return block_steps(
        queries[0], key_rows[0], values[0], out_gate[0], input_gate[0], forget_gate[0], out_weight
    )[None]


def block_steps(query, key, value, gate, input_log, forget, out_weight):
    tokens, heads = query.shape[0], input_log.shape[0]
    key_width, value_width = query.shape[1] // heads, value.shape[1] // heads
    shape = jax.ShapeDtypeStruct
    device_count = lax.axis_size("dp")

    def swap(piece, bit):
        return lax.ppermute(piece, "dp", [(i, i ^ bit) for i in range(device_count)])

    (gates,) = kernel_call(
        gates_kernel, [input_log, forget], [shape((2 * heads, tokens), jnp.float32)], 0, 2
    )
    pair = [(0, 1), (2, 3)]
    earlier = [
        lax.ppermute(gates, "sp", pair),
        lax.ppermute(key, "sp", pair),
        lax.ppermute(value, "sp", pair),
    ]
    here = [gates, key, value]
    near = lax.ppermute(query, "sp", [(2, 1)])
    far = lax.ppermute(query, "sp", [(3, 1)])

    half = out_weight.shape[0] // 2
    from_x = swap(out_weight, XBIT)
    from_y = swap(out_weight, YBIT)
    from_core = swap(out_weight, CORE)
    top = swap(from_x[:half], YBIT)
    bottom = swap(from_y[half:], XBIT)
    pieces = [
        (0, 0, out_weight),
        (CORE, 0, from_core),
        (XBIT, 0, from_x),
        (XBIT | CORE, 0, swap(from_x, CORE)),
        (YBIT, 0, from_y),
        (YBIT | CORE, 0, swap(from_y, CORE)),
        (XBIT | YBIT, 0, top),
        (XBIT | YBIT, half, bottom),
        (XBIT | YBIT | CORE, 0, swap(top, CORE)),
        (XBIT | YBIT | CORE, half, swap(bottom, CORE)),
    ]

    work = 2 * tokens * tokens * (key_width + value_width)
    sums = [
        x
        for count in COUNTS
        for x in (
            shape((tokens, count * value_width), jnp.float32),
            shape((tokens, LANES), jnp.float32),
        )
    ]
    own = kernel_call(
        functools.partial(own_kernel, COUNTS), [*here, query], sums, 3 * heads * work // 2, 8
    )
    nears, fars = [], []
    first = 0
    for count in COUNTS:
        message = shape((tokens, count * value_width + LANES), jnp.bfloat16)
        given_next, given_later = kernel_call(
            functools.partial(serve_kernel, heads, first, count),
            [*earlier, *here, near, far],
            [message] * 2,
            4 * count * work,
            8,
        )
        nears.append(lax.ppermute(given_next, "sp", [(1, 2)]))
        fars.append(lax.ppermute(given_later, "sp", [(1, 3)]))
        first += count
    home = kernel_call(
        functools.partial(join_kernel, COUNTS),
        [*earlier, query, *own],
        sums,
        3 * heads * work // 2,
        8,
    )
    columns = out_weight.shape[1] * device_count
    (out,) = kernel_call(
        functools.partial(finish_kernel, tuple((mask, start) for mask, start, _ in pieces), COUNTS),
        [gate, *home[::2], *home[1::2], *nears, *fars, *(piece for _, _, piece in pieces)],
        [shape((tokens, columns), jnp.bfloat16)],
        2 * tokens * value.shape[1] * columns,
        16,
    )
    return out


def body(queries, key_rows, values, out_gate, input_gate, forget_gate, out_weight):
    group_count = lax.axis_size("sp")
    token_count = queries.shape[1]
    head_count = input_gate.shape[1]
    copies = group_count // head_count
    head_key = queries.shape[2] // head_count
    slice_width = values.shape[2] // group_count

    def spread(source):
        widened = jnp.broadcast_to(
            source[0].reshape(token_count, head_count, 1, head_key),
            (token_count, head_count, copies, head_key),
        )
        return widened.reshape(token_count, group_count, head_key)

    def spread_gate(source):
        return jnp.repeat(source[0].T, copies, axis=1)

    query_all, key_all = (
        lax.all_to_all(spread(queries), "sp", split_axis=1, concat_axis=0, tiled=True),
        lax.all_to_all(spread(key_rows), "sp", split_axis=1, concat_axis=0, tiled=True),
    )
    value_all, input_all, forget_all = (
        lax.all_to_all(
            values[0].reshape(token_count, group_count, slice_width),
            "sp",
            split_axis=1,
            concat_axis=0,
            tiled=True,
        ),
        lax.all_to_all(spread_gate(input_gate), "sp", split_axis=1, concat_axis=0, tiled=True),
        lax.all_to_all(spread_gate(forget_gate), "sp", split_axis=1, concat_axis=0, tiled=True),
    )
    output = memory_cell(
        query_all[:, 0],
        key_all[:, 0],
        value_all[:, 0],
        input_all[:, 0].astype(jnp.float32),
        jax.nn.log_sigmoid(forget_all[:, 0].astype(jnp.float32)),
    )
    hidden = output.astype(jnp.bfloat16)
    token_rows = lax.all_to_all(hidden, "sp", split_axis=0, concat_axis=1, tiled=True)
    gated_rows = (
        token_rows.astype(jnp.float32) * jax.nn.sigmoid(out_gate[0].astype(jnp.float32))
    ).astype(jnp.bfloat16)
    projected = jnp.dot(
        gated_rows,
        lax.all_gather(out_weight, "dp", axis=1, tiled=True),
        preferred_element_type=jnp.float32,
    )
    return projected.astype(jnp.bfloat16)[None]


def solution(mesh):
    blocks = mesh.shape["sp"] == 4 and mesh.shape["dp"] == 8
    return jax.shard_map(
        block_body if blocks else body,
        mesh=mesh,
        in_specs=(
            P("dp", "sp", None),
            P("dp", "sp", None),
            P("dp", "sp", None),
            P("dp", "sp", None),
            P("dp", None, "sp"),
            P("dp", None, "sp"),
            P(None, "dp"),
        ),
        out_specs=P("dp", "sp", None),
        check_vma=False,
    )
```

```python
import functools

import jax
import jax.numpy as jnp
from jax import lax
from jax.experimental import pallas as pl
from jax.experimental.pallas import tpu as pltpu
from jax.sharding import PartitionSpec as P


BLOCK = 128


def memory_cell(query_rows, key_in, value_rows, input_log, forget_log):
    block_count = query_rows.shape[0] // BLOCK
    key_width = query_rows.shape[1]
    value_width = value_rows.shape[1]
    key_scale = key_width ** (-0.5)
    causal = lax.broadcasted_iota(jnp.int32, (BLOCK, BLOCK), 0) >= lax.broadcasted_iota(
        jnp.int32, (BLOCK, BLOCK), 1
    )
    highest = lax.Precision.HIGHEST

    def block_step(state_in, inputs):
        memory, normer, stabil = state_in
        query_part, key_part, value_part, gain_part, decay_part = inputs
        query_part = query_part.astype(jnp.float32)
        key_part = key_part.astype(jnp.float32) * key_scale
        value_part = value_part.astype(jnp.float32)
        running = jnp.cumsum(decay_part)
        log_weight = running[:, None] - running[None, :] + gain_part[None, :]
        log_weight = jnp.where(causal, log_weight, -jnp.inf)
        carried_log = running + stabil
        row_top = jnp.maximum(carried_log, jnp.max(log_weight, axis=1))
        scores = jnp.dot(query_part, key_part.T, precision=highest) * jnp.exp(
            log_weight - row_top[:, None]
        )
        carried = jnp.exp(carried_log - row_top)
        numerator = jnp.dot(scores, value_part, precision=highest) + carried[:, None] * jnp.dot(
            query_part, memory, precision=highest
        )
        denominator = jnp.sum(scores, axis=1) + carried * jnp.dot(
            query_part, normer, precision=highest
        )
        output = numerator / jnp.maximum(jnp.abs(denominator), 1.0)[:, None]
        block_end = running[-1]
        weight_log = block_end - running + gain_part
        new_top = jnp.maximum(block_end + stabil, jnp.max(weight_log))
        weights = jnp.exp(weight_log - new_top)
        retain = jnp.exp(block_end + stabil - new_top)
        memory = retain * memory + jnp.dot(
            (key_part * weights[:, None]).T, value_part, precision=highest
        )
        normer = retain * normer + jnp.dot(weights, key_part, precision=highest)
        return ((memory, normer, new_top), output)

    start_state = (
        jnp.zeros((key_width, value_width), jnp.float32),
        jnp.zeros((key_width,), jnp.float32),
        jnp.zeros((), jnp.float32),
    )
    blocks = tuple(
        (
            source.reshape((block_count, BLOCK) + source.shape[1:])
            for source in (query_rows, key_in, value_rows, input_log, forget_log)
        )
    )
    _, outputs = lax.scan(block_step, start_state, blocks)
    return outputs.reshape(block_count * BLOCK, value_width)


LANES = 128


def log_forget(gates):
    return -jnp.log1p(jnp.exp(-gates))


def running_sum(rows):
    width = rows.shape[1]
    upto = lax.broadcasted_iota(jnp.int32, (width, width), 0) <= lax.broadcasted_iota(
        jnp.int32, (width, width), 1
    )
    return jnp.dot(
        rows,
        upto.astype(jnp.float32),
        precision=lax.Precision.HIGHEST,
        preferred_element_type=jnp.float32,
    )


def times_transpose(left, right):
    return lax.dot_general(
        left, right, (((1,), (1,)), ((), ())), preferred_element_type=jnp.float32
    )


def three_terms(value):
    high = value.astype(jnp.bfloat16).astype(jnp.float32)
    middle = (value - high).astype(jnp.bfloat16).astype(jnp.float32)
    return [high, middle, value - high - middle]


def to_lanes(columns, rows):
    lane = lax.broadcasted_iota(jnp.int32, (rows, LANES), 1)
    tile = jnp.zeros((rows, LANES), jnp.float32)
    for place, column in enumerate(columns):
        tile = jnp.where(lane == place, column, tile)
    return tile


MIB = 1 << 20
COUNTS = (2, 2)
CORE, XBIT, YBIT = 1, 2, 4


def gates_kernel(input_ref, forget_ref, out_ref):
    running = running_sum(log_forget(forget_ref[...].astype(jnp.float32)))
    heads, tokens = running.shape
    level = input_ref[...].astype(jnp.float32) - running
    decay = jnp.broadcast_to(running[:, tokens - 1 :], (heads, tokens))
    out_ref[...] = jnp.concatenate([level, decay], axis=0)


def levels(ref):
    heads = ref.shape[0] // 2
    return ref[:heads, :], ref[heads:, :1]


def two_term_dot(left, right):
    high = left.astype(jnp.bfloat16)
    low = (left - high.astype(jnp.float32)).astype(jnp.bfloat16)
    return jnp.dot(high, right, preferred_element_type=jnp.float32) + jnp.dot(
        low, right, preferred_element_type=jnp.float32
    )


def own_kernel(counts, gates_ref, key_ref, value_ref, query_ref, *outs):
    heads = sum(counts)
    tokens = query_ref.shape[0]
    key_width, value_width = query_ref.shape[1] // heads, value_ref.shape[1] // heads
    level, _ = levels(gates_ref)
    causal = lax.broadcasted_iota(jnp.int32, (tokens, tokens), 0) >= lax.broadcasted_iota(
        jnp.int32, (tokens, tokens), 1
    )
    key_scale = key_width ** (-0.5)
    first = 0
    for total_ref, note_ref, count in zip(outs[::2], outs[1::2], counts):
        notes = []
        for head in range(first, first + count):
            keys = slice(head * key_width, (head + 1) * key_width)
            channels = slice(head * value_width, (head + 1) * value_width)
            out = slice((head - first) * value_width, (head - first + 1) * value_width)
            masked = jnp.where(causal, level[head : head + 1], -jnp.inf)
            top = jnp.max(masked, axis=1, keepdims=True)
            scores = times_transpose(query_ref[:, keys], key_ref[:, keys]) * key_scale
            scores = scores * jnp.exp(masked - top)
            total_ref[:, out] = two_term_dot(scores, value_ref[:, channels])
            notes += [jnp.sum(scores, axis=1, keepdims=True), top]
        note_ref[...] = to_lanes(notes, tokens)
        first += count


def join_kernel(counts, gates0_ref, key0_ref, value0_ref, query_ref, *refs):
    chunks, heads = len(counts), sum(counts)
    tokens = query_ref.shape[0]
    key_width, value_width = query_ref.shape[1] // heads, value0_ref.shape[1] // heads
    block = lax.axis_index("sp")
    second = lax.rem(block, 2) == 1
    level0, end0 = levels(gates0_ref)
    top0 = jnp.max(level0, axis=1, keepdims=True)
    top0 = jnp.where(block == 1, jnp.maximum(top0, 0.0), top0)
    weight0 = jnp.exp(level0 - top0) * (key_width ** (-0.5))
    state = jnp.where(second, top0 + end0, jnp.where(block == 0, 0.0, -jnp.inf))
    shift = jnp.where(block == 3, end0, 0.0)
    first = 0
    for chunk, count in enumerate(counts):
        own_total, own_note, total_ref, note_ref = refs[chunk * 2 : chunk * 2 + 2] + refs[
            (chunks + chunk) * 2 : (chunks + chunk) * 2 + 2
        ]
        own = own_note[...]
        notes = []
        for head in range(first, first + count):
            pick = slice(head, head + 1)
            keys = slice(head * key_width, (head + 1) * key_width)
            channels = slice(head * value_width, (head + 1) * value_width)
            place = head - first
            out = slice(place * value_width, (place + 1) * value_width)
            own_top = own[:, 2 * place + 1 : 2 * place + 2]
            top = jnp.maximum(own_top, state[pick])
            scale = jnp.exp(own_top - top)
            scale0 = jnp.where(second, jnp.exp(state[pick] - top), 0.0)
            scores = times_transpose(query_ref[:, keys], key0_ref[:, keys])
            scores = scores * weight0[pick] * scale0
            total_ref[:, out] = scale * own_total[:, out] + two_term_dot(
                scores, value0_ref[:, channels]
            )
            sums = scale * own[:, 2 * place : 2 * place + 1] + jnp.sum(
                scores, axis=1, keepdims=True
            )
            notes += [sums, top, shift[pick]]
        note_ref[...] = to_lanes(notes, tokens)
        first += count


def serve_kernel(
    counts, gates0_ref, key0_ref, value0_ref, gates_ref, key_ref, value_ref,
    near_ref, far_ref, next_ref, later_ref, score_ref,
):
    heads, count = sum(counts), counts[0]
    tokens = near_ref.shape[0]
    key_width, value_width = near_ref.shape[1] // heads, value_ref.shape[1] // heads
    level0, end0 = levels(gates0_ref)
    level1, end1 = levels(gates_ref)
    level = jnp.concatenate([level0, level1 - end0], axis=1)
    top = jnp.maximum(jnp.max(level, axis=1, keepdims=True), 0.0)
    weight = jnp.exp(level - top) * (key_width ** (-0.5))
    reach = top + end0 + end1
    next_notes, later_notes = [], []
    for head in range(heads):
        keys = slice(head * key_width, (head + 1) * key_width)
        key_both = jnp.concatenate([key0_ref[:, keys], key_ref[:, keys]], axis=0)
        rows = jnp.concatenate([near_ref[:, keys], far_ref[:, keys]], axis=0)
        scores = times_transpose(rows, key_both) * weight[head : head + 1]
        sums = jnp.sum(scores, axis=1, keepdims=True)
        scores = scores.astype(jnp.bfloat16)
        if head < count:
            channels = slice(head * value_width, (head + 1) * value_width)
            give(scores, value0_ref, value_ref, channels, next_ref, later_ref, channels)
        else:
            place = head - count
            score_ref[:, place * 2 * tokens : (place + 1) * 2 * tokens] = scores
        terms = three_terms(reach[head : head + 1])
        next_notes += three_terms(sums[:tokens]) + terms
        later_notes += three_terms(sums[tokens:]) + terms
    next_ref[:, count * value_width :] = to_lanes(next_notes, tokens).astype(jnp.bfloat16)
    later_ref[:, count * value_width :] = to_lanes(later_notes, tokens).astype(jnp.bfloat16)


def give(scores, value0_ref, value_ref, channels, next_ref, later_ref, out):
    tokens = value_ref.shape[0]
    values = jnp.concatenate([value0_ref[:, channels], value_ref[:, channels]], axis=0)
    given = jnp.dot(scores, values, preferred_element_type=jnp.float32).astype(jnp.bfloat16)
    next_ref[:, out] = given[:tokens]
    later_ref[:, out] = given[tokens:]


def serve_rest_kernel(first, count, score_ref, value0_ref, value_ref, next_ref, later_ref):
    width = score_ref.shape[1] // count
    value_width = next_ref.shape[1] // count
    for place in range(count):
        channels = slice((first + place) * value_width, (first + place + 1) * value_width)
        out = slice(place * value_width, (place + 1) * value_width)
        scores = score_ref[:, place * width : (place + 1) * width]
        give(scores, value0_ref, value_ref, channels, next_ref, later_ref, out)


def gated_rows(heads, first, count, total_ref, note_ref, near_ref, far_ref, lanes, gate_ref):
    value_width = gate_ref.shape[1] // heads
    given = lax.axis_index("sp") >= 2
    own = note_ref[...]
    gated = []
    for place in range(count):
        out = slice(place * value_width, (place + 1) * value_width)
        channels = slice((first + place) * value_width, (first + place + 1) * value_width)
        at = 6 * (first + place)
        sums = lanes[:, at : at + 1] + lanes[:, at + 1 : at + 2] + lanes[:, at + 2 : at + 3]
        at += 3
        reach = lanes[:, at : at + 1] + lanes[:, at + 1 : at + 2] + lanes[:, at + 2 : at + 3]
        reach = reach + own[:, 3 * place + 2 : 3 * place + 3]
        top = own[:, 3 * place + 1 : 3 * place + 2]
        peak = jnp.where(given, jnp.maximum(top, reach), top)
        scale = jnp.exp(top - peak)
        scale_given = jnp.where(given, jnp.exp(reach - peak), 0.0)
        weight = scale * own[:, 3 * place : 3 * place + 1] + scale_given * sums
        inverse = 1.0 / jnp.maximum(jnp.abs(weight), 1.0)
        message = near_ref[:, out].astype(jnp.float32) + far_ref[:, out].astype(jnp.float32)
        cell = (scale * inverse) * total_ref[:, out] + (scale_given * inverse) * message
        hidden = cell.astype(jnp.bfloat16).astype(jnp.float32)
        gate = jax.nn.sigmoid(gate_ref[:, channels].astype(jnp.float32))
        gated.append((hidden * gate).astype(jnp.bfloat16))
    return jnp.concatenate(gated, axis=1)


def product(left, right):
    return jnp.dot(left, right, preferred_element_type=jnp.float32)


def first_kernel(counts, gate_ref, total_ref, note_ref, near_ref, far_ref, *refs):
    pieces, gated_ref, lane_ref, part_ref = refs[:-3], refs[-3], refs[-2], refs[-1]
    rows = gated_ref.shape[1]
    lanes = near_ref[:, rows:].astype(jnp.float32) + far_ref[:, rows:].astype(jnp.float32)
    lane_ref[...] = lanes
    gated = gated_rows(
        sum(counts), 0, counts[0], total_ref, note_ref, near_ref, far_ref, lanes, gate_ref
    )
    gated_ref[...] = gated
    width = pieces[0].shape[1]
    for place, piece in enumerate(pieces):
        part_ref[:, place * width : (place + 1) * width] = product(gated, piece[:rows, :])


def finish_kernel(
    counts, whole, plan, gate_ref, total_ref, note_ref, near_ref, far_ref, gated_ref, lane_ref,
    part_ref, *refs,
):
    pieces, out_ref = refs[:-1], refs[-1]
    rows, device = gated_ref.shape[1], lax.axis_index("dp")
    width = pieces[0].shape[1]
    gated = gated_rows(
        sum(counts), counts[0], counts[1], total_ref, note_ref, near_ref, far_ref,
        lane_ref[...], gate_ref,
    )

    def put(mask, columns):
        start = pl.multiple_of((device ^ mask) * width, width)
        out_ref[:, pl.ds(start, width)] = columns.astype(out_ref.dtype)

    for place, (mask, piece) in enumerate(zip(whole, pieces)):
        part = part_ref[:, place * width : (place + 1) * width]
        put(mask, part + product(gated, piece[rows:, :]))
    both = jnp.concatenate([gated_ref[...], gated], axis=1)
    sums = {}
    for (mask, start), piece in zip(plan, pieces[len(whole) :]):
        part = product(both[:, start : start + piece.shape[0]], piece[...])
        sums[mask] = sums[mask] + part if mask in sums else part
    for mask, columns in sums.items():
        put(mask, columns)


def kernel_call(kernel, operands, outs, flops, limit):
    vmem = pl.BlockSpec(memory_space=pltpu.VMEM)
    size = sum(x.size * x.dtype.itemsize for x in (*operands, *outs))
    return pl.pallas_call(
        kernel,
        out_shape=outs,
        in_specs=[vmem] * len(operands),
        out_specs=[vmem] * len(outs),
        compiler_params=pltpu.CompilerParams(vmem_limit_bytes=limit * MIB),
        cost_estimate=pl.CostEstimate(flops=flops, bytes_accessed=size, transcendentals=0),
    )(*operands)


def block_body(queries, key_rows, values, out_gate, input_gate, forget_gate, out_weight):
    return block_steps(
        queries[0], key_rows[0], values[0], out_gate[0], input_gate[0], forget_gate[0], out_weight
    )[None]


def block_steps(query, key, value, gate, input_log, forget, out_weight):
    tokens, heads = query.shape[0], input_log.shape[0]
    key_width, value_width = query.shape[1] // heads, value.shape[1] // heads
    shape = jax.ShapeDtypeStruct
    device_count = lax.axis_size("dp")

    def swap(piece, bit):
        return lax.ppermute(piece, "dp", [(i, i ^ bit) for i in range(device_count)])

    (gates,) = kernel_call(
        gates_kernel, [input_log, forget], [shape((2 * heads, tokens), jnp.float32)], 0, 2
    )
    pair = [(0, 1), (2, 3)]
    earlier = [
        lax.ppermute(gates, "sp", pair),
        lax.ppermute(key, "sp", pair),
        lax.ppermute(value, "sp", pair),
    ]
    here = [gates, key, value]
    near = lax.ppermute(query, "sp", [(2, 1)])
    far = lax.ppermute(query, "sp", [(3, 1)])

    half = out_weight.shape[0] // 2
    from_x = swap(out_weight, XBIT)
    from_y = swap(out_weight, YBIT)
    from_core = swap(out_weight, CORE)
    top = swap(from_x[:half], YBIT)
    bottom = swap(from_y[half:], XBIT)
    whole = {
        0: out_weight,
        CORE: from_core,
        XBIT: from_x,
        XBIT | CORE: swap(from_x, CORE),
        YBIT: from_y,
        YBIT | CORE: swap(from_y, CORE),
    }
    corner = [
        ((XBIT | YBIT, 0), top),
        ((XBIT | YBIT, half), bottom),
        ((XBIT | YBIT | CORE, 0), swap(top, CORE)),
        ((XBIT | YBIT | CORE, half), swap(bottom, CORE)),
    ]

    work = 2 * tokens * tokens * (key_width + value_width)
    sums = [
        x
        for count in COUNTS
        for x in (
            shape((tokens, count * value_width), jnp.float32),
            shape((tokens, LANES), jnp.float32),
        )
    ]
    own = kernel_call(
        functools.partial(own_kernel, COUNTS), [*here, query], sums, 3 * heads * work // 2, 8
    )
    first, rest = COUNTS
    message = shape((tokens, first * value_width + LANES), jnp.bfloat16)
    given_next, given_later, scores = kernel_call(
        functools.partial(serve_kernel, COUNTS),
        [*earlier, *here, near, far],
        [message, message, shape((2 * tokens, rest * 2 * tokens), jnp.bfloat16)],
        4 * heads * work,
        8,
    )
    message = shape((tokens, rest * value_width), jnp.bfloat16)
    rest_next, rest_later = kernel_call(
        functools.partial(serve_rest_kernel, first, rest),
        [scores, earlier[2], value],
        [message] * 2,
        2 * rest * work,
        8,
    )
    nears = [lax.ppermute(given_next, "sp", [(1, 2)]), lax.ppermute(rest_next, "sp", [(1, 2)])]
    fars = [lax.ppermute(given_later, "sp", [(1, 3)]), lax.ppermute(rest_later, "sp", [(1, 3)])]
    home = kernel_call(
        functools.partial(join_kernel, COUNTS),
        [*earlier, query, *own],
        sums,
        3 * heads * work // 2,
        8,
    )
    width = out_weight.shape[1]
    kept = kernel_call(
        functools.partial(first_kernel, COUNTS),
        [gate, *home[:2], nears[0], fars[0], *whole.values()],
        [
            shape((tokens, first * value_width), jnp.bfloat16),
            shape((tokens, LANES), jnp.float32),
            shape((tokens, len(whole) * width), jnp.float32),
        ],
        2 * tokens * first * value_width * len(whole) * width,
        10,
    )
    (out,) = kernel_call(
        functools.partial(finish_kernel, COUNTS, tuple(whole), tuple(place for place, _ in corner)),
        [
            gate, *home[2:], nears[1], fars[1], *kept, *whole.values(),
            *(piece for _, piece in corner),
        ],
        [shape((tokens, width * device_count), jnp.bfloat16)],
        2 * tokens * rest * value_width * width * device_count,
        12,
    )
    return out


def body(queries, key_rows, values, out_gate, input_gate, forget_gate, out_weight):
    group_count = lax.axis_size("sp")
    token_count = queries.shape[1]
    head_count = input_gate.shape[1]
    copies = group_count // head_count
    head_key = queries.shape[2] // head_count
    slice_width = values.shape[2] // group_count

    def spread(source):
        widened = jnp.broadcast_to(
            source[0].reshape(token_count, head_count, 1, head_key),
            (token_count, head_count, copies, head_key),
        )
        return widened.reshape(token_count, group_count, head_key)

    def spread_gate(source):
        return jnp.repeat(source[0].T, copies, axis=1)

    query_all, key_all = (
        lax.all_to_all(spread(queries), "sp", split_axis=1, concat_axis=0, tiled=True),
        lax.all_to_all(spread(key_rows), "sp", split_axis=1, concat_axis=0, tiled=True),
    )
    value_all, input_all, forget_all = (
        lax.all_to_all(
            values[0].reshape(token_count, group_count, slice_width),
            "sp",
            split_axis=1,
            concat_axis=0,
            tiled=True,
        ),
        lax.all_to_all(spread_gate(input_gate), "sp", split_axis=1, concat_axis=0, tiled=True),
        lax.all_to_all(spread_gate(forget_gate), "sp", split_axis=1, concat_axis=0, tiled=True),
    )
    output = memory_cell(
        query_all[:, 0],
        key_all[:, 0],
        value_all[:, 0],
        input_all[:, 0].astype(jnp.float32),
        jax.nn.log_sigmoid(forget_all[:, 0].astype(jnp.float32)),
    )
    hidden = output.astype(jnp.bfloat16)
    token_rows = lax.all_to_all(hidden, "sp", split_axis=0, concat_axis=1, tiled=True)
    gated_rows = (
        token_rows.astype(jnp.float32) * jax.nn.sigmoid(out_gate[0].astype(jnp.float32))
    ).astype(jnp.bfloat16)
    projected = jnp.dot(
        gated_rows,
        lax.all_gather(out_weight, "dp", axis=1, tiled=True),
        preferred_element_type=jnp.float32,
    )
    return projected.astype(jnp.bfloat16)[None]


def solution(mesh):
    blocks = mesh.shape["sp"] == 4 and mesh.shape["dp"] == 8
    return jax.shard_map(
        block_body if blocks else body,
        mesh=mesh,
        in_specs=(
            P("dp", "sp", None),
            P("dp", "sp", None),
            P("dp", "sp", None),
            P("dp", "sp", None),
            P("dp", None, "sp"),
            P("dp", None, "sp"),
            P(None, "dp"),
        ),
        out_specs=P("dp", "sp", None),
        check_vma=False,
    )
```

```python
import functools

import jax
import jax.numpy as jnp
from jax import lax
from jax.experimental import pallas as pl
from jax.experimental.pallas import tpu as pltpu
from jax.sharding import PartitionSpec as P


BLOCK = 128


def memory_cell(query_rows, key_in, value_rows, input_log, forget_log):
    block_count = query_rows.shape[0] // BLOCK
    key_width = query_rows.shape[1]
    value_width = value_rows.shape[1]
    key_scale = key_width ** (-0.5)
    causal = lax.broadcasted_iota(jnp.int32, (BLOCK, BLOCK), 0) >= lax.broadcasted_iota(
        jnp.int32, (BLOCK, BLOCK), 1
    )
    highest = lax.Precision.HIGHEST

    def block_step(state_in, inputs):
        memory, normer, stabil = state_in
        query_part, key_part, value_part, gain_part, decay_part = inputs
        query_part = query_part.astype(jnp.float32)
        key_part = key_part.astype(jnp.float32) * key_scale
        value_part = value_part.astype(jnp.float32)
        running = jnp.cumsum(decay_part)
        log_weight = running[:, None] - running[None, :] + gain_part[None, :]
        log_weight = jnp.where(causal, log_weight, -jnp.inf)
        carried_log = running + stabil
        row_top = jnp.maximum(carried_log, jnp.max(log_weight, axis=1))
        scores = jnp.dot(query_part, key_part.T, precision=highest) * jnp.exp(
            log_weight - row_top[:, None]
        )
        carried = jnp.exp(carried_log - row_top)
        numerator = jnp.dot(scores, value_part, precision=highest) + carried[:, None] * jnp.dot(
            query_part, memory, precision=highest
        )
        denominator = jnp.sum(scores, axis=1) + carried * jnp.dot(
            query_part, normer, precision=highest
        )
        output = numerator / jnp.maximum(jnp.abs(denominator), 1.0)[:, None]
        block_end = running[-1]
        weight_log = block_end - running + gain_part
        new_top = jnp.maximum(block_end + stabil, jnp.max(weight_log))
        weights = jnp.exp(weight_log - new_top)
        retain = jnp.exp(block_end + stabil - new_top)
        memory = retain * memory + jnp.dot(
            (key_part * weights[:, None]).T, value_part, precision=highest
        )
        normer = retain * normer + jnp.dot(weights, key_part, precision=highest)
        return ((memory, normer, new_top), output)

    start_state = (
        jnp.zeros((key_width, value_width), jnp.float32),
        jnp.zeros((key_width,), jnp.float32),
        jnp.zeros((), jnp.float32),
    )
    blocks = tuple(
        (
            source.reshape((block_count, BLOCK) + source.shape[1:])
            for source in (query_rows, key_in, value_rows, input_log, forget_log)
        )
    )
    _, outputs = lax.scan(block_step, start_state, blocks)
    return outputs.reshape(block_count * BLOCK, value_width)


LANES = 128


def log_forget(gates):
    return -jnp.log1p(jnp.exp(-gates))


def running_sum(rows):
    width = rows.shape[1]
    upto = lax.broadcasted_iota(jnp.int32, (width, width), 0) <= lax.broadcasted_iota(
        jnp.int32, (width, width), 1
    )
    return jnp.dot(
        rows,
        upto.astype(jnp.float32),
        precision=lax.Precision.HIGHEST,
        preferred_element_type=jnp.float32,
    )


def times_transpose(left, right):
    return lax.dot_general(
        left, right, (((1,), (1,)), ((), ())), preferred_element_type=jnp.float32
    )


def three_terms(value):
    high = value.astype(jnp.bfloat16).astype(jnp.float32)
    middle = (value - high).astype(jnp.bfloat16).astype(jnp.float32)
    return [high, middle, value - high - middle]


def to_lanes(columns, rows):
    lane = lax.broadcasted_iota(jnp.int32, (rows, LANES), 1)
    tile = jnp.zeros((rows, LANES), jnp.float32)
    for place, column in enumerate(columns):
        tile = jnp.where(lane == place, column, tile)
    return tile


MIB = 1 << 20
COUNTS = (2, 2)
CORE, XBIT, YBIT = 1, 2, 4


def gates_kernel(input_ref, forget_ref, out_ref):
    running = running_sum(log_forget(forget_ref[...].astype(jnp.float32)))
    heads, tokens = running.shape
    level = input_ref[...].astype(jnp.float32) - running
    decay = jnp.broadcast_to(running[:, tokens - 1 :], (heads, tokens))
    out_ref[...] = jnp.concatenate([level, decay], axis=0)


def levels(ref):
    heads = ref.shape[0] // 2
    return ref[:heads, :], ref[heads:, :1]


def two_term_dot(left, right):
    high = left.astype(jnp.bfloat16)
    low = (left - high.astype(jnp.float32)).astype(jnp.bfloat16)
    return jnp.dot(high, right, preferred_element_type=jnp.float32) + jnp.dot(
        low, right, preferred_element_type=jnp.float32
    )


def own_kernel(counts, gates_ref, key_ref, value_ref, query_ref, *outs):
    heads = sum(counts)
    tokens = query_ref.shape[0]
    key_width, value_width = query_ref.shape[1] // heads, value_ref.shape[1] // heads
    level, _ = levels(gates_ref)
    causal = lax.broadcasted_iota(jnp.int32, (tokens, tokens), 0) >= lax.broadcasted_iota(
        jnp.int32, (tokens, tokens), 1
    )
    key_scale = key_width ** (-0.5)
    first = 0
    for total_ref, note_ref, count in zip(outs[::2], outs[1::2], counts):
        notes = []
        for head in range(first, first + count):
            keys = slice(head * key_width, (head + 1) * key_width)
            channels = slice(head * value_width, (head + 1) * value_width)
            out = slice((head - first) * value_width, (head - first + 1) * value_width)
            masked = jnp.where(causal, level[head : head + 1], -jnp.inf)
            top = jnp.max(masked, axis=1, keepdims=True)
            scores = times_transpose(query_ref[:, keys], key_ref[:, keys]) * key_scale
            scores = scores * jnp.exp(masked - top)
            total_ref[:, out] = two_term_dot(scores, value_ref[:, channels])
            notes += [jnp.sum(scores, axis=1, keepdims=True), top]
        note_ref[...] = to_lanes(notes, tokens)
        first += count


def join_kernel(counts, gates0_ref, key0_ref, *refs):
    chunks, heads = len(counts), sum(counts)
    values0, query_ref, refs = refs[:chunks], refs[chunks], refs[chunks + 1 :]
    tokens = query_ref.shape[0]
    key_width, value_width = query_ref.shape[1] // heads, values0[0].shape[1] // counts[0]
    block = lax.axis_index("sp")
    second = lax.rem(block, 2) == 1
    level0, end0 = levels(gates0_ref)
    top0 = jnp.max(level0, axis=1, keepdims=True)
    top0 = jnp.where(block == 1, jnp.maximum(top0, 0.0), top0)
    weight0 = jnp.exp(level0 - top0) * (key_width ** (-0.5))
    state = jnp.where(second, top0 + end0, jnp.where(block == 0, 0.0, -jnp.inf))
    shift = jnp.where(block == 3, end0, 0.0)
    first = 0
    for chunk, count in enumerate(counts):
        own_total, own_note, total_ref, note_ref = refs[chunk * 2 : chunk * 2 + 2] + refs[
            (chunks + chunk) * 2 : (chunks + chunk) * 2 + 2
        ]
        own = own_note[...]
        notes = []
        for head in range(first, first + count):
            pick = slice(head, head + 1)
            keys = slice(head * key_width, (head + 1) * key_width)
            place = head - first
            out = slice(place * value_width, (place + 1) * value_width)
            own_top = own[:, 2 * place + 1 : 2 * place + 2]
            top = jnp.maximum(own_top, state[pick])
            scale = jnp.exp(own_top - top)
            scale0 = jnp.where(second, jnp.exp(state[pick] - top), 0.0)
            scores = times_transpose(query_ref[:, keys], key0_ref[:, keys])
            scores = scores * weight0[pick] * scale0
            total_ref[:, out] = scale * own_total[:, out] + two_term_dot(
                scores, values0[chunk][:, out]
            )
            sums = scale * own[:, 2 * place : 2 * place + 1] + jnp.sum(
                scores, axis=1, keepdims=True
            )
            notes += [sums, top, shift[pick]]
        note_ref[...] = to_lanes(notes, tokens)
        first += count


def serve_kernel(
    counts, gates0_ref, key0_ref, value0_ref, gates_ref, key_ref, value_ref,
    near_ref, far_ref, next_ref, later_ref, score_ref,
):
    heads, count = sum(counts), counts[0]
    tokens = near_ref.shape[0]
    key_width, value_width = near_ref.shape[1] // heads, value_ref.shape[1] // heads
    level0, end0 = levels(gates0_ref)
    level1, end1 = levels(gates_ref)
    level = jnp.concatenate([level0, level1 - end0], axis=1)
    top = jnp.maximum(jnp.max(level, axis=1, keepdims=True), 0.0)
    weight = jnp.exp(level - top) * (key_width ** (-0.5))
    reach = top + end0 + end1
    next_notes, later_notes = [], []
    for head in range(heads):
        keys = slice(head * key_width, (head + 1) * key_width)
        key_both = jnp.concatenate([key0_ref[:, keys], key_ref[:, keys]], axis=0)
        rows = jnp.concatenate([near_ref[:, keys], far_ref[:, keys]], axis=0)
        scores = times_transpose(rows, key_both) * weight[head : head + 1]
        sums = jnp.sum(scores, axis=1, keepdims=True)
        scores = scores.astype(jnp.bfloat16)
        if head < count:
            channels = slice(head * value_width, (head + 1) * value_width)
            give(scores, value0_ref[:, channels], value_ref[:, channels], next_ref, later_ref, channels)
        else:
            place = head - count
            score_ref[:, place * 2 * tokens : (place + 1) * 2 * tokens] = scores
        terms = three_terms(reach[head : head + 1])
        next_notes += three_terms(sums[:tokens]) + terms
        later_notes += three_terms(sums[tokens:]) + terms
    next_ref[:, count * value_width :] = to_lanes(next_notes, tokens).astype(jnp.bfloat16)
    later_ref[:, count * value_width :] = to_lanes(later_notes, tokens).astype(jnp.bfloat16)


def give(scores, value0, value1, next_ref, later_ref, out):
    tokens = value1.shape[0]
    values = jnp.concatenate([value0, value1], axis=0)
    given = jnp.dot(scores, values, preferred_element_type=jnp.float32).astype(jnp.bfloat16)
    next_ref[:, out] = given[:tokens]
    later_ref[:, out] = given[tokens:]


def serve_rest_kernel(first, count, score_ref, value0_ref, value_ref, next_ref, later_ref):
    width = score_ref.shape[1] // count
    value_width = next_ref.shape[1] // count
    for place in range(count):
        channels = slice((first + place) * value_width, (first + place + 1) * value_width)
        out = slice(place * value_width, (place + 1) * value_width)
        scores = score_ref[:, place * width : (place + 1) * width]
        give(scores, value0_ref[:, out], value_ref[:, channels], next_ref, later_ref, out)


def gated_rows(heads, first, count, total_ref, note_ref, near_ref, far_ref, lanes, gate_ref):
    value_width = gate_ref.shape[1] // heads
    given = lax.axis_index("sp") >= 2
    own = note_ref[...]
    gated = []
    for place in range(count):
        out = slice(place * value_width, (place + 1) * value_width)
        channels = slice((first + place) * value_width, (first + place + 1) * value_width)
        at = 6 * (first + place)
        sums = lanes[:, at : at + 1] + lanes[:, at + 1 : at + 2] + lanes[:, at + 2 : at + 3]
        at += 3
        reach = lanes[:, at : at + 1] + lanes[:, at + 1 : at + 2] + lanes[:, at + 2 : at + 3]
        reach = reach + own[:, 3 * place + 2 : 3 * place + 3]
        top = own[:, 3 * place + 1 : 3 * place + 2]
        peak = jnp.where(given, jnp.maximum(top, reach), top)
        scale = jnp.exp(top - peak)
        scale_given = jnp.where(given, jnp.exp(reach - peak), 0.0)
        weight = scale * own[:, 3 * place : 3 * place + 1] + scale_given * sums
        inverse = 1.0 / jnp.maximum(jnp.abs(weight), 1.0)
        message = near_ref[:, out].astype(jnp.float32) + far_ref[:, out].astype(jnp.float32)
        cell = (scale * inverse) * total_ref[:, out] + (scale_given * inverse) * message
        hidden = cell.astype(jnp.bfloat16).astype(jnp.float32)
        gate = jax.nn.sigmoid(gate_ref[:, channels].astype(jnp.float32))
        gated.append((hidden * gate).astype(jnp.bfloat16))
    return jnp.concatenate(gated, axis=1)


def product(left, right):
    return jnp.dot(left, right, preferred_element_type=jnp.float32)


def first_kernel(counts, gate_ref, total_ref, note_ref, near_ref, far_ref, *refs):
    pieces, gated_ref, lane_ref, part_ref = refs[:-3], refs[-3], refs[-2], refs[-1]
    rows = gated_ref.shape[1]
    lanes = near_ref[:, rows:].astype(jnp.float32) + far_ref[:, rows:].astype(jnp.float32)
    lane_ref[...] = lanes
    gated = gated_rows(
        sum(counts), 0, counts[0], total_ref, note_ref, near_ref, far_ref, lanes, gate_ref
    )
    gated_ref[...] = gated
    width = pieces[0].shape[1]
    for place, piece in enumerate(pieces):
        part_ref[:, place * width : (place + 1) * width] = product(gated, piece[:rows, :])


def finish_kernel(
    counts, whole, plan, gate_ref, total_ref, note_ref, near_ref, far_ref, gated_ref, lane_ref,
    part_ref, *refs,
):
    pieces, out_ref = refs[:-1], refs[-1]
    rows, device = gated_ref.shape[1], lax.axis_index("dp")
    width = pieces[0].shape[1]
    gated = gated_rows(
        sum(counts), counts[0], counts[1], total_ref, note_ref, near_ref, far_ref,
        lane_ref[...], gate_ref,
    )

    def put(mask, columns):
        start = pl.multiple_of((device ^ mask) * width, width)
        out_ref[:, pl.ds(start, width)] = columns.astype(out_ref.dtype)

    for place, (mask, piece) in enumerate(zip(whole, pieces)):
        part = part_ref[:, place * width : (place + 1) * width]
        put(mask, part + product(gated, piece[rows:, :]))
    both = jnp.concatenate([gated_ref[...], gated], axis=1)
    sums = {}
    for (mask, start), piece in zip(plan, pieces[len(whole) :]):
        part = product(both[:, start : start + piece.shape[0]], piece[...])
        sums[mask] = sums[mask] + part if mask in sums else part
    for mask, columns in sums.items():
        put(mask, columns)


def kernel_call(kernel, operands, outs, flops, limit):
    vmem = pl.BlockSpec(memory_space=pltpu.VMEM)
    size = sum(x.size * x.dtype.itemsize for x in (*operands, *outs))
    return pl.pallas_call(
        kernel,
        out_shape=outs,
        in_specs=[vmem] * len(operands),
        out_specs=[vmem] * len(outs),
        compiler_params=pltpu.CompilerParams(vmem_limit_bytes=limit * MIB),
        cost_estimate=pl.CostEstimate(flops=flops, bytes_accessed=size, transcendentals=0),
    )(*operands)


def block_body(queries, key_rows, values, out_gate, input_gate, forget_gate, out_weight):
    return block_steps(
        queries[0], key_rows[0], values[0], out_gate[0], input_gate[0], forget_gate[0], out_weight
    )[None]


def block_steps(query, key, value, gate, input_log, forget, out_weight):
    tokens, heads = query.shape[0], input_log.shape[0]
    key_width, value_width = query.shape[1] // heads, value.shape[1] // heads
    shape = jax.ShapeDtypeStruct
    device_count = lax.axis_size("dp")

    def swap(piece, bit):
        return lax.ppermute(piece, "dp", [(i, i ^ bit) for i in range(device_count)])

    (gates,) = kernel_call(
        gates_kernel, [input_log, forget], [shape((2 * heads, tokens), jnp.float32)], 0, 2
    )
    pair = [(0, 1), (2, 3)]
    first, rest = COUNTS
    split = first * value_width
    earlier = [lax.ppermute(gates, "sp", pair), lax.ppermute(key, "sp", pair)]
    values0 = [
        lax.ppermute(value[:, :split], "sp", pair), lax.ppermute(value[:, split:], "sp", pair)
    ]
    here = [gates, key, value]
    near = lax.ppermute(query, "sp", [(2, 1)])
    far = lax.ppermute(query, "sp", [(3, 1)])

    half = out_weight.shape[0] // 2
    from_x = swap(out_weight, XBIT)
    from_y = swap(out_weight, YBIT)
    from_core = swap(out_weight, CORE)
    top = swap(from_x[:half], YBIT)
    bottom = swap(from_y[half:], XBIT)
    whole = {
        0: out_weight,
        CORE: from_core,
        XBIT: from_x,
        XBIT | CORE: swap(from_x, CORE),
        YBIT: from_y,
        YBIT | CORE: swap(from_y, CORE),
    }
    corner = [
        ((XBIT | YBIT, 0), top),
        ((XBIT | YBIT, half), bottom),
        ((XBIT | YBIT | CORE, 0), swap(top, CORE)),
        ((XBIT | YBIT | CORE, half), swap(bottom, CORE)),
    ]

    work = 2 * tokens * tokens * (key_width + value_width)
    sums = [
        x
        for count in COUNTS
        for x in (
            shape((tokens, count * value_width), jnp.float32),
            shape((tokens, LANES), jnp.float32),
        )
    ]
    own = kernel_call(
        functools.partial(own_kernel, COUNTS), [*here, query], sums, 3 * heads * work // 2, 8
    )
    message = shape((tokens, first * value_width + LANES), jnp.bfloat16)
    given_next, given_later, scores = kernel_call(
        functools.partial(serve_kernel, COUNTS),
        [*earlier, values0[0], *here, near, far],
        [message, message, shape((2 * tokens, rest * 2 * tokens), jnp.bfloat16)],
        4 * heads * work,
        8,
    )
    message = shape((tokens, rest * value_width), jnp.bfloat16)
    rest_next, rest_later = kernel_call(
        functools.partial(serve_rest_kernel, first, rest),
        [scores, values0[1], value],
        [message] * 2,
        2 * rest * work,
        8,
    )
    nears = [lax.ppermute(given_next, "sp", [(1, 2)]), lax.ppermute(rest_next, "sp", [(1, 2)])]
    fars = [lax.ppermute(given_later, "sp", [(1, 3)]), lax.ppermute(rest_later, "sp", [(1, 3)])]
    home = kernel_call(
        functools.partial(join_kernel, COUNTS),
        [*earlier, *values0, query, *own],
        sums,
        3 * heads * work // 2,
        8,
    )
    width = out_weight.shape[1]
    kept = kernel_call(
        functools.partial(first_kernel, COUNTS),
        [gate, *home[:2], nears[0], fars[0], *whole.values()],
        [
            shape((tokens, first * value_width), jnp.bfloat16),
            shape((tokens, LANES), jnp.float32),
            shape((tokens, len(whole) * width), jnp.float32),
        ],
        2 * tokens * first * value_width * len(whole) * width,
        10,
    )
    (out,) = kernel_call(
        functools.partial(finish_kernel, COUNTS, tuple(whole), tuple(place for place, _ in corner)),
        [
            gate, *home[2:], nears[1], fars[1], *kept, *whole.values(),
            *(piece for _, piece in corner),
        ],
        [shape((tokens, width * device_count), jnp.bfloat16)],
        2 * tokens * rest * value_width * width * device_count,
        12,
    )
    return out


def body(queries, key_rows, values, out_gate, input_gate, forget_gate, out_weight):
    group_count = lax.axis_size("sp")
    token_count = queries.shape[1]
    head_count = input_gate.shape[1]
    copies = group_count // head_count
    head_key = queries.shape[2] // head_count
    slice_width = values.shape[2] // group_count

    def spread(source):
        widened = jnp.broadcast_to(
            source[0].reshape(token_count, head_count, 1, head_key),
            (token_count, head_count, copies, head_key),
        )
        return widened.reshape(token_count, group_count, head_key)

    def spread_gate(source):
        return jnp.repeat(source[0].T, copies, axis=1)

    query_all, key_all = (
        lax.all_to_all(spread(queries), "sp", split_axis=1, concat_axis=0, tiled=True),
        lax.all_to_all(spread(key_rows), "sp", split_axis=1, concat_axis=0, tiled=True),
    )
    value_all, input_all, forget_all = (
        lax.all_to_all(
            values[0].reshape(token_count, group_count, slice_width),
            "sp",
            split_axis=1,
            concat_axis=0,
            tiled=True,
        ),
        lax.all_to_all(spread_gate(input_gate), "sp", split_axis=1, concat_axis=0, tiled=True),
        lax.all_to_all(spread_gate(forget_gate), "sp", split_axis=1, concat_axis=0, tiled=True),
    )
    output = memory_cell(
        query_all[:, 0],
        key_all[:, 0],
        value_all[:, 0],
        input_all[:, 0].astype(jnp.float32),
        jax.nn.log_sigmoid(forget_all[:, 0].astype(jnp.float32)),
    )
    hidden = output.astype(jnp.bfloat16)
    token_rows = lax.all_to_all(hidden, "sp", split_axis=0, concat_axis=1, tiled=True)
    gated_rows = (
        token_rows.astype(jnp.float32) * jax.nn.sigmoid(out_gate[0].astype(jnp.float32))
    ).astype(jnp.bfloat16)
    projected = jnp.dot(
        gated_rows,
        lax.all_gather(out_weight, "dp", axis=1, tiled=True),
        preferred_element_type=jnp.float32,
    )
    return projected.astype(jnp.bfloat16)[None]


def solution(mesh):
    blocks = mesh.shape["sp"] == 4 and mesh.shape["dp"] == 8
    return jax.shard_map(
        block_body if blocks else body,
        mesh=mesh,
        in_specs=(
            P("dp", "sp", None),
            P("dp", "sp", None),
            P("dp", "sp", None),
            P("dp", "sp", None),
            P("dp", None, "sp"),
            P("dp", None, "sp"),
            P(None, "dp"),
        ),
        out_specs=P("dp", "sp", None),
        check_vma=False,
    )
```

```python
import functools

import jax
import jax.numpy as jnp
from jax import lax
from jax.experimental import pallas as pl
from jax.experimental.pallas import tpu as pltpu
from jax.sharding import PartitionSpec as P


BLOCK = 128


def memory_cell(query_rows, key_in, value_rows, input_log, forget_log):
    block_count = query_rows.shape[0] // BLOCK
    key_width = query_rows.shape[1]
    value_width = value_rows.shape[1]
    key_scale = key_width ** (-0.5)
    causal = lax.broadcasted_iota(jnp.int32, (BLOCK, BLOCK), 0) >= lax.broadcasted_iota(
        jnp.int32, (BLOCK, BLOCK), 1
    )
    highest = lax.Precision.HIGHEST

    def block_step(state_in, inputs):
        memory, normer, stabil = state_in
        query_part, key_part, value_part, gain_part, decay_part = inputs
        query_part = query_part.astype(jnp.float32)
        key_part = key_part.astype(jnp.float32) * key_scale
        value_part = value_part.astype(jnp.float32)
        running = jnp.cumsum(decay_part)
        log_weight = running[:, None] - running[None, :] + gain_part[None, :]
        log_weight = jnp.where(causal, log_weight, -jnp.inf)
        carried_log = running + stabil
        row_top = jnp.maximum(carried_log, jnp.max(log_weight, axis=1))
        scores = jnp.dot(query_part, key_part.T, precision=highest) * jnp.exp(
            log_weight - row_top[:, None]
        )
        carried = jnp.exp(carried_log - row_top)
        numerator = jnp.dot(scores, value_part, precision=highest) + carried[:, None] * jnp.dot(
            query_part, memory, precision=highest
        )
        denominator = jnp.sum(scores, axis=1) + carried * jnp.dot(
            query_part, normer, precision=highest
        )
        output = numerator / jnp.maximum(jnp.abs(denominator), 1.0)[:, None]
        block_end = running[-1]
        weight_log = block_end - running + gain_part
        new_top = jnp.maximum(block_end + stabil, jnp.max(weight_log))
        weights = jnp.exp(weight_log - new_top)
        retain = jnp.exp(block_end + stabil - new_top)
        memory = retain * memory + jnp.dot(
            (key_part * weights[:, None]).T, value_part, precision=highest
        )
        normer = retain * normer + jnp.dot(weights, key_part, precision=highest)
        return ((memory, normer, new_top), output)

    start_state = (
        jnp.zeros((key_width, value_width), jnp.float32),
        jnp.zeros((key_width,), jnp.float32),
        jnp.zeros((), jnp.float32),
    )
    blocks = tuple(
        (
            source.reshape((block_count, BLOCK) + source.shape[1:])
            for source in (query_rows, key_in, value_rows, input_log, forget_log)
        )
    )
    _, outputs = lax.scan(block_step, start_state, blocks)
    return outputs.reshape(block_count * BLOCK, value_width)


LANES = 128


def log_forget(gates):
    return -jnp.log1p(jnp.exp(-gates))


def running_sum(rows):
    width = rows.shape[1]
    upto = lax.broadcasted_iota(jnp.int32, (width, width), 0) <= lax.broadcasted_iota(
        jnp.int32, (width, width), 1
    )
    return jnp.dot(
        rows,
        upto.astype(jnp.float32),
        precision=lax.Precision.HIGHEST,
        preferred_element_type=jnp.float32,
    )


def times_transpose(left, right):
    return lax.dot_general(
        left, right, (((1,), (1,)), ((), ())), preferred_element_type=jnp.float32
    )


def three_terms(value):
    high = value.astype(jnp.bfloat16).astype(jnp.float32)
    middle = (value - high).astype(jnp.bfloat16).astype(jnp.float32)
    return [high, middle, value - high - middle]


def to_lanes(columns, rows):
    lane = lax.broadcasted_iota(jnp.int32, (rows, LANES), 1)
    tile = jnp.zeros((rows, LANES), jnp.float32)
    for place, column in enumerate(columns):
        tile = jnp.where(lane == place, column, tile)
    return tile


MIB = 1 << 20
COUNTS = (2, 2)
CORE, XBIT, YBIT = 1, 2, 4


def gates_kernel(input_ref, forget_ref, out_ref):
    running = running_sum(log_forget(forget_ref[...].astype(jnp.float32)))
    heads, tokens = running.shape
    level = input_ref[...].astype(jnp.float32) - running
    decay = jnp.broadcast_to(running[:, tokens - 1 :], (heads, tokens))
    out_ref[...] = jnp.concatenate([level, decay], axis=0)


def levels(ref):
    heads = ref.shape[0] // 2
    return ref[:heads, :], ref[heads:, :1]


def two_term_dot(left, right):
    high = left.astype(jnp.bfloat16)
    low = (left - high.astype(jnp.float32)).astype(jnp.bfloat16)
    return jnp.dot(high, right, preferred_element_type=jnp.float32) + jnp.dot(
        low, right, preferred_element_type=jnp.float32
    )


def own_kernel(counts, gates_ref, key_ref, value_ref, query_ref, *outs):
    heads = sum(counts)
    tokens = query_ref.shape[0]
    key_width, value_width = query_ref.shape[1] // heads, value_ref.shape[1] // heads
    level, _ = levels(gates_ref)
    causal = lax.broadcasted_iota(jnp.int32, (tokens, tokens), 0) >= lax.broadcasted_iota(
        jnp.int32, (tokens, tokens), 1
    )
    key_scale = key_width ** (-0.5)
    first = 0
    for total_ref, note_ref, count in zip(outs[::2], outs[1::2], counts):
        notes = []
        for head in range(first, first + count):
            keys = slice(head * key_width, (head + 1) * key_width)
            channels = slice(head * value_width, (head + 1) * value_width)
            out = slice((head - first) * value_width, (head - first + 1) * value_width)
            masked = jnp.where(causal, level[head : head + 1], -jnp.inf)
            top = jnp.max(masked, axis=1, keepdims=True)
            scores = times_transpose(query_ref[:, keys], key_ref[:, keys]) * key_scale
            scores = scores * jnp.exp(masked - top)
            total_ref[:, out] = two_term_dot(scores, value_ref[:, channels])
            notes += [jnp.sum(scores, axis=1, keepdims=True), top]
        note_ref[...] = to_lanes(notes, tokens)
        first += count


def join_kernel(counts, gates0_ref, key0_ref, *refs):
    chunks, heads = len(counts), sum(counts)
    values0, query_ref, refs = refs[:chunks], refs[chunks], refs[chunks + 1 :]
    tokens = query_ref.shape[0]
    key_width, value_width = query_ref.shape[1] // heads, values0[0].shape[1] // counts[0]
    block = lax.axis_index("sp")
    second = lax.rem(block, 2) == 1
    level0, end0 = levels(gates0_ref)
    top0 = jnp.max(level0, axis=1, keepdims=True)
    top0 = jnp.where(block == 1, jnp.maximum(top0, 0.0), top0)
    weight0 = jnp.exp(level0 - top0) * (key_width ** (-0.5))
    state = jnp.where(second, top0 + end0, jnp.where(block == 0, 0.0, -jnp.inf))
    shift = jnp.where(block == 3, end0, 0.0)
    first = 0
    for chunk, count in enumerate(counts):
        own_total, own_note, total_ref, note_ref = refs[chunk * 2 : chunk * 2 + 2] + refs[
            (chunks + chunk) * 2 : (chunks + chunk) * 2 + 2
        ]
        own = own_note[...]
        notes = []
        for head in range(first, first + count):
            pick = slice(head, head + 1)
            keys = slice(head * key_width, (head + 1) * key_width)
            place = head - first
            out = slice(place * value_width, (place + 1) * value_width)
            own_top = own[:, 2 * place + 1 : 2 * place + 2]
            top = jnp.maximum(own_top, state[pick])
            scale = jnp.exp(own_top - top)
            scale0 = jnp.where(second, jnp.exp(state[pick] - top), 0.0)
            scores = times_transpose(query_ref[:, keys], key0_ref[:, keys])
            scores = scores * weight0[pick] * scale0
            total_ref[:, out] = scale * own_total[:, out] + two_term_dot(
                scores, values0[chunk][:, out]
            )
            sums = scale * own[:, 2 * place : 2 * place + 1] + jnp.sum(
                scores, axis=1, keepdims=True
            )
            notes += [sums, top, shift[pick]]
        note_ref[...] = to_lanes(notes, tokens)
        first += count


def serve_kernel(
    counts, gates0_ref, key0_ref, value0_ref, gates_ref, key_ref, value_ref,
    near_ref, far_ref, next_ref, later_ref, score_ref,
):
    heads, count = sum(counts), counts[0]
    tokens = near_ref.shape[0]
    key_width, value_width = near_ref.shape[1] // heads, value_ref.shape[1] // heads
    level0, end0 = levels(gates0_ref)
    level1, end1 = levels(gates_ref)
    level = jnp.concatenate([level0, level1 - end0], axis=1)
    top = jnp.maximum(jnp.max(level, axis=1, keepdims=True), 0.0)
    weight = jnp.exp(level - top) * (key_width ** (-0.5))
    reach = top + end0 + end1
    next_notes, later_notes = [], []
    for head in range(heads):
        keys = slice(head * key_width, (head + 1) * key_width)
        key_both = jnp.concatenate([key0_ref[:, keys], key_ref[:, keys]], axis=0)
        rows = jnp.concatenate([near_ref[:, keys], far_ref[:, keys]], axis=0)
        scores = times_transpose(rows, key_both) * weight[head : head + 1]
        sums = jnp.sum(scores, axis=1, keepdims=True)
        scores = scores.astype(jnp.bfloat16)
        if head < count:
            channels = slice(head * value_width, (head + 1) * value_width)
            give(scores, value0_ref[:, channels], value_ref[:, channels], next_ref, later_ref, channels)
        else:
            place = head - count
            score_ref[:, place * 2 * tokens : (place + 1) * 2 * tokens] = scores
        terms = three_terms(reach[head : head + 1])
        next_notes += three_terms(sums[:tokens]) + terms
        later_notes += three_terms(sums[tokens:]) + terms
    next_ref[:, count * value_width :] = to_lanes(next_notes, tokens).astype(jnp.bfloat16)
    later_ref[:, count * value_width :] = to_lanes(later_notes, tokens).astype(jnp.bfloat16)


def give(scores, value0, value1, next_ref, later_ref, out):
    tokens = value1.shape[0]
    values = jnp.concatenate([value0, value1], axis=0)
    given = jnp.dot(scores, values, preferred_element_type=jnp.float32).astype(jnp.bfloat16)
    next_ref[:, out] = given[:tokens]
    later_ref[:, out] = given[tokens:]


def serve_rest_kernel(first, count, score_ref, value0_ref, value_ref, next_ref, later_ref):
    width = score_ref.shape[1] // count
    value_width = next_ref.shape[1] // count
    for place in range(count):
        channels = slice((first + place) * value_width, (first + place + 1) * value_width)
        out = slice(place * value_width, (place + 1) * value_width)
        scores = score_ref[:, place * width : (place + 1) * width]
        give(scores, value0_ref[:, out], value_ref[:, channels], next_ref, later_ref, out)


def gated_rows(heads, first, count, total_ref, note_ref, near_ref, far_ref, lanes, gate_ref):
    value_width = gate_ref.shape[1] // heads
    given = lax.axis_index("sp") >= 2
    own = note_ref[...]
    gated = []
    for place in range(count):
        out = slice(place * value_width, (place + 1) * value_width)
        channels = slice((first + place) * value_width, (first + place + 1) * value_width)
        at = 6 * (first + place)
        sums = lanes[:, at : at + 1] + lanes[:, at + 1 : at + 2] + lanes[:, at + 2 : at + 3]
        at += 3
        reach = lanes[:, at : at + 1] + lanes[:, at + 1 : at + 2] + lanes[:, at + 2 : at + 3]
        reach = reach + own[:, 3 * place + 2 : 3 * place + 3]
        top = own[:, 3 * place + 1 : 3 * place + 2]
        peak = jnp.where(given, jnp.maximum(top, reach), top)
        scale = jnp.exp(top - peak)
        scale_given = jnp.where(given, jnp.exp(reach - peak), 0.0)
        weight = scale * own[:, 3 * place : 3 * place + 1] + scale_given * sums
        inverse = 1.0 / jnp.maximum(jnp.abs(weight), 1.0)
        message = near_ref[:, out].astype(jnp.float32) + far_ref[:, out].astype(jnp.float32)
        cell = (scale * inverse) * total_ref[:, out] + (scale_given * inverse) * message
        hidden = cell.astype(jnp.bfloat16).astype(jnp.float32)
        gate = jax.nn.sigmoid(gate_ref[:, channels].astype(jnp.float32))
        gated.append((hidden * gate).astype(jnp.bfloat16))
    return jnp.concatenate(gated, axis=1)


def product(left, right):
    return jnp.dot(left, right, preferred_element_type=jnp.float32)


def first_kernel(counts, gate_ref, total_ref, note_ref, near_ref, far_ref, *refs):
    pieces, gated_ref, lane_ref, part_ref = refs[:-3], refs[-3], refs[-2], refs[-1]
    rows = gated_ref.shape[1]
    lanes = near_ref[:, rows:].astype(jnp.float32) + far_ref[:, rows:].astype(jnp.float32)
    lane_ref[...] = lanes
    gated = gated_rows(
        sum(counts), 0, counts[0], total_ref, note_ref, near_ref, far_ref, lanes, gate_ref
    )
    gated_ref[...] = gated
    width = pieces[0].shape[1]
    for place, piece in enumerate(pieces):
        part_ref[:, place * width : (place + 1) * width] = product(gated, piece[:rows, :])


def finish_kernel(
    counts, whole, last, gate_ref, total_ref, note_ref, near_ref, far_ref, gated_ref, lane_ref,
    part_ref, *refs,
):
    pieces, out_ref = refs[:-1], refs[-1]
    rows, device = gated_ref.shape[1], lax.axis_index("dp")
    width = pieces[0].shape[1]
    gated = gated_rows(
        sum(counts), counts[0], counts[1], total_ref, note_ref, near_ref, far_ref,
        lane_ref[...], gate_ref,
    )

    def put(masks, columns):
        mask = jnp.where(device & CORE, masks[1], masks[0])
        start = pl.multiple_of((device ^ mask) * width, width)
        out_ref[:, pl.ds(start, width)] = columns.astype(out_ref.dtype)

    for place, (masks, piece) in enumerate(zip(whole, pieces)):
        part = part_ref[:, place * width : (place + 1) * width]
        put(masks, part + product(gated, piece[rows:, :]))
    both = jnp.concatenate([gated_ref[...], gated], axis=1)
    for masks, piece in zip(last, pieces[len(whole) :]):
        put(masks, product(both, piece[...]))


def kernel_call(kernel, operands, outs, flops, limit):
    vmem = pl.BlockSpec(memory_space=pltpu.VMEM)
    size = sum(x.size * x.dtype.itemsize for x in (*operands, *outs))
    return pl.pallas_call(
        kernel,
        out_shape=outs,
        in_specs=[vmem] * len(operands),
        out_specs=[vmem] * len(outs),
        compiler_params=pltpu.CompilerParams(vmem_limit_bytes=limit * MIB),
        cost_estimate=pl.CostEstimate(flops=flops, bytes_accessed=size, transcendentals=0),
    )(*operands)


def block_body(queries, key_rows, values, out_gate, input_gate, forget_gate, out_weight):
    return block_steps(
        queries[0], key_rows[0], values[0], out_gate[0], input_gate[0], forget_gate[0], out_weight
    )[None]


def block_steps(query, key, value, gate, input_log, forget, out_weight):
    tokens, heads = query.shape[0], input_log.shape[0]
    key_width, value_width = query.shape[1] // heads, value.shape[1] // heads
    shape = jax.ShapeDtypeStruct
    device_count = lax.axis_size("dp")

    def swap(piece, bit):
        return lax.ppermute(piece, "dp", [(i, i ^ bit) for i in range(device_count)])

    (gates,) = kernel_call(
        gates_kernel, [input_log, forget], [shape((2 * heads, tokens), jnp.float32)], 0, 2
    )
    pair = [(0, 1), (2, 3)]
    first, rest = COUNTS
    split = first * value_width
    earlier = [lax.ppermute(gates, "sp", pair), lax.ppermute(key, "sp", pair)]
    values0 = [
        lax.ppermute(value[:, :split], "sp", pair), lax.ppermute(value[:, split:], "sp", pair)
    ]
    here = [gates, key, value]
    near = lax.ppermute(query, "sp", [(2, 1)])
    far = lax.ppermute(query, "sp", [(3, 1)])

    def cross(piece, even, odd):
        pairs = [(i, i ^ (odd if i & CORE else even)) for i in range(device_count)]
        return lax.ppermute(piece, "dp", pairs)

    side_a = cross(out_weight, XBIT, YBIT)
    side_b = cross(out_weight, YBIT, XBIT)
    corner = cross(side_a, YBIT, XBIT)
    whole = {
        (0, 0): out_weight,
        (CORE, CORE): swap(out_weight, CORE),
        (XBIT, YBIT): side_a,
        (YBIT | CORE, XBIT | CORE): swap(side_a, CORE),
        (YBIT, XBIT): side_b,
        (XBIT | CORE, YBIT | CORE): swap(side_b, CORE),
    }
    last = {
        (XBIT | YBIT,) * 2: corner,
        (XBIT | YBIT | CORE,) * 2: swap(corner, CORE),
    }

    work = 2 * tokens * tokens * (key_width + value_width)
    sums = [
        x
        for count in COUNTS
        for x in (
            shape((tokens, count * value_width), jnp.float32),
            shape((tokens, LANES), jnp.float32),
        )
    ]
    own = kernel_call(
        functools.partial(own_kernel, COUNTS), [*here, query], sums, 3 * heads * work // 2, 8
    )
    message = shape((tokens, first * value_width + LANES), jnp.bfloat16)
    given_next, given_later, scores = kernel_call(
        functools.partial(serve_kernel, COUNTS),
        [*earlier, values0[0], *here, near, far],
        [message, message, shape((2 * tokens, rest * 2 * tokens), jnp.bfloat16)],
        4 * heads * work,
        8,
    )
    message = shape((tokens, rest * value_width), jnp.bfloat16)
    rest_next, rest_later = kernel_call(
        functools.partial(serve_rest_kernel, first, rest),
        [scores, values0[1], value],
        [message] * 2,
        2 * rest * work,
        8,
    )
    nears = [lax.ppermute(given_next, "sp", [(1, 2)]), lax.ppermute(rest_next, "sp", [(1, 2)])]
    fars = [lax.ppermute(given_later, "sp", [(1, 3)]), lax.ppermute(rest_later, "sp", [(1, 3)])]
    home = kernel_call(
        functools.partial(join_kernel, COUNTS),
        [*earlier, *values0, query, *own],
        sums,
        3 * heads * work // 2,
        8,
    )
    width = out_weight.shape[1]
    kept = kernel_call(
        functools.partial(first_kernel, COUNTS),
        [gate, *home[:2], nears[0], fars[0], *whole.values()],
        [
            shape((tokens, first * value_width), jnp.bfloat16),
            shape((tokens, LANES), jnp.float32),
            shape((tokens, len(whole) * width), jnp.float32),
        ],
        2 * tokens * first * value_width * len(whole) * width,
        10,
    )
    (out,) = kernel_call(
        functools.partial(finish_kernel, COUNTS, tuple(whole), tuple(last)),
        [
            gate, *home[2:], nears[1], fars[1], *kept, *whole.values(),
            *last.values(),
        ],
        [shape((tokens, width * device_count), jnp.bfloat16)],
        2 * tokens * rest * value_width * width * device_count,
        12,
    )
    return out


def body(queries, key_rows, values, out_gate, input_gate, forget_gate, out_weight):
    group_count = lax.axis_size("sp")
    token_count = queries.shape[1]
    head_count = input_gate.shape[1]
    copies = group_count // head_count
    head_key = queries.shape[2] // head_count
    slice_width = values.shape[2] // group_count

    def spread(source):
        widened = jnp.broadcast_to(
            source[0].reshape(token_count, head_count, 1, head_key),
            (token_count, head_count, copies, head_key),
        )
        return widened.reshape(token_count, group_count, head_key)

    def spread_gate(source):
        return jnp.repeat(source[0].T, copies, axis=1)

    query_all, key_all = (
        lax.all_to_all(spread(queries), "sp", split_axis=1, concat_axis=0, tiled=True),
        lax.all_to_all(spread(key_rows), "sp", split_axis=1, concat_axis=0, tiled=True),
    )
    value_all, input_all, forget_all = (
        lax.all_to_all(
            values[0].reshape(token_count, group_count, slice_width),
            "sp",
            split_axis=1,
            concat_axis=0,
            tiled=True,
        ),
        lax.all_to_all(spread_gate(input_gate), "sp", split_axis=1, concat_axis=0, tiled=True),
        lax.all_to_all(spread_gate(forget_gate), "sp", split_axis=1, concat_axis=0, tiled=True),
    )
    output = memory_cell(
        query_all[:, 0],
        key_all[:, 0],
        value_all[:, 0],
        input_all[:, 0].astype(jnp.float32),
        jax.nn.log_sigmoid(forget_all[:, 0].astype(jnp.float32)),
    )
    hidden = output.astype(jnp.bfloat16)
    token_rows = lax.all_to_all(hidden, "sp", split_axis=0, concat_axis=1, tiled=True)
    gated_rows = (
        token_rows.astype(jnp.float32) * jax.nn.sigmoid(out_gate[0].astype(jnp.float32))
    ).astype(jnp.bfloat16)
    projected = jnp.dot(
        gated_rows,
        lax.all_gather(out_weight, "dp", axis=1, tiled=True),
        preferred_element_type=jnp.float32,
    )
    return projected.astype(jnp.bfloat16)[None]


def solution(mesh):
    blocks = mesh.shape["sp"] == 4 and mesh.shape["dp"] == 8
    return jax.shard_map(
        block_body if blocks else body,
        mesh=mesh,
        in_specs=(
            P("dp", "sp", None),
            P("dp", "sp", None),
            P("dp", "sp", None),
            P("dp", "sp", None),
            P("dp", None, "sp"),
            P("dp", None, "sp"),
            P(None, "dp"),
        ),
        out_specs=P("dp", "sp", None),
        check_vma=False,
    )
```

```python
import functools

import jax
import jax.numpy as jnp
from jax import lax
from jax.experimental import pallas as pl
from jax.experimental.pallas import tpu as pltpu
from jax.sharding import PartitionSpec as P


BLOCK = 128


def memory_cell(query_rows, key_in, value_rows, input_log, forget_log):
    block_count = query_rows.shape[0] // BLOCK
    key_width = query_rows.shape[1]
    value_width = value_rows.shape[1]
    key_scale = key_width ** (-0.5)
    causal = lax.broadcasted_iota(jnp.int32, (BLOCK, BLOCK), 0) >= lax.broadcasted_iota(
        jnp.int32, (BLOCK, BLOCK), 1
    )
    highest = lax.Precision.HIGHEST

    def block_step(state_in, inputs):
        memory, normer, stabil = state_in
        query_part, key_part, value_part, gain_part, decay_part = inputs
        query_part = query_part.astype(jnp.float32)
        key_part = key_part.astype(jnp.float32) * key_scale
        value_part = value_part.astype(jnp.float32)
        running = jnp.cumsum(decay_part)
        log_weight = running[:, None] - running[None, :] + gain_part[None, :]
        log_weight = jnp.where(causal, log_weight, -jnp.inf)
        carried_log = running + stabil
        row_top = jnp.maximum(carried_log, jnp.max(log_weight, axis=1))
        scores = jnp.dot(query_part, key_part.T, precision=highest) * jnp.exp(
            log_weight - row_top[:, None]
        )
        carried = jnp.exp(carried_log - row_top)
        numerator = jnp.dot(scores, value_part, precision=highest) + carried[:, None] * jnp.dot(
            query_part, memory, precision=highest
        )
        denominator = jnp.sum(scores, axis=1) + carried * jnp.dot(
            query_part, normer, precision=highest
        )
        output = numerator / jnp.maximum(jnp.abs(denominator), 1.0)[:, None]
        block_end = running[-1]
        weight_log = block_end - running + gain_part
        new_top = jnp.maximum(block_end + stabil, jnp.max(weight_log))
        weights = jnp.exp(weight_log - new_top)
        retain = jnp.exp(block_end + stabil - new_top)
        memory = retain * memory + jnp.dot(
            (key_part * weights[:, None]).T, value_part, precision=highest
        )
        normer = retain * normer + jnp.dot(weights, key_part, precision=highest)
        return ((memory, normer, new_top), output)

    start_state = (
        jnp.zeros((key_width, value_width), jnp.float32),
        jnp.zeros((key_width,), jnp.float32),
        jnp.zeros((), jnp.float32),
    )
    blocks = tuple(
        (
            source.reshape((block_count, BLOCK) + source.shape[1:])
            for source in (query_rows, key_in, value_rows, input_log, forget_log)
        )
    )
    _, outputs = lax.scan(block_step, start_state, blocks)
    return outputs.reshape(block_count * BLOCK, value_width)


LANES = 128


def log_forget(gates):
    return -jnp.log1p(jnp.exp(-gates))


def running_sum(rows):
    width = rows.shape[1]
    upto = lax.broadcasted_iota(jnp.int32, (width, width), 0) <= lax.broadcasted_iota(
        jnp.int32, (width, width), 1
    )
    return jnp.dot(
        rows,
        upto.astype(jnp.float32),
        precision=lax.Precision.HIGHEST,
        preferred_element_type=jnp.float32,
    )


def times_transpose(left, right):
    return lax.dot_general(
        left, right, (((1,), (1,)), ((), ())), preferred_element_type=jnp.float32
    )


def three_terms(value):
    high = value.astype(jnp.bfloat16).astype(jnp.float32)
    middle = (value - high).astype(jnp.bfloat16).astype(jnp.float32)
    return [high, middle, value - high - middle]


def to_lanes(columns, rows):
    lane = lax.broadcasted_iota(jnp.int32, (rows, LANES), 1)
    tile = jnp.zeros((rows, LANES), jnp.float32)
    for place, column in enumerate(columns):
        tile = jnp.where(lane == place, column, tile)
    return tile


MIB = 1 << 20
CORE, XBIT, YBIT = 1, 2, 4


def gate_levels(payloads, tokens):
    gates = [payload[tokens:, :tokens].astype(jnp.float32) for payload in payloads]
    heads = gates[0].shape[0] // 2
    running = running_sum(log_forget(jnp.concatenate([g[heads:] for g in gates], axis=0)))
    parts = []
    for place, gate in enumerate(gates):
        sums = running[place * heads : (place + 1) * heads]
        parts.append((gate[:heads] - sums, sums[:, tokens - 1 :]))
    return parts


def two_term_dot(left, right):
    high = left.astype(jnp.bfloat16)
    low = (left - high.astype(jnp.float32)).astype(jnp.bfloat16)
    return jnp.dot(high, right, preferred_element_type=jnp.float32) + jnp.dot(
        low, right, preferred_element_type=jnp.float32
    )


def half_slices(place, key_width, value_width, count):
    start = count * key_width + place * value_width
    return (
        slice(place * key_width, (place + 1) * key_width),
        slice(start, start + value_width),
        slice(place * value_width, (place + 1) * value_width),
    )


def own_kernel(count, low_ref, high_ref, query_ref, *outs):
    tokens, key_width = query_ref.shape[0], query_ref.shape[1] // (2 * count)
    value_width = low_ref.shape[1] // count - key_width
    ((level, _),) = gate_levels([low_ref], tokens)
    causal = lax.broadcasted_iota(jnp.int32, (tokens, tokens), 0) >= lax.broadcasted_iota(
        jnp.int32, (tokens, tokens), 1
    )
    for half, payload in enumerate((low_ref, high_ref)):
        total_ref, note_ref = outs[2 * half : 2 * half + 2]
        notes = []
        for place in range(count):
            head = half * count + place
            keys, channels, out = half_slices(place, key_width, value_width, count)
            masked = jnp.where(causal, level[head : head + 1], -jnp.inf)
            top = jnp.max(masked, axis=1, keepdims=True)
            rows = query_ref[:, head * key_width : (head + 1) * key_width]
            scores = times_transpose(rows, payload[:tokens, keys]) * (key_width ** (-0.5))
            scores = scores * jnp.exp(masked - top)
            total_ref[:, out] = two_term_dot(scores, payload[:tokens, channels])
            notes += [jnp.sum(scores, axis=1, keepdims=True), top]
        note_ref[...] = to_lanes(notes, tokens)


def join_kernel(count, pair_ref, before_ref, last_ref, query_ref, *refs):
    tokens, key_width = query_ref.shape[0], query_ref.shape[1] // (2 * count)
    value_width = pair_ref.shape[1] // count - key_width
    block = lax.axis_index("sp")
    second, both = lax.rem(block, 2) == 1, block == 2
    upper = (block == 1) | both
    start = jnp.where(block == 0, 0.0, -jnp.inf)
    (level, end), (level0, end0), (level1, end1) = gate_levels(
        [pair_ref, before_ref, last_ref], tokens
    )
    top = jnp.max(level, axis=1, keepdims=True)
    top = jnp.where(block == 1, jnp.maximum(top, 0.0), top)
    end0 = jnp.where(both, end0, 0.0)
    level1 = level1 - end0
    top1 = jnp.maximum(jnp.max(level1, axis=1, keepdims=True), 0.0)
    top1 = jnp.where(both, jnp.maximum(top1, jnp.max(level0, axis=1, keepdims=True)), top1)
    weight0 = jnp.where(both, jnp.exp(level0 - top1), 0.0)
    cases = (
        (
            [pair_ref],
            jnp.exp(level - top),
            second,
            jnp.where(second, top + end, start),
            jnp.where(block == 3, end, 0.0),
        ),
        (
            [before_ref, last_ref],
            jnp.concatenate([weight0, jnp.exp(level1 - top1)], axis=1),
            upper,
            jnp.where(upper, top1 + end0 + end1, start),
            jnp.zeros_like(end),
        ),
    )
    for half, (payloads, weight, valid, state, shift) in enumerate(cases):
        own_total, own_note, total_ref, note_ref = (
            refs[2 * half], refs[2 * half + 1], refs[2 * half + 4], refs[2 * half + 5]
        )
        own = own_note[...]
        notes = []
        for place in range(count):
            head = half * count + place
            pick = slice(head, head + 1)
            keys, channels, out = half_slices(place, key_width, value_width, count)
            own_top = own[:, 2 * place + 1 : 2 * place + 2]
            peak = jnp.maximum(own_top, state[pick])
            scale = jnp.exp(own_top - peak)
            scale0 = jnp.where(valid, jnp.exp(state[pick] - peak), 0.0) * (key_width ** (-0.5))
            key_all = jnp.concatenate([p[:tokens, keys] for p in payloads], axis=0)
            value_all = jnp.concatenate([p[:tokens, channels] for p in payloads], axis=0)
            rows = query_ref[:, head * key_width : (head + 1) * key_width]
            scores = times_transpose(rows, key_all) * weight[pick] * scale0
            total_ref[:, out] = scale * own_total[:, out] + two_term_dot(scores, value_all)
            sums = scale * own[:, 2 * place : 2 * place + 1] + jnp.sum(
                scores, axis=1, keepdims=True
            )
            notes += [sums, peak, shift[pick]]
        note_ref[...] = to_lanes(notes, tokens)


def answer(count, half, payloads, rows_refs, out_refs):
    tokens, key_width = rows_refs[0].shape[0], rows_refs[0].shape[1] // (2 * count)
    value_width = payloads[0].shape[1] // count - key_width
    levels, shift = [], 0.0
    for level, end in gate_levels(payloads, tokens):
        levels.append(level - shift)
        shift = shift + end
    level = jnp.concatenate(levels, axis=1)
    top = jnp.maximum(jnp.max(level, axis=1, keepdims=True), 0.0)
    weight = jnp.exp(level - top) * (key_width ** (-0.5))
    reach = top + shift
    notes = [[] for _ in out_refs]
    for place in range(count):
        pick = slice(half * count + place, half * count + place + 1)
        keys, channels, out = half_slices(place, key_width, value_width, count)
        key_all = jnp.concatenate([p[:tokens, keys] for p in payloads], axis=0)
        value_all = jnp.concatenate([p[:tokens, channels] for p in payloads], axis=0)
        columns = slice(pick.start * key_width, pick.stop * key_width)
        rows = jnp.concatenate([ref[:, columns] for ref in rows_refs], axis=0)
        scores = times_transpose(rows, key_all) * weight[pick]
        sums = jnp.sum(scores, axis=1, keepdims=True)
        given = product(scores.astype(jnp.bfloat16), value_all).astype(jnp.bfloat16)
        for i, ref in enumerate(out_refs):
            here = slice(i * tokens, (i + 1) * tokens)
            ref[:, out] = given[here]
            notes[i] += three_terms(sums[here]) + three_terms(reach[pick])
    for ref, note in zip(out_refs, notes):
        ref[:, count * value_width :] = to_lanes(note, tokens).astype(jnp.bfloat16)


def serve_low_kernel(count, pair_ref, low_ref, near_ref, far_ref, next_ref, later_ref):
    answer(count, 0, [pair_ref, low_ref], [near_ref, far_ref], [next_ref, later_ref])


def serve_high_kernel(count, before_ref, last_ref, high_ref, near_ref, next_ref):
    answer(count, 1, [before_ref, last_ref, high_ref], [near_ref], [next_ref])


def gated_rows(count, half, given, message, total_ref, note_ref, gate_ref):
    value_width = total_ref.shape[1] // count
    own = note_ref[...]
    lanes = message(slice(count * value_width, count * value_width + LANES))
    gated = []
    for place in range(count):
        out = slice(place * value_width, (place + 1) * value_width)
        start = (half * count + place) * value_width
        at = 6 * place
        sums = lanes[:, at : at + 1] + lanes[:, at + 1 : at + 2] + lanes[:, at + 2 : at + 3]
        at += 3
        reach = lanes[:, at : at + 1] + lanes[:, at + 1 : at + 2] + lanes[:, at + 2 : at + 3]
        reach = reach + own[:, 3 * place + 2 : 3 * place + 3]
        top = own[:, 3 * place + 1 : 3 * place + 2]
        peak = jnp.where(given, jnp.maximum(top, reach), top)
        scale = jnp.exp(top - peak)
        scale_given = jnp.where(given, jnp.exp(reach - peak), 0.0)
        weight = scale * own[:, 3 * place : 3 * place + 1] + scale_given * sums
        inverse = 1.0 / jnp.maximum(jnp.abs(weight), 1.0)
        cell = (scale * inverse) * total_ref[:, out] + (scale_given * inverse) * message(out)
        hidden = cell.astype(jnp.bfloat16).astype(jnp.float32)
        gate = jax.nn.sigmoid(gate_ref[:, start : start + value_width].astype(jnp.float32))
        gated.append((hidden * gate).astype(jnp.bfloat16))
    return jnp.concatenate(gated, axis=1)


def product(left, right):
    return jnp.dot(left, right, preferred_element_type=jnp.float32)


def first_kernel(count, gate_ref, total_ref, note_ref, next_ref, *refs):
    pieces, gated_ref, part_ref = refs[:-2], refs[-2], refs[-1]
    rows = gated_ref.shape[1]

    def message(columns):
        return next_ref[:, columns].astype(jnp.float32)

    given = lax.axis_index("sp") == 3
    gated = gated_rows(count, 1, given, message, total_ref, note_ref, gate_ref)
    gated_ref[...] = gated
    width = pieces[0].shape[1]
    for place, piece in enumerate(pieces):
        part_ref[:, place * width : (place + 1) * width] = product(gated, piece[rows:, :])


def finish_kernel(
    count, whole, last, gate_ref, total_ref, note_ref, next_ref, later_ref, gated_ref, part_ref, *refs
):
    pieces, out_ref = refs[:-1], refs[-1]
    rows, device = gated_ref.shape[1], lax.axis_index("dp")
    width = pieces[0].shape[1]

    def message(columns):
        return next_ref[:, columns].astype(jnp.float32) + later_ref[:, columns].astype(jnp.float32)

    gated = gated_rows(count, 0, lax.axis_index("sp") >= 2, message, total_ref, note_ref, gate_ref)

    def put(masks, columns):
        mask = jnp.where(device & CORE, masks[1], masks[0])
        start = pl.multiple_of((device ^ mask) * width, width)
        out_ref[:, pl.ds(start, width)] = columns.astype(out_ref.dtype)

    for place, (masks, piece) in enumerate(zip(whole, pieces)):
        part = part_ref[:, place * width : (place + 1) * width]
        put(masks, part + product(gated, piece[:rows, :]))
    both = jnp.concatenate([gated, gated_ref[...]], axis=1)
    for masks, piece in zip(last, pieces[len(whole) :]):
        put(masks, product(both, piece[...]))


def kernel_call(kernel, operands, outs, flops, limit):
    vmem = pl.BlockSpec(memory_space=pltpu.VMEM)
    size = sum(x.size * x.dtype.itemsize for x in (*operands, *outs))
    return pl.pallas_call(
        kernel,
        out_shape=outs,
        in_specs=[vmem] * len(operands),
        out_specs=[vmem] * len(outs),
        compiler_params=pltpu.CompilerParams(vmem_limit_bytes=limit * MIB),
        cost_estimate=pl.CostEstimate(flops=flops, bytes_accessed=size, transcendentals=0),
    )(*operands)


def block_body(queries, key_rows, values, out_gate, input_gate, forget_gate, out_weight):
    return block_steps(
        queries[0], key_rows[0], values[0], out_gate[0], input_gate[0], forget_gate[0], out_weight
    )[None]


def block_steps(query, key, value, gate, input_log, forget, out_weight):
    tokens, heads = query.shape[0], input_log.shape[0]
    key_width, value_width = query.shape[1] // heads, value.shape[1] // heads
    shape = jax.ShapeDtypeStruct
    device_count = lax.axis_size("dp")

    def swap(piece, bit):
        return lax.ppermute(piece, "dp", [(i, i ^ bit) for i in range(device_count)])

    count = heads // 2
    gates = jnp.concatenate([input_log, forget], axis=0)

    def payload(half):
        wide = key.shape[1] // 2
        tall = value.shape[1] // 2
        parts = [
            key[:, half * wide : (half + 1) * wide],
            value[:, half * tall : (half + 1) * tall],
        ]
        below = jnp.pad(gates, ((0, 0), (0, wide + tall - tokens)))
        return jnp.concatenate([jnp.concatenate(parts, axis=1), below], axis=0)

    high = payload(1)
    low = payload(0)
    last = lax.ppermute(high, "sp", [(0, 1), (1, 2)])
    near = lax.ppermute(query, "sp", [(2, 1), (3, 2)])
    far = lax.ppermute(query, "sp", [(3, 1)])
    pair = lax.ppermute(low, "sp", [(0, 1), (2, 3)])
    before = lax.ppermute(last, "sp", [(1, 2)])

    def cross(piece, even, odd):
        pairs = [(i, i ^ (odd if i & CORE else even)) for i in range(device_count)]
        return lax.ppermute(piece, "dp", pairs)

    side_a = cross(out_weight, XBIT, YBIT)
    side_b = cross(out_weight, YBIT, XBIT)
    corner = cross(side_a, YBIT, XBIT)
    whole = {
        (0, 0): out_weight,
        (CORE, CORE): swap(out_weight, CORE),
        (XBIT, YBIT): side_a,
        (YBIT | CORE, XBIT | CORE): swap(side_a, CORE),
        (YBIT, XBIT): side_b,
        (XBIT | CORE, YBIT | CORE): swap(side_b, CORE),
    }
    corners = {
        (XBIT | YBIT,) * 2: corner,
        (XBIT | YBIT | CORE,) * 2: swap(corner, CORE),
    }

    work = 2 * tokens * tokens * (key_width + value_width)
    sums = [
        shape((tokens, count * value_width), jnp.float32),
        shape((tokens, LANES), jnp.float32),
    ] * 2
    own = kernel_call(
        functools.partial(own_kernel, count), [low, high, query], sums, 3 * heads * work // 2, 8
    )
    message = shape((tokens, count * value_width + LANES), jnp.bfloat16)
    given_next, given_later = kernel_call(
        functools.partial(serve_low_kernel, count),
        [pair, low, near, far],
        [message] * 2,
        4 * count * work,
        8,
    )
    (given_high,) = kernel_call(
        functools.partial(serve_high_kernel, count),
        [before, last, high, near],
        [message],
        3 * count * work,
        8,
    )
    from_next = lax.ppermute(given_next, "sp", [(1, 2)])
    from_later = lax.ppermute(given_later, "sp", [(1, 3)])
    from_high = lax.ppermute(given_high, "sp", [(2, 3)])
    home = kernel_call(
        functools.partial(join_kernel, count),
        [pair, before, last, query, *own],
        sums,
        3 * heads * work // 2,
        8,
    )
    width = out_weight.shape[1]
    kept = kernel_call(
        functools.partial(first_kernel, count),
        [gate, *home[2:], from_high, *whole.values()],
        [
            shape((tokens, count * value_width), jnp.bfloat16),
            shape((tokens, len(whole) * width), jnp.float32),
        ],
        2 * tokens * count * value_width * len(whole) * width,
        10,
    )
    (out,) = kernel_call(
        functools.partial(finish_kernel, count, tuple(whole), tuple(corners)),
        [gate, *home[:2], from_next, from_later, *kept, *whole.values(), *corners.values()],
        [shape((tokens, width * device_count), jnp.bfloat16)],
        2 * tokens * count * value_width * width * device_count,
        12,
    )
    return out


def body(queries, key_rows, values, out_gate, input_gate, forget_gate, out_weight):
    group_count = lax.axis_size("sp")
    token_count = queries.shape[1]
    head_count = input_gate.shape[1]
    copies = group_count // head_count
    head_key = queries.shape[2] // head_count
    slice_width = values.shape[2] // group_count

    def spread(source):
        widened = jnp.broadcast_to(
            source[0].reshape(token_count, head_count, 1, head_key),
            (token_count, head_count, copies, head_key),
        )
        return widened.reshape(token_count, group_count, head_key)

    def spread_gate(source):
        return jnp.repeat(source[0].T, copies, axis=1)

    query_all, key_all = (
        lax.all_to_all(spread(queries), "sp", split_axis=1, concat_axis=0, tiled=True),
        lax.all_to_all(spread(key_rows), "sp", split_axis=1, concat_axis=0, tiled=True),
    )
    value_all, input_all, forget_all = (
        lax.all_to_all(
            values[0].reshape(token_count, group_count, slice_width),
            "sp",
            split_axis=1,
            concat_axis=0,
            tiled=True,
        ),
        lax.all_to_all(spread_gate(input_gate), "sp", split_axis=1, concat_axis=0, tiled=True),
        lax.all_to_all(spread_gate(forget_gate), "sp", split_axis=1, concat_axis=0, tiled=True),
    )
    output = memory_cell(
        query_all[:, 0],
        key_all[:, 0],
        value_all[:, 0],
        input_all[:, 0].astype(jnp.float32),
        jax.nn.log_sigmoid(forget_all[:, 0].astype(jnp.float32)),
    )
    hidden = output.astype(jnp.bfloat16)
    token_rows = lax.all_to_all(hidden, "sp", split_axis=0, concat_axis=1, tiled=True)
    gated_rows = (
        token_rows.astype(jnp.float32) * jax.nn.sigmoid(out_gate[0].astype(jnp.float32))
    ).astype(jnp.bfloat16)
    projected = jnp.dot(
        gated_rows,
        lax.all_gather(out_weight, "dp", axis=1, tiled=True),
        preferred_element_type=jnp.float32,
    )
    return projected.astype(jnp.bfloat16)[None]


def solution(mesh):
    blocks = mesh.shape["sp"] == 4 and mesh.shape["dp"] == 8
    return jax.shard_map(
        block_body if blocks else body,
        mesh=mesh,
        in_specs=(
            P("dp", "sp", None),
            P("dp", "sp", None),
            P("dp", "sp", None),
            P("dp", "sp", None),
            P("dp", None, "sp"),
            P("dp", None, "sp"),
            P(None, "dp"),
        ),
        out_specs=P("dp", "sp", None),
        check_vma=False,
    )
```

```python
import functools

import jax
import jax.numpy as jnp
from jax import lax
from jax.experimental import pallas as pl
from jax.experimental.pallas import tpu as pltpu
from jax.sharding import PartitionSpec as P


BLOCK = 128


def memory_cell(query_rows, key_in, value_rows, input_log, forget_log):
    block_count = query_rows.shape[0] // BLOCK
    key_width = query_rows.shape[1]
    value_width = value_rows.shape[1]
    key_scale = key_width ** (-0.5)
    causal = lax.broadcasted_iota(jnp.int32, (BLOCK, BLOCK), 0) >= lax.broadcasted_iota(
        jnp.int32, (BLOCK, BLOCK), 1
    )
    highest = lax.Precision.HIGHEST

    def block_step(state_in, inputs):
        memory, normer, stabil = state_in
        query_part, key_part, value_part, gain_part, decay_part = inputs
        query_part = query_part.astype(jnp.float32)
        key_part = key_part.astype(jnp.float32) * key_scale
        value_part = value_part.astype(jnp.float32)
        running = jnp.cumsum(decay_part)
        log_weight = running[:, None] - running[None, :] + gain_part[None, :]
        log_weight = jnp.where(causal, log_weight, -jnp.inf)
        carried_log = running + stabil
        row_top = jnp.maximum(carried_log, jnp.max(log_weight, axis=1))
        scores = jnp.dot(query_part, key_part.T, precision=highest) * jnp.exp(
            log_weight - row_top[:, None]
        )
        carried = jnp.exp(carried_log - row_top)
        numerator = jnp.dot(scores, value_part, precision=highest) + carried[:, None] * jnp.dot(
            query_part, memory, precision=highest
        )
        denominator = jnp.sum(scores, axis=1) + carried * jnp.dot(
            query_part, normer, precision=highest
        )
        output = numerator / jnp.maximum(jnp.abs(denominator), 1.0)[:, None]
        block_end = running[-1]
        weight_log = block_end - running + gain_part
        new_top = jnp.maximum(block_end + stabil, jnp.max(weight_log))
        weights = jnp.exp(weight_log - new_top)
        retain = jnp.exp(block_end + stabil - new_top)
        memory = retain * memory + jnp.dot(
            (key_part * weights[:, None]).T, value_part, precision=highest
        )
        normer = retain * normer + jnp.dot(weights, key_part, precision=highest)
        return ((memory, normer, new_top), output)

    start_state = (
        jnp.zeros((key_width, value_width), jnp.float32),
        jnp.zeros((key_width,), jnp.float32),
        jnp.zeros((), jnp.float32),
    )
    blocks = tuple(
        (
            source.reshape((block_count, BLOCK) + source.shape[1:])
            for source in (query_rows, key_in, value_rows, input_log, forget_log)
        )
    )
    _, outputs = lax.scan(block_step, start_state, blocks)
    return outputs.reshape(block_count * BLOCK, value_width)


LANES = 128


def log_forget(gates):
    return -jnp.log1p(jnp.exp(-gates))


def running_sum(rows):
    width = rows.shape[1]
    upto = lax.broadcasted_iota(jnp.int32, (width, width), 0) <= lax.broadcasted_iota(
        jnp.int32, (width, width), 1
    )
    return jnp.dot(
        rows,
        upto.astype(jnp.float32),
        precision=lax.Precision.HIGHEST,
        preferred_element_type=jnp.float32,
    )


def times_transpose(left, right):
    return lax.dot_general(
        left, right, (((1,), (1,)), ((), ())), preferred_element_type=jnp.float32
    )


def three_terms(value):
    high = value.astype(jnp.bfloat16).astype(jnp.float32)
    middle = (value - high).astype(jnp.bfloat16).astype(jnp.float32)
    return [high, middle, value - high - middle]


def to_lanes(columns, rows):
    lane = lax.broadcasted_iota(jnp.int32, (rows, LANES), 1)
    tile = jnp.zeros((rows, LANES), jnp.float32)
    for place, column in enumerate(columns):
        tile = jnp.where(lane == place, column, tile)
    return tile


MIB = 1 << 20
CORE, XBIT, YBIT = 1, 2, 4


def gate_levels(payloads, tokens):
    gates = [payload[tokens:, :tokens].astype(jnp.float32) for payload in payloads]
    heads = gates[0].shape[0] // 2
    running = running_sum(log_forget(jnp.concatenate([g[heads:] for g in gates], axis=0)))
    parts = []
    for place, gate in enumerate(gates):
        sums = running[place * heads : (place + 1) * heads]
        parts.append((gate[:heads] - sums, sums[:, tokens - 1 :]))
    return parts


def two_term_dot(left, right):
    high = left.astype(jnp.bfloat16)
    low = (left - high.astype(jnp.float32)).astype(jnp.bfloat16)
    return jnp.dot(high, right, preferred_element_type=jnp.float32) + jnp.dot(
        low, right, preferred_element_type=jnp.float32
    )


def half_slices(place, key_width, value_width, count):
    start = count * key_width + place * value_width
    return (
        slice(place * key_width, (place + 1) * key_width),
        slice(start, start + value_width),
        slice(place * value_width, (place + 1) * value_width),
    )


def own_kernel(count, low_ref, high_ref, query_ref, *outs):
    tokens, key_width = query_ref.shape[0], query_ref.shape[1] // (2 * count)
    value_width = low_ref.shape[1] // count - key_width
    ((level, _),) = gate_levels([low_ref], tokens)
    causal = lax.broadcasted_iota(jnp.int32, (tokens, tokens), 0) >= lax.broadcasted_iota(
        jnp.int32, (tokens, tokens), 1
    )
    for half, payload in enumerate((low_ref, high_ref)):
        total_ref, note_ref = outs[2 * half : 2 * half + 2]
        notes = []
        for place in range(count):
            head = half * count + place
            keys, channels, out = half_slices(place, key_width, value_width, count)
            masked = jnp.where(causal, level[head : head + 1], -jnp.inf)
            top = jnp.max(masked, axis=1, keepdims=True)
            rows = query_ref[:, head * key_width : (head + 1) * key_width]
            scores = times_transpose(rows, payload[:tokens, keys]) * (key_width ** (-0.5))
            scores = scores * jnp.exp(masked - top)
            total_ref[:, out] = two_term_dot(scores, payload[:tokens, channels])
            notes += [jnp.sum(scores, axis=1, keepdims=True), top]
        note_ref[...] = to_lanes(notes, tokens)


def join_kernel(count, pair_ref, before_ref, last_ref, query_ref, *refs):
    tokens, key_width = query_ref.shape[0], query_ref.shape[1] // (2 * count)
    value_width = pair_ref.shape[1] // count - key_width
    block = lax.axis_index("sp")
    second, both = lax.rem(block, 2) == 1, block == 2
    upper = (block == 1) | both
    start = jnp.where(block == 0, 0.0, -jnp.inf)
    (level, end), (level0, end0), (level1, end1) = gate_levels(
        [pair_ref, before_ref, last_ref], tokens
    )
    top = jnp.max(level, axis=1, keepdims=True)
    top = jnp.where(block == 1, jnp.maximum(top, 0.0), top)
    end0 = jnp.where(both, end0, 0.0)
    level1 = level1 - end0
    top1 = jnp.maximum(jnp.max(level1, axis=1, keepdims=True), 0.0)
    top1 = jnp.where(both, jnp.maximum(top1, jnp.max(level0, axis=1, keepdims=True)), top1)
    weight0 = jnp.where(both, jnp.exp(level0 - top1), 0.0)
    cases = (
        (
            [pair_ref],
            jnp.exp(level - top),
            second,
            jnp.where(second, top + end, start),
            jnp.where(block == 3, end, 0.0),
        ),
        (
            [before_ref, last_ref],
            jnp.concatenate([weight0, jnp.exp(level1 - top1)], axis=1),
            upper,
            jnp.where(upper, top1 + end0 + end1, start),
            jnp.zeros_like(end),
        ),
    )
    for half, (payloads, weight, valid, state, shift) in enumerate(cases):
        own_total, own_note, total_ref, note_ref = (
            refs[2 * half], refs[2 * half + 1], refs[2 * half + 4], refs[2 * half + 5]
        )
        own = own_note[...]
        notes = []
        for place in range(count):
            head = half * count + place
            pick = slice(head, head + 1)
            keys, channels, out = half_slices(place, key_width, value_width, count)
            own_top = own[:, 2 * place + 1 : 2 * place + 2]
            peak = jnp.maximum(own_top, state[pick])
            scale = jnp.exp(own_top - peak)
            scale0 = jnp.where(valid, jnp.exp(state[pick] - peak), 0.0) * (key_width ** (-0.5))
            key_all = jnp.concatenate([p[:tokens, keys] for p in payloads], axis=0)
            value_all = jnp.concatenate([p[:tokens, channels] for p in payloads], axis=0)
            rows = query_ref[:, head * key_width : (head + 1) * key_width]
            scores = times_transpose(rows, key_all) * weight[pick] * scale0
            total_ref[:, out] = scale * own_total[:, out] + two_term_dot(scores, value_all)
            sums = scale * own[:, 2 * place : 2 * place + 1] + jnp.sum(
                scores, axis=1, keepdims=True
            )
            notes += [sums, peak, shift[pick]]
        note_ref[...] = to_lanes(notes, tokens)


def answer(count, half, payloads, rows_refs, out_refs):
    tokens, key_width = rows_refs[0].shape[0], rows_refs[0].shape[1] // (2 * count)
    value_width = payloads[0].shape[1] // count - key_width
    levels, shift = [], 0.0
    for level, end in gate_levels(payloads, tokens):
        levels.append(level - shift)
        shift = shift + end
    level = jnp.concatenate(levels, axis=1)
    top = jnp.maximum(jnp.max(level, axis=1, keepdims=True), 0.0)
    weight = jnp.exp(level - top) * (key_width ** (-0.5))
    reach = top + shift
    notes = [[] for _ in out_refs]
    for place in range(count):
        pick = slice(half * count + place, half * count + place + 1)
        keys, channels, out = half_slices(place, key_width, value_width, count)
        key_all = jnp.concatenate([p[:tokens, keys] for p in payloads], axis=0)
        value_all = jnp.concatenate([p[:tokens, channels] for p in payloads], axis=0)
        columns = slice(pick.start * key_width, pick.stop * key_width)
        rows = jnp.concatenate([ref[:, columns] for ref in rows_refs], axis=0)
        scores = times_transpose(rows, key_all) * weight[pick]
        sums = jnp.sum(scores, axis=1, keepdims=True)
        given = product(scores.astype(jnp.bfloat16), value_all).astype(jnp.bfloat16)
        for i, ref in enumerate(out_refs):
            here = slice(i * tokens, (i + 1) * tokens)
            ref[:, out] = given[here]
            notes[i] += three_terms(sums[here]) + three_terms(reach[pick])
    for ref, note in zip(out_refs, notes):
        ref[:, count * value_width :] = to_lanes(note, tokens).astype(jnp.bfloat16)


def serve_low_kernel(count, pair_ref, low_ref, near_ref, far_ref, next_ref, later_ref):
    answer(count, 0, [pair_ref, low_ref], [near_ref, far_ref], [next_ref, later_ref])


def serve_high_kernel(count, before_ref, last_ref, high_ref, near_ref, next_ref):
    answer(count, 1, [before_ref, last_ref, high_ref], [near_ref], [next_ref])


def gated_rows(count, half, given, message, totals, notes, gate_ref):
    value_width = totals[0].shape[1] // count
    low = half == 0
    own = jnp.where(low, notes[0][...], notes[1][...])
    lanes = message(slice(count * value_width, count * value_width + LANES))
    gated = []
    for place in range(count):
        out = slice(place * value_width, (place + 1) * value_width)
        start = pl.multiple_of((half * count + place) * value_width, value_width)
        at = 6 * place
        sums = lanes[:, at : at + 1] + lanes[:, at + 1 : at + 2] + lanes[:, at + 2 : at + 3]
        at += 3
        reach = lanes[:, at : at + 1] + lanes[:, at + 1 : at + 2] + lanes[:, at + 2 : at + 3]
        reach = reach + own[:, 3 * place + 2 : 3 * place + 3]
        top = own[:, 3 * place + 1 : 3 * place + 2]
        peak = jnp.where(given, jnp.maximum(top, reach), top)
        scale = jnp.exp(top - peak)
        scale_given = jnp.where(given, jnp.exp(reach - peak), 0.0)
        weight = scale * own[:, 3 * place : 3 * place + 1] + scale_given * sums
        inverse = 1.0 / jnp.maximum(jnp.abs(weight), 1.0)
        total = jnp.where(low, totals[0][:, out], totals[1][:, out])
        cell = (scale * inverse) * total + (scale_given * inverse) * message(out)
        hidden = cell.astype(jnp.bfloat16).astype(jnp.float32)
        gate = jax.nn.sigmoid(gate_ref[:, pl.ds(start, value_width)].astype(jnp.float32))
        gated.append((hidden * gate).astype(jnp.bfloat16))
    return jnp.concatenate(gated, axis=1)


def product(left, right):
    return jnp.dot(left, right, preferred_element_type=jnp.float32)


def first_half():
    return jnp.where(lax.axis_index("sp") == 3, 0, 1)


def rows_of(piece, half, rows):
    return piece[pl.ds(pl.multiple_of(half * rows, rows), rows), :]


def first_kernel(count, gate_ref, low_ref, low_note, high_ref, high_note, later_ref, *refs):
    pieces, gated_ref, part_ref = refs[:-2], refs[-2], refs[-1]
    rows, half = gated_ref.shape[1], first_half()

    def message(columns):
        return later_ref[:, columns].astype(jnp.float32)

    given = lax.axis_index("sp") == 3
    totals, notes = (low_ref, high_ref), (low_note, high_note)
    gated = gated_rows(count, half, given, message, totals, notes, gate_ref)
    gated_ref[...] = gated
    width = pieces[0].shape[1]
    for place, piece in enumerate(pieces):
        part_ref[:, place * width : (place + 1) * width] = product(
            gated, rows_of(piece, half, rows)
        )


def finish_kernel(
    count, whole, last, gate_ref, low_ref, low_note, high_ref, high_note, next_ref, nextx_ref,
    gated_ref, part_ref, *refs,
):
    pieces, out_ref = refs[:-1], refs[-1]
    rows, device = gated_ref.shape[1], lax.axis_index("dp")
    width = pieces[0].shape[1]
    half = first_half()

    def message(columns):
        return next_ref[:, columns].astype(jnp.float32) + nextx_ref[:, columns].astype(jnp.float32)

    given = lax.axis_index("sp") >= 2
    totals, notes = (low_ref, high_ref), (low_note, high_note)
    gated = gated_rows(count, 1 - half, given, message, totals, notes, gate_ref)

    def put(masks, columns):
        mask = jnp.where(device & CORE, masks[1], masks[0])
        start = pl.multiple_of((device ^ mask) * width, width)
        out_ref[:, pl.ds(start, width)] = columns.astype(out_ref.dtype)

    for place, (masks, piece) in enumerate(zip(whole, pieces)):
        part = part_ref[:, place * width : (place + 1) * width]
        put(masks, part + product(gated, rows_of(piece, 1 - half, rows)))
    for masks, piece in zip(last, pieces[len(whole) :]):
        part = product(gated_ref[...], rows_of(piece, half, rows))
        put(masks, part + product(gated, rows_of(piece, 1 - half, rows)))


def kernel_call(kernel, operands, outs, flops, limit):
    vmem = pl.BlockSpec(memory_space=pltpu.VMEM)
    size = sum(x.size * x.dtype.itemsize for x in (*operands, *outs))
    return pl.pallas_call(
        kernel,
        out_shape=outs,
        in_specs=[vmem] * len(operands),
        out_specs=[vmem] * len(outs),
        compiler_params=pltpu.CompilerParams(vmem_limit_bytes=limit * MIB),
        cost_estimate=pl.CostEstimate(flops=flops, bytes_accessed=size, transcendentals=0),
    )(*operands)


def block_body(queries, key_rows, values, out_gate, input_gate, forget_gate, out_weight):
    return block_steps(
        queries[0], key_rows[0], values[0], out_gate[0], input_gate[0], forget_gate[0], out_weight
    )[None]


def block_steps(query, key, value, gate, input_log, forget, out_weight):
    tokens, heads = query.shape[0], input_log.shape[0]
    key_width, value_width = query.shape[1] // heads, value.shape[1] // heads
    shape = jax.ShapeDtypeStruct
    device_count = lax.axis_size("dp")

    def swap(piece, bit):
        return lax.ppermute(piece, "dp", [(i, i ^ bit) for i in range(device_count)])

    count = heads // 2
    gates = jnp.concatenate([input_log, forget], axis=0)

    def payload(half):
        wide = key.shape[1] // 2
        tall = value.shape[1] // 2
        parts = [
            key[:, half * wide : (half + 1) * wide],
            value[:, half * tall : (half + 1) * tall],
        ]
        below = jnp.pad(gates, ((0, 0), (0, wide + tall - tokens)))
        return jnp.concatenate([jnp.concatenate(parts, axis=1), below], axis=0)

    high = payload(1)
    low = payload(0)
    last = lax.ppermute(high, "sp", [(0, 1), (1, 2)])
    near = lax.ppermute(query, "sp", [(2, 1), (3, 2)])
    far = lax.ppermute(query, "sp", [(3, 1)])
    pair = lax.ppermute(low, "sp", [(0, 1), (2, 3)])
    before = lax.ppermute(last, "sp", [(1, 2)])

    def cross(piece, even, odd):
        pairs = [(i, i ^ (odd if i & CORE else even)) for i in range(device_count)]
        return lax.ppermute(piece, "dp", pairs)

    side_a = cross(out_weight, XBIT, YBIT)
    side_b = cross(out_weight, YBIT, XBIT)
    corner = cross(side_a, YBIT, XBIT)
    whole = {
        (0, 0): out_weight,
        (CORE, CORE): swap(out_weight, CORE),
        (XBIT, YBIT): side_a,
        (YBIT | CORE, XBIT | CORE): swap(side_a, CORE),
        (YBIT, XBIT): side_b,
        (XBIT | CORE, YBIT | CORE): swap(side_b, CORE),
    }
    corners = {
        (XBIT | YBIT,) * 2: corner,
        (XBIT | YBIT | CORE,) * 2: swap(corner, CORE),
    }

    work = 2 * tokens * tokens * (key_width + value_width)
    sums = [
        shape((tokens, count * value_width), jnp.float32),
        shape((tokens, LANES), jnp.float32),
    ] * 2
    own = kernel_call(
        functools.partial(own_kernel, count), [low, high, query], sums, 3 * heads * work // 2, 8
    )
    message = shape((tokens, count * value_width + LANES), jnp.bfloat16)
    given_next, given_later = kernel_call(
        functools.partial(serve_low_kernel, count),
        [pair, low, near, far],
        [message] * 2,
        4 * count * work,
        8,
    )
    (given_high,) = kernel_call(
        functools.partial(serve_high_kernel, count),
        [before, last, high, near],
        [message],
        3 * count * work,
        8,
    )
    from_next = lax.ppermute(given_next, "sp", [(1, 2)])
    from_later = lax.ppermute(given_later, "sp", [(1, 3)])
    from_high = lax.ppermute(given_high, "sp", [(2, 3)])
    home = kernel_call(
        functools.partial(join_kernel, count),
        [pair, before, last, query, *own],
        sums,
        3 * heads * work // 2,
        8,
    )
    width = out_weight.shape[1]
    kept = kernel_call(
        functools.partial(first_kernel, count),
        [gate, *home, from_later, *whole.values()],
        [
            shape((tokens, count * value_width), jnp.bfloat16),
            shape((tokens, len(whole) * width), jnp.float32),
        ],
        2 * tokens * count * value_width * len(whole) * width,
        10,
    )
    (out,) = kernel_call(
        functools.partial(finish_kernel, count, tuple(whole), tuple(corners)),
        [gate, *home, from_next, from_high, *kept, *whole.values(), *corners.values()],
        [shape((tokens, width * device_count), jnp.bfloat16)],
        2 * tokens * count * value_width * width * device_count,
        12,
    )
    return out


def body(queries, key_rows, values, out_gate, input_gate, forget_gate, out_weight):
    group_count = lax.axis_size("sp")
    token_count = queries.shape[1]
    head_count = input_gate.shape[1]
    copies = group_count // head_count
    head_key = queries.shape[2] // head_count
    slice_width = values.shape[2] // group_count

    def spread(source):
        widened = jnp.broadcast_to(
            source[0].reshape(token_count, head_count, 1, head_key),
            (token_count, head_count, copies, head_key),
        )
        return widened.reshape(token_count, group_count, head_key)

    def spread_gate(source):
        return jnp.repeat(source[0].T, copies, axis=1)

    query_all, key_all = (
        lax.all_to_all(spread(queries), "sp", split_axis=1, concat_axis=0, tiled=True),
        lax.all_to_all(spread(key_rows), "sp", split_axis=1, concat_axis=0, tiled=True),
    )
    value_all, input_all, forget_all = (
        lax.all_to_all(
            values[0].reshape(token_count, group_count, slice_width),
            "sp",
            split_axis=1,
            concat_axis=0,
            tiled=True,
        ),
        lax.all_to_all(spread_gate(input_gate), "sp", split_axis=1, concat_axis=0, tiled=True),
        lax.all_to_all(spread_gate(forget_gate), "sp", split_axis=1, concat_axis=0, tiled=True),
    )
    output = memory_cell(
        query_all[:, 0],
        key_all[:, 0],
        value_all[:, 0],
        input_all[:, 0].astype(jnp.float32),
        jax.nn.log_sigmoid(forget_all[:, 0].astype(jnp.float32)),
    )
    hidden = output.astype(jnp.bfloat16)
    token_rows = lax.all_to_all(hidden, "sp", split_axis=0, concat_axis=1, tiled=True)
    gated_rows = (
        token_rows.astype(jnp.float32) * jax.nn.sigmoid(out_gate[0].astype(jnp.float32))
    ).astype(jnp.bfloat16)
    projected = jnp.dot(
        gated_rows,
        lax.all_gather(out_weight, "dp", axis=1, tiled=True),
        preferred_element_type=jnp.float32,
    )
    return projected.astype(jnp.bfloat16)[None]


def solution(mesh):
    blocks = mesh.shape["sp"] == 4 and mesh.shape["dp"] == 8
    return jax.shard_map(
        block_body if blocks else body,
        mesh=mesh,
        in_specs=(
            P("dp", "sp", None),
            P("dp", "sp", None),
            P("dp", "sp", None),
            P("dp", "sp", None),
            P("dp", None, "sp"),
            P("dp", None, "sp"),
            P(None, "dp"),
        ),
        out_specs=P("dp", "sp", None),
        check_vma=False,
    )
```

```python
import functools

import jax
import jax.numpy as jnp
from jax import lax
from jax.experimental import pallas as pl
from jax.experimental.pallas import tpu as pltpu
from jax.sharding import PartitionSpec as P


BLOCK = 128


def memory_cell(query_rows, key_in, value_rows, input_log, forget_log):
    block_count = query_rows.shape[0] // BLOCK
    key_width = query_rows.shape[1]
    value_width = value_rows.shape[1]
    key_scale = key_width ** (-0.5)
    causal = lax.broadcasted_iota(jnp.int32, (BLOCK, BLOCK), 0) >= lax.broadcasted_iota(
        jnp.int32, (BLOCK, BLOCK), 1
    )
    highest = lax.Precision.HIGHEST

    def block_step(state_in, inputs):
        memory, normer, stabil = state_in
        query_part, key_part, value_part, gain_part, decay_part = inputs
        query_part = query_part.astype(jnp.float32)
        key_part = key_part.astype(jnp.float32) * key_scale
        value_part = value_part.astype(jnp.float32)
        running = jnp.cumsum(decay_part)
        log_weight = running[:, None] - running[None, :] + gain_part[None, :]
        log_weight = jnp.where(causal, log_weight, -jnp.inf)
        carried_log = running + stabil
        row_top = jnp.maximum(carried_log, jnp.max(log_weight, axis=1))
        scores = jnp.dot(query_part, key_part.T, precision=highest) * jnp.exp(
            log_weight - row_top[:, None]
        )
        carried = jnp.exp(carried_log - row_top)
        numerator = jnp.dot(scores, value_part, precision=highest) + carried[:, None] * jnp.dot(
            query_part, memory, precision=highest
        )
        denominator = jnp.sum(scores, axis=1) + carried * jnp.dot(
            query_part, normer, precision=highest
        )
        output = numerator / jnp.maximum(jnp.abs(denominator), 1.0)[:, None]
        block_end = running[-1]
        weight_log = block_end - running + gain_part
        new_top = jnp.maximum(block_end + stabil, jnp.max(weight_log))
        weights = jnp.exp(weight_log - new_top)
        retain = jnp.exp(block_end + stabil - new_top)
        memory = retain * memory + jnp.dot(
            (key_part * weights[:, None]).T, value_part, precision=highest
        )
        normer = retain * normer + jnp.dot(weights, key_part, precision=highest)
        return ((memory, normer, new_top), output)

    start_state = (
        jnp.zeros((key_width, value_width), jnp.float32),
        jnp.zeros((key_width,), jnp.float32),
        jnp.zeros((), jnp.float32),
    )
    blocks = tuple(
        (
            source.reshape((block_count, BLOCK) + source.shape[1:])
            for source in (query_rows, key_in, value_rows, input_log, forget_log)
        )
    )
    _, outputs = lax.scan(block_step, start_state, blocks)
    return outputs.reshape(block_count * BLOCK, value_width)


LANES = 128
NOTES = 8


def log_forget(gates):
    return -jnp.log1p(jnp.exp(-gates))


def running_sum(rows):
    width = rows.shape[1]
    upto = lax.broadcasted_iota(jnp.int32, (width, width), 0) <= lax.broadcasted_iota(
        jnp.int32, (width, width), 1
    )
    return jnp.dot(
        rows,
        upto.astype(jnp.float32),
        precision=lax.Precision.HIGHEST,
        preferred_element_type=jnp.float32,
    )


def times_transpose(left, right):
    return lax.dot_general(
        left, right, (((1,), (1,)), ((), ())), preferred_element_type=jnp.float32
    )


def three_terms(value):
    high = value.astype(jnp.bfloat16).astype(jnp.float32)
    middle = (value - high).astype(jnp.bfloat16).astype(jnp.float32)
    return [high, middle, value - high - middle]


def to_lanes(columns, rows):
    lane = lax.broadcasted_iota(jnp.int32, (rows, LANES), 1)
    tile = jnp.zeros((rows, LANES), jnp.float32)
    for place, column in enumerate(columns):
        tile = jnp.where(lane == place, column, tile)
    return tile


MIB = 1 << 20
CORE, XBIT, YBIT = 1, 2, 4


def gate_levels(payloads, tokens):
    gates = [payload[tokens:, :tokens].astype(jnp.float32) for payload in payloads]
    heads = gates[0].shape[0] // 2
    running = running_sum(log_forget(jnp.concatenate([g[heads:] for g in gates], axis=0)))
    parts = []
    for place, gate in enumerate(gates):
        sums = running[place * heads : (place + 1) * heads]
        parts.append((gate[:heads] - sums, sums[:, tokens - 1 :]))
    return parts


def two_term_dot(left, right):
    high = left.astype(jnp.bfloat16)
    low = (left - high.astype(jnp.float32)).astype(jnp.bfloat16)
    return jnp.dot(high, right, preferred_element_type=jnp.float32) + jnp.dot(
        low, right, preferred_element_type=jnp.float32
    )


def half_slices(place, key_width, value_width, count):
    start = count * key_width + place * value_width
    return (
        slice(place * key_width, (place + 1) * key_width),
        slice(start, start + value_width),
        slice(place * value_width, (place + 1) * value_width),
    )


def own_kernel(count, low_ref, high_ref, query_ref, *outs):
    tokens, key_width = query_ref.shape[0], query_ref.shape[1] // (2 * count)
    value_width = low_ref.shape[1] // count - key_width
    ((level, _),) = gate_levels([low_ref], tokens)
    causal = lax.broadcasted_iota(jnp.int32, (tokens, tokens), 0) >= lax.broadcasted_iota(
        jnp.int32, (tokens, tokens), 1
    )
    for half, payload in enumerate((low_ref, high_ref)):
        total_ref, note_ref = outs[2 * half : 2 * half + 2]
        notes = []
        for place in range(count):
            head = half * count + place
            keys, channels, out = half_slices(place, key_width, value_width, count)
            masked = jnp.where(causal, level[head : head + 1], -jnp.inf)
            top = jnp.max(masked, axis=1, keepdims=True)
            rows = query_ref[:, head * key_width : (head + 1) * key_width]
            scores = times_transpose(rows, payload[:tokens, keys]) * (key_width ** (-0.5))
            scores = scores * jnp.exp(masked - top)
            total_ref[:, out] = two_term_dot(scores, payload[:tokens, channels])
            notes += [jnp.sum(scores, axis=1, keepdims=True), top]
        note_ref[...] = to_lanes(notes, tokens)


def join_kernel(count, pair_ref, before_ref, last_ref, query_ref, *refs):
    tokens, key_width = query_ref.shape[0], query_ref.shape[1] // (2 * count)
    value_width = pair_ref.shape[1] // count - key_width
    block = lax.axis_index("sp")
    second, both = lax.rem(block, 2) == 1, block == 2
    upper = (block == 1) | both
    start = jnp.where(block == 0, 0.0, -jnp.inf)
    (level, end), (level0, end0), (level1, end1) = gate_levels(
        [pair_ref, before_ref, last_ref], tokens
    )
    top = jnp.max(level, axis=1, keepdims=True)
    top = jnp.where(block == 1, jnp.maximum(top, 0.0), top)
    end0 = jnp.where(both, end0, 0.0)
    level1 = level1 - end0
    top1 = jnp.maximum(jnp.max(level1, axis=1, keepdims=True), 0.0)
    top1 = jnp.where(both, jnp.maximum(top1, jnp.max(level0, axis=1, keepdims=True)), top1)
    weight0 = jnp.where(both, jnp.exp(level0 - top1), 0.0)
    cases = (
        (
            [pair_ref],
            jnp.exp(level - top),
            second,
            jnp.where(second, top + end, start),
            jnp.where(block == 3, end, 0.0),
        ),
        (
            [before_ref, last_ref],
            jnp.concatenate([weight0, jnp.exp(level1 - top1)], axis=1),
            upper,
            jnp.where(upper, top1 + end0 + end1, start),
            jnp.zeros_like(end),
        ),
    )
    for half, (payloads, weight, valid, state, shift) in enumerate(cases):
        own_total, own_note, total_ref, note_ref = (
            refs[2 * half], refs[2 * half + 1], refs[2 * half + 4], refs[2 * half + 5]
        )
        own = own_note[...]
        notes = []
        for place in range(count):
            head = half * count + place
            pick = slice(head, head + 1)
            keys, channels, out = half_slices(place, key_width, value_width, count)
            own_top = own[:, 2 * place + 1 : 2 * place + 2]
            peak = jnp.maximum(own_top, state[pick])
            scale = jnp.exp(own_top - peak)
            scale0 = jnp.where(valid, jnp.exp(state[pick] - peak), 0.0) * (key_width ** (-0.5))
            key_all = jnp.concatenate([p[:tokens, keys] for p in payloads], axis=0)
            value_all = jnp.concatenate([p[:tokens, channels] for p in payloads], axis=0)
            rows = query_ref[:, head * key_width : (head + 1) * key_width]
            scores = times_transpose(rows, key_all) * weight[pick] * scale0
            total_ref[:, out] = scale * own_total[:, out] + two_term_dot(scores, value_all)
            sums = scale * own[:, 2 * place : 2 * place + 1] + jnp.sum(
                scores, axis=1, keepdims=True
            )
            notes += [sums, peak, shift[pick]]
        note_ref[...] = to_lanes(notes, tokens)


def answer(count, half, payloads, rows_refs, out_refs):
    tokens, key_width = rows_refs[0].shape[0], rows_refs[0].shape[1] // (2 * count)
    value_width = payloads[0].shape[1] // count - key_width
    levels, shift = [], 0.0
    for level, end in gate_levels(payloads, tokens):
        levels.append(level - shift)
        shift = shift + end
    level = jnp.concatenate(levels, axis=1)
    top = jnp.maximum(jnp.max(level, axis=1, keepdims=True), 0.0)
    weight = jnp.exp(level - top) * (key_width ** (-0.5))
    reach = top + shift
    notes = [[] for _ in out_refs]
    for place in range(count):
        pick = slice(half * count + place, half * count + place + 1)
        keys, channels, out = half_slices(place, key_width, value_width, count)
        key_all = jnp.concatenate([p[:tokens, keys] for p in payloads], axis=0)
        value_all = jnp.concatenate([p[:tokens, channels] for p in payloads], axis=0)
        columns = slice(pick.start * key_width, pick.stop * key_width)
        rows = jnp.concatenate([ref[:, columns] for ref in rows_refs], axis=0)
        scores = times_transpose(rows, key_all) * weight[pick]
        sums = jnp.sum(scores, axis=1, keepdims=True)
        given = product(scores.astype(jnp.bfloat16), value_all).astype(jnp.bfloat16)
        for i, ref in enumerate(out_refs):
            here = slice(i * tokens, (i + 1) * tokens)
            ref[:tokens, out] = given[here]
            notes[i] += three_terms(sums[here]) + three_terms(reach[pick])
            notes[i] += [jnp.zeros((1, 1), jnp.float32)] * (NOTES - 6)
    for ref, note in zip(out_refs, notes):
        rows = jnp.transpose(to_lanes(note, tokens))
        for place in range(count):
            group = slice(place * tokens, (place + 1) * tokens)
            ref[tokens:, group] = rows[place * NOTES : (place + 1) * NOTES].astype(jnp.bfloat16)
        ref[tokens:, count * tokens :] = jnp.zeros(
            (NOTES, ref.shape[1] - count * tokens), jnp.bfloat16
        )


def serve_low_kernel(count, pair_ref, low_ref, near_ref, far_ref, next_ref, later_ref):
    answer(count, 0, [pair_ref, low_ref], [near_ref, far_ref], [next_ref, later_ref])


def serve_high_kernel(count, before_ref, last_ref, high_ref, near_ref, next_ref):
    answer(count, 1, [before_ref, last_ref, high_ref], [near_ref], [next_ref])


def gated_rows(count, half, given, message, totals, notes, gate_ref):
    value_width = totals[0].shape[1] // count
    low = half == 0
    own = jnp.where(low, notes[0][...], notes[1][...])
    tokens = totals[0].shape[0]
    tiles = [
        message(slice(tokens, None), slice(place * tokens, (place + 1) * tokens))
        for place in range(count)
    ]
    tiles.append(jnp.zeros((LANES - count * NOTES, tokens), jnp.float32))
    lanes = jnp.transpose(jnp.concatenate(tiles, axis=0))
    gated = []
    for place in range(count):
        out = slice(place * value_width, (place + 1) * value_width)
        start = pl.multiple_of((half * count + place) * value_width, value_width)
        at = NOTES * place
        sums = lanes[:, at : at + 1] + lanes[:, at + 1 : at + 2] + lanes[:, at + 2 : at + 3]
        at += 3
        reach = lanes[:, at : at + 1] + lanes[:, at + 1 : at + 2] + lanes[:, at + 2 : at + 3]
        reach = reach + own[:, 3 * place + 2 : 3 * place + 3]
        top = own[:, 3 * place + 1 : 3 * place + 2]
        peak = jnp.where(given, jnp.maximum(top, reach), top)
        scale = jnp.exp(top - peak)
        scale_given = jnp.where(given, jnp.exp(reach - peak), 0.0)
        weight = scale * own[:, 3 * place : 3 * place + 1] + scale_given * sums
        inverse = 1.0 / jnp.maximum(jnp.abs(weight), 1.0)
        total = jnp.where(low, totals[0][:, out], totals[1][:, out])
        cell = (scale * inverse) * total + (scale_given * inverse) * message(slice(0, tokens), out)
        hidden = cell.astype(jnp.bfloat16).astype(jnp.float32)
        gate = jax.nn.sigmoid(gate_ref[:, pl.ds(start, value_width)].astype(jnp.float32))
        gated.append((hidden * gate).astype(jnp.bfloat16))
    return jnp.concatenate(gated, axis=1)


def product(left, right):
    return jnp.dot(left, right, preferred_element_type=jnp.float32)


def first_half():
    return jnp.where(lax.axis_index("sp") == 3, 0, 1)


def rows_of(piece, half, rows):
    return piece[pl.ds(pl.multiple_of(half * rows, rows), rows), :]


def first_kernel(count, gate_ref, low_ref, low_note, high_ref, high_note, later_ref, *refs):
    pieces, gated_ref, part_ref = refs[:-2], refs[-2], refs[-1]
    rows, half = gated_ref.shape[1], first_half()

    def message(rows, columns):
        return later_ref[rows, columns].astype(jnp.float32)

    given = lax.axis_index("sp") == 3
    totals, notes = (low_ref, high_ref), (low_note, high_note)
    gated = gated_rows(count, half, given, message, totals, notes, gate_ref)
    gated_ref[...] = gated
    width = pieces[0].shape[1]
    for place, piece in enumerate(pieces):
        part_ref[:, place * width : (place + 1) * width] = product(
            gated, rows_of(piece, half, rows)
        )


def finish_kernel(
    count, whole, last, gate_ref, low_ref, low_note, high_ref, high_note, next_ref, nextx_ref,
    gated_ref, part_ref, *refs,
):
    pieces, out_ref = refs[:-1], refs[-1]
    rows, device = gated_ref.shape[1], lax.axis_index("dp")
    width = pieces[0].shape[1]
    half = first_half()

    def message(rows, columns):
        return next_ref[rows, columns].astype(jnp.float32) + nextx_ref[rows, columns].astype(
            jnp.float32
        )

    given = lax.axis_index("sp") >= 2
    totals, notes = (low_ref, high_ref), (low_note, high_note)
    gated = gated_rows(count, 1 - half, given, message, totals, notes, gate_ref)

    def put(masks, columns):
        mask = jnp.where(device & CORE, masks[1], masks[0])
        start = pl.multiple_of((device ^ mask) * width, width)
        out_ref[:, pl.ds(start, width)] = columns.astype(out_ref.dtype)

    for place, (masks, piece) in enumerate(zip(whole, pieces)):
        part = part_ref[:, place * width : (place + 1) * width]
        put(masks, part + product(gated, rows_of(piece, 1 - half, rows)))
    for masks, piece in zip(last, pieces[len(whole) :]):
        part = product(gated_ref[...], rows_of(piece, half, rows))
        put(masks, part + product(gated, rows_of(piece, 1 - half, rows)))


def kernel_call(kernel, operands, outs, flops, limit):
    vmem = pl.BlockSpec(memory_space=pltpu.VMEM)
    size = sum(x.size * x.dtype.itemsize for x in (*operands, *outs))
    return pl.pallas_call(
        kernel,
        out_shape=outs,
        in_specs=[vmem] * len(operands),
        out_specs=[vmem] * len(outs),
        compiler_params=pltpu.CompilerParams(vmem_limit_bytes=limit * MIB),
        cost_estimate=pl.CostEstimate(flops=flops, bytes_accessed=size, transcendentals=0),
    )(*operands)


def block_body(queries, key_rows, values, out_gate, input_gate, forget_gate, out_weight):
    return block_steps(
        queries[0], key_rows[0], values[0], out_gate[0], input_gate[0], forget_gate[0], out_weight
    )[None]


def block_steps(query, key, value, gate, input_log, forget, out_weight):
    tokens, heads = query.shape[0], input_log.shape[0]
    key_width, value_width = query.shape[1] // heads, value.shape[1] // heads
    shape = jax.ShapeDtypeStruct
    device_count = lax.axis_size("dp")

    def swap(piece, bit):
        return lax.ppermute(piece, "dp", [(i, i ^ bit) for i in range(device_count)])

    count = heads // 2
    gates = jnp.concatenate([input_log, forget], axis=0)

    def payload(half):
        wide = key.shape[1] // 2
        tall = value.shape[1] // 2
        parts = [
            key[:, half * wide : (half + 1) * wide],
            value[:, half * tall : (half + 1) * tall],
        ]
        below = jnp.pad(gates, ((0, 0), (0, wide + tall - tokens)))
        return jnp.concatenate([jnp.concatenate(parts, axis=1), below], axis=0)

    high = payload(1)
    low = payload(0)
    last = lax.ppermute(high, "sp", [(0, 1), (1, 2)])
    near = lax.ppermute(query, "sp", [(2, 1), (3, 2)])
    far = lax.ppermute(query, "sp", [(3, 1)])
    pair = lax.ppermute(low, "sp", [(0, 1), (2, 3)])
    before = lax.ppermute(last, "sp", [(1, 2)])

    def cross(piece, even, odd):
        pairs = [(i, i ^ (odd if i & CORE else even)) for i in range(device_count)]
        return lax.ppermute(piece, "dp", pairs)

    side_a = cross(out_weight, XBIT, YBIT)
    side_b = cross(out_weight, YBIT, XBIT)
    corner = cross(side_a, YBIT, XBIT)
    whole = {
        (0, 0): out_weight,
        (CORE, CORE): swap(out_weight, CORE),
        (XBIT, YBIT): side_a,
        (YBIT | CORE, XBIT | CORE): swap(side_a, CORE),
        (YBIT, XBIT): side_b,
        (XBIT | CORE, YBIT | CORE): swap(side_b, CORE),
    }
    corners = {
        (XBIT | YBIT,) * 2: corner,
        (XBIT | YBIT | CORE,) * 2: swap(corner, CORE),
    }

    work = 2 * tokens * tokens * (key_width + value_width)
    sums = [
        shape((tokens, count * value_width), jnp.float32),
        shape((tokens, LANES), jnp.float32),
    ] * 2
    own = kernel_call(
        functools.partial(own_kernel, count), [low, high, query], sums, 3 * heads * work // 2, 8
    )
    message = shape((tokens + NOTES, count * value_width), jnp.bfloat16)
    given_next, given_later = kernel_call(
        functools.partial(serve_low_kernel, count),
        [pair, low, near, far],
        [message] * 2,
        4 * count * work,
        8,
    )
    (given_high,) = kernel_call(
        functools.partial(serve_high_kernel, count),
        [before, last, high, near],
        [message],
        3 * count * work,
        8,
    )
    from_next = lax.ppermute(given_next, "sp", [(1, 2)])
    from_later = lax.ppermute(given_later, "sp", [(1, 3)])
    from_high = lax.ppermute(given_high, "sp", [(2, 3)])
    home = kernel_call(
        functools.partial(join_kernel, count),
        [pair, before, last, query, *own],
        sums,
        3 * heads * work // 2,
        8,
    )
    width = out_weight.shape[1]
    kept = kernel_call(
        functools.partial(first_kernel, count),
        [gate, *home, from_later, *whole.values()],
        [
            shape((tokens, count * value_width), jnp.bfloat16),
            shape((tokens, len(whole) * width), jnp.float32),
        ],
        2 * tokens * count * value_width * len(whole) * width,
        10,
    )
    (out,) = kernel_call(
        functools.partial(finish_kernel, count, tuple(whole), tuple(corners)),
        [gate, *home, from_next, from_high, *kept, *whole.values(), *corners.values()],
        [shape((tokens, width * device_count), jnp.bfloat16)],
        2 * tokens * count * value_width * width * device_count,
        12,
    )
    return out


def body(queries, key_rows, values, out_gate, input_gate, forget_gate, out_weight):
    group_count = lax.axis_size("sp")
    token_count = queries.shape[1]
    head_count = input_gate.shape[1]
    copies = group_count // head_count
    head_key = queries.shape[2] // head_count
    slice_width = values.shape[2] // group_count

    def spread(source):
        widened = jnp.broadcast_to(
            source[0].reshape(token_count, head_count, 1, head_key),
            (token_count, head_count, copies, head_key),
        )
        return widened.reshape(token_count, group_count, head_key)

    def spread_gate(source):
        return jnp.repeat(source[0].T, copies, axis=1)

    query_all, key_all = (
        lax.all_to_all(spread(queries), "sp", split_axis=1, concat_axis=0, tiled=True),
        lax.all_to_all(spread(key_rows), "sp", split_axis=1, concat_axis=0, tiled=True),
    )
    value_all, input_all, forget_all = (
        lax.all_to_all(
            values[0].reshape(token_count, group_count, slice_width),
            "sp",
            split_axis=1,
            concat_axis=0,
            tiled=True,
        ),
        lax.all_to_all(spread_gate(input_gate), "sp", split_axis=1, concat_axis=0, tiled=True),
        lax.all_to_all(spread_gate(forget_gate), "sp", split_axis=1, concat_axis=0, tiled=True),
    )
    output = memory_cell(
        query_all[:, 0],
        key_all[:, 0],
        value_all[:, 0],
        input_all[:, 0].astype(jnp.float32),
        jax.nn.log_sigmoid(forget_all[:, 0].astype(jnp.float32)),
    )
    hidden = output.astype(jnp.bfloat16)
    token_rows = lax.all_to_all(hidden, "sp", split_axis=0, concat_axis=1, tiled=True)
    gated_rows = (
        token_rows.astype(jnp.float32) * jax.nn.sigmoid(out_gate[0].astype(jnp.float32))
    ).astype(jnp.bfloat16)
    projected = jnp.dot(
        gated_rows,
        lax.all_gather(out_weight, "dp", axis=1, tiled=True),
        preferred_element_type=jnp.float32,
    )
    return projected.astype(jnp.bfloat16)[None]


def solution(mesh):
    blocks = mesh.shape["sp"] == 4 and mesh.shape["dp"] == 8
    return jax.shard_map(
        block_body if blocks else body,
        mesh=mesh,
        in_specs=(
            P("dp", "sp", None),
            P("dp", "sp", None),
            P("dp", "sp", None),
            P("dp", "sp", None),
            P("dp", None, "sp"),
            P("dp", None, "sp"),
            P(None, "dp"),
        ),
        out_specs=P("dp", "sp", None),
        check_vma=False,
    )
```
